128 devices in a mesh: kv: 16 (over z, x), tp: 8 (over y, core).
Axes of the slice: x: 4, y: 4, z: 4, core: 2. Of those that a mesh axis runs over, the one named last changes fastest.
Arguments:
- tokens: bfloat16 [65536, 2048], P('kv'), may hold values from -6 to 6
- w_query: bfloat16 [2048, 2048], P(None, 'tp'), may hold values from -0.125 to 0.125
- w_key: bfloat16 [2048, 2048], P(None, 'tp'), may hold values from -0.125 to 0.125
- w_value: bfloat16 [2048, 2048], P(None, 'tp'), may hold values from -0.125 to 0.125
- w_out: bfloat16 [2048, 2048], P('tp'), may hold values from -1 to 1, as said below
- query_gain: float32 [128], replicated, may hold values from 0.5 to 1.5
- key_gain: float32 [128], replicated, may hold values from 0.5 to 1.5
- out_gain: float32 [2048], replicated, may hold values from 0.5 to 1.5
- chosen: int32 [1024, 8], P('kv'), may hold values from -1 to 1023, as said below
Outputs:
- layer_out: bfloat16 [65536, 2048], P('kv', 'tp')
The draws below stay inside these ranges and needn't reach their ends.
Inputs may be any that keep to these rules, and one draw needn't show every extreme that they name: Row b of chosen lists min(8, b + 1) different key blocks, all at most b, with block b in the first slot, and -1 in the remaining slots. Split the blocks into groups of 64 consecutive blocks. The rows of one group other than the first name together at most 8 different blocks of the first group, and at most 2 different blocks of any other group but their own. Both bounds are reached. Entries of w_out have mean zero; the scale of a column grows smoothly with the feature index, by a factor of 8 from the first to the last feature.
All inputs are finite; a program needn't handle non-finite values.
Results may differ from the reference program's by a relative error of at most 0.025.
Values may be sent and summed in bfloat16 or wider, within the bound.
No kernel may reach another device: no remote copies, remote signals or barrier semaphores. Data moves between devices by JAX's collectives and lax.ppermute only.
A program may use at most 192 MiB of HBM per device.

```python
import jax
import jax.numpy as jnp
from jax import lax

D = 2048
HEADS = 16
HEAD_DIM = 128
BLOCK = 64
CHOSEN = 8
HOT = 8
REACH = 2
QB_DEV = 64
QBLOCKS = 1024
SEQ = 65536


def draw_w_out(key, part):
    rows = HEADS * HEAD_DIM
    base = jax.random.truncated_normal(key, -4.0, 4.0, (rows, D), jnp.float32)
    feature_pos = jnp.arange(D, dtype=jnp.float32) / D
    column_scale = jnp.exp2(3.0 * feature_pos - 1.5)
    return (base * column_scale[None, :] * rows ** (-0.5)).astype(jnp.bfloat16)


def draw_chosen(key, part):
    blocks_dev = QB_DEV
    owners = QBLOCKS // QB_DEV
    key_level, key_pool, key_pick = jax.random.split(key, 3)
    popularity = jax.random.randint(key_level, (QBLOCKS,), 0, 4)
    weight = 1 + popularity * popularity * popularity
    pool_jitter = jax.random.randint(key_pool, (owners, owners, blocks_dev), 0, 4096)
    positions = jnp.arange(blocks_dev, dtype=jnp.int32)
    pool_scores = pool_jitter * weight.reshape(owners, blocks_dev)[None] * blocks_dev + positions
    ranking = jnp.argsort(-pool_scores, axis=-1).astype(jnp.int32)
    first_pool = ranking[:, 0, :HOT]
    other_pool = ranking[:, :, :REACH]
    first_member = jnp.any(first_pool[:, :, None] == positions[None, None, :], axis=1)
    other_member = jnp.any(other_pool[:, :, :, None] == positions[None, None, None, :], axis=2)
    requester = jnp.arange(owners, dtype=jnp.int32)[:, None]
    owner_ids = jnp.arange(owners, dtype=jnp.int32)[None, :]
    member = jnp.where((owner_ids == 0)[:, :, None], first_member[:, None, :], other_member)
    member = member & (owner_ids < requester)[:, :, None]
    in_pool = member.reshape(owners, QBLOCKS)
    row_ids = jnp.arange(QBLOCKS, dtype=jnp.int32)
    device = row_ids // blocks_dev
    within = row_ids % blocks_dev
    forced_first = first_pool[device, within % HOT]
    previous = jnp.maximum(device - 1, 0)
    forced_second = other_pool[device, previous, within % REACH] + previous * blocks_dev
    columns = row_ids[None, :]
    local_earlier = (columns < row_ids[:, None]) & (columns >= (device * blocks_dev)[:, None])
    candidate = local_earlier | in_pool[device]
    candidate = candidate & jnp.logical_not((columns == forced_first[:, None]) & (device >= 1)[:, None])
    candidate = candidate & jnp.logical_not((columns == forced_second[:, None]) & (device >= 2)[:, None])
    jitter = jax.random.randint(key_pick, (QBLOCKS, QBLOCKS), 0, 4096)
    scores = jnp.where(candidate, jitter * weight[None, :] * QBLOCKS + columns, -1)
    values, picked = lax.top_k(scores, CHOSEN - 1)
    picked = jnp.where(values >= 0, picked, -1).astype(jnp.int32)
    trailing_one = jnp.concatenate([forced_first[:, None], picked[:, :CHOSEN - 2]], axis=1)
    trailing_two = jnp.concatenate([forced_first[:, None], forced_second[:, None], picked[:, :CHOSEN - 3]], axis=1)
    trailing = jnp.where((device >= 2)[:, None], trailing_two, jnp.where((device >= 1)[:, None], trailing_one, picked))
    return jnp.concatenate([row_ids[:, None], trailing], axis=1).astype(jnp.int32)


def shard_levels(key, dims, cuts, low, top_value):
    def one(position, parts):
        draws = jax.random.uniform(jax.random.fold_in(jax.random.fold_in(key, 6), position), (parts,), jnp.float32, low / len(cuts), top_value / len(cuts))
        return jnp.repeat(jnp.exp(draws), dims[position] // parts).reshape((-1,) + (1,) * (len(dims) - position - 1))

    gain = one(*cuts[0])
    for cut in cuts[1:]:
        gain = gain * one(*cut)
    return gain


def bell_draw(stream_key, shape, width, limit, cuts=(), kind=jnp.bfloat16):
    array = width * jax.random.normal(stream_key, shape, jnp.float32)
    if cuts:
        array = array * shard_levels(stream_key, shape, cuts, -0.22, 0.18)
    return jnp.clip(array, -limit, limit).astype(kind)


def setup_inputs(seed: int = 0) -> dict:
    streams_of = jax.random.split(jax.random.key(seed), 10)
    return {
        "tokens": bell_draw(streams_of[0], (SEQ, D), 1.0, 6.0, ((0, 16),)),
        "w_query": bell_draw(streams_of[1], (D, HEADS * HEAD_DIM), D ** -0.5, 0.125, ((1, 8),)),
        "w_key": bell_draw(streams_of[2], (D, HEADS * HEAD_DIM), D ** -0.5, 0.125, ((1, 8),)),
        "w_value": bell_draw(streams_of[3], (D, HEADS * HEAD_DIM), D ** -0.5, 0.125, ((1, 8),)),
        "w_out": draw_w_out(jax.random.fold_in(streams_of[9], 71), 0),
        "query_gain": jnp.clip(1.0 + 0.1 * jax.random.normal(streams_of[5], (HEAD_DIM,), jnp.float32), 0.5, 1.5),
        "key_gain": jnp.clip(1.0 + 0.1 * jax.random.normal(streams_of[6], (HEAD_DIM,), jnp.float32), 0.5, 1.5),
        "out_gain": jnp.clip(1.0 + 0.1 * jax.random.normal(streams_of[7], (D,), jnp.float32), 0.5, 1.5),
        "chosen": draw_chosen(jax.random.fold_in(streams_of[9], 71), 0),
    }


norm_eps = 1e-06

def head_norm(values, gain_row):
    factor = lax.rsqrt(lax.optimization_barrier(jnp.mean(values * values, axis=-1, keepdims=True)) + norm_eps)
    return (values * factor * gain_row).astype(jnp.bfloat16)

def project(tokens, weight):
    return jnp.dot(tokens, weight, preferred_element_type=jnp.float32).astype(jnp.bfloat16)

def reference(tokens, w_query, w_key, w_value, w_out, query_gain, key_gain, out_gain, chosen):
    length = tokens.shape[0]
    queries = project(tokens, w_query).reshape(length, HEADS, HEAD_DIM)
    queries = head_norm(queries.astype(jnp.float32), query_gain)
    key_rows = project(tokens, w_key).reshape(length, HEADS, HEAD_DIM)
    key_rows = head_norm(key_rows.astype(jnp.float32), key_gain)
    value_rows = project(tokens, w_value).reshape(length, HEADS, HEAD_DIM)
    key_blocks = key_rows.reshape(QBLOCKS, BLOCK, HEADS, HEAD_DIM)
    value_blocks = value_rows.reshape(QBLOCKS, BLOCK, HEADS, HEAD_DIM)
    groups = QBLOCKS // QB_DEV
    query_groups = queries.reshape(groups, QB_DEV, BLOCK, HEADS, HEAD_DIM)
    chosen_groups = chosen.reshape(groups, QB_DEV, CHOSEN)

    def one_group(group_item):
        query_part, picked_rows = group_item
        usable = picked_rows >= 0
        gather_at = jnp.where(usable, picked_rows, 0).astype(jnp.int32)
        key_sel = key_blocks[gather_at].astype(jnp.float32)
        value_sel = value_blocks[gather_at].astype(jnp.float32)
        logits = jnp.einsum('bqhd,bjkhd->bhqjk', query_part.astype(jnp.float32), key_sel) * HEAD_DIM ** (-0.5)
        logits = jnp.where(usable[:, None, None, :, None], logits, -jnp.inf)
        flattened = logits.reshape(QB_DEV, HEADS, BLOCK, CHOSEN * BLOCK)
        row_peak = lax.optimization_barrier(jnp.max(flattened, axis=-1, keepdims=True))
        weights = jnp.exp(flattened - row_peak)
        totals = lax.optimization_barrier(jnp.sum(weights, axis=-1))
        rounded = lax.optimization_barrier(weights.astype(jnp.bfloat16)).astype(jnp.float32)
        rounded = rounded.reshape(QB_DEV, HEADS, BLOCK, CHOSEN, BLOCK)
        combined = jnp.einsum('bhqjk,bjkhd->bqhd', rounded, value_sel)
        return (combined / jnp.transpose(totals, (0, 2, 1))[..., None]).astype(jnp.bfloat16)
    attended = lax.map(one_group, (query_groups, chosen_groups))
    attended = attended.reshape(length, HEADS * HEAD_DIM)
    combined = jnp.dot(attended, w_out, preferred_element_type=jnp.float32)
    factor = lax.rsqrt(lax.optimization_barrier(jnp.mean(combined * combined, axis=-1, keepdims=True)) + norm_eps)
    return (combined * factor * out_gain).astype(jnp.bfloat16)
```

```python
import jax
import jax.numpy as jnp
from jax import lax
from jax.experimental import pallas as pl
from jax.experimental.pallas import tpu as pltpu
from jax.sharding import Mesh
from jax.sharding import PartitionSpec as P

HEAD_DIM = 128
BLOCK = 64
HOT = 8
KV = ("kv_0", "kv_1")
TP = ("tp_0", "tp_1")
WIDTH = 256
PAIR = 2
norm_eps = 1e-06
LOG2E = 1.4426950408889634
bf16 = jnp.bfloat16
f32 = jnp.float32
VMEM_LIMIT = 60 * 1024 * 1024


def head_norm(values, gain_row):
    factor = lax.rsqrt(jnp.mean(values * values, axis=-1, keepdims=True) + norm_eps)
    return (values * factor * gain_row).astype(bf16)


def kv_kernel(tok, wk, wv, gain, out):
    rows = tok[...]
    keys = jnp.dot(rows, wk[...], preferred_element_type=f32)
    blocks = out.shape[0]
    for h in range(2):
        lanes = slice(h * HEAD_DIM, (h + 1) * HEAD_DIM)
        normed = head_norm(keys[:, lanes], gain[...])
        out[:, 0, :, lanes] = normed.reshape(blocks, BLOCK, HEAD_DIM)
    vals = jnp.dot(rows, wv[...], preferred_element_type=f32).astype(bf16)
    out[:, 1, :, :] = vals.reshape(blocks, BLOCK, WIDTH)


def project_kv(tokens, w_key, w_value, gain):
    length, depth = tokens.shape
    tile = min(512, length)
    blocks = tile // BLOCK
    return pl.pallas_call(
        kv_kernel,
        grid=(length // tile,),
        in_specs=[
            pl.BlockSpec((tile, depth), lambda i: (i, 0)),
            pl.BlockSpec((depth, WIDTH), lambda i: (0, 0)),
            pl.BlockSpec((depth, WIDTH), lambda i: (0, 0)),
            pl.BlockSpec((1, HEAD_DIM), lambda i: (0, 0)),
        ],
        out_specs=pl.BlockSpec((blocks, PAIR, BLOCK, WIDTH), lambda i: (i, 0, 0, 0)),
        out_shape=jax.ShapeDtypeStruct((length // BLOCK, PAIR, BLOCK, WIDTH), bf16),
        compiler_params=pltpu.CompilerParams(vmem_limit_bytes=VMEM_LIMIT),
        cost_estimate=pl.CostEstimate(
            flops=4 * length * depth * WIDTH, bytes_accessed=2 * length * depth, transcendentals=0
        ),
        name="project_kv",
    )(tokens, w_key, w_value, gain)


def q_kernel(tok, wq, gain, out):
    values = jnp.dot(tok[...], wq[...], preferred_element_type=f32)
    for h in range(2):
        lanes = slice(h * HEAD_DIM, (h + 1) * HEAD_DIM)
        out[:, lanes] = head_norm(values[:, lanes], gain[...])


def project_q(tokens, w_query, gain):
    length, depth = tokens.shape
    tile = 512
    return pl.pallas_call(
        q_kernel,
        grid=(length // tile,),
        in_specs=[
            pl.BlockSpec((tile, depth), lambda i: (i, 0)),
            pl.BlockSpec((depth, WIDTH), lambda i: (0, 0)),
            pl.BlockSpec((1, HEAD_DIM), lambda i: (0, 0)),
        ],
        out_specs=pl.BlockSpec((tile, WIDTH), lambda i: (i, 0)),
        out_shape=jax.ShapeDtypeStruct((length, WIDTH), bf16),
        compiler_params=pltpu.CompilerParams(vmem_limit_bytes=VMEM_LIMIT),
        cost_estimate=pl.CostEstimate(
            flops=2 * length * depth * WIDTH, bytes_accessed=2 * length * depth, transcendentals=0
        ),
        name="project_q",
    )(tokens, w_query, gain)


def attention_kernel(at, q, mask, local, got, out, table, sems):
    step = pl.program_id(0)
    here = local.shape[0]

    @pl.when(step == 0)
    def _():
        first = pltpu.make_async_copy(local, table.at[pl.ds(0, here)], sems.at[0])
        second = pltpu.make_async_copy(got, table.at[pl.ds(here, got.shape[0])], sems.at[1])
        first.start()
        second.start()
        first.wait()
        second.wait()

    blocks = q.shape[0] // BLOCK
    slots = mask.shape[1] // BLOCK

    def one(i, carry):
        row = pl.multiple_of(i * BLOCK, BLOCK)
        rows = q[pl.ds(row, BLOCK), :]
        blank = jnp.zeros((BLOCK, HEAD_DIM), bf16)
        both = jnp.concatenate(
            [
                jnp.concatenate([rows[:, :HEAD_DIM], blank], axis=1),
                jnp.concatenate([blank, rows[:, HEAD_DIM:]], axis=1),
            ],
            axis=0,
        )
        base = (step * blocks + i) * slots
        picks = [at[base + j] for j in range(slots)]
        keys = jnp.concatenate([table[p, 0] for p in picks], axis=0)
        logits = lax.dot_general(both, keys, (((1,), (1,)), ((), ())), preferred_element_type=f32)
        weights = jnp.exp2(logits) * mask[pl.ds(i, 1), :]
        totals = jnp.sum(weights, axis=-1, keepdims=True)
        values = jnp.concatenate([table[p, 1] for p in picks], axis=0)
        sums = jnp.dot(weights.astype(bf16), values, preferred_element_type=f32)
        scale = 1.0 / totals
        out[pl.ds(row, BLOCK), :HEAD_DIM] = (
            sums[:BLOCK, :HEAD_DIM] * scale[:BLOCK]
        ).astype(bf16)
        out[pl.ds(row, BLOCK), HEAD_DIM:] = (
            sums[BLOCK:, HEAD_DIM:] * scale[BLOCK:]
        ).astype(bf16)
        return carry

    lax.fori_loop(0, blocks, one, 0, unroll=4)


def attend(at, queries, mask, local, got):
    length = queries.shape[0]
    slots = mask.shape[1] // BLOCK
    per = 16
    steps = length // (per * BLOCK)
    return pl.pallas_call(
        attention_kernel,
        grid_spec=pltpu.PrefetchScalarGridSpec(
            num_scalar_prefetch=1,
            grid=(steps,),
            in_specs=[
                pl.BlockSpec((per * BLOCK, WIDTH), lambda i, at: (i, 0)),
                pl.BlockSpec((per, slots * BLOCK), lambda i, at: (i, 0)),
                pl.BlockSpec(memory_space=pl.ANY),
                pl.BlockSpec(memory_space=pl.ANY),
            ],
            out_specs=pl.BlockSpec((per * BLOCK, WIDTH), lambda i, at: (i, 0)),
            scratch_shapes=[
                pltpu.VMEM((local.shape[0] + got.shape[0],) + local.shape[1:], bf16),
                pltpu.SemaphoreType.DMA((2,)),
            ],
        ),
        out_shape=jax.ShapeDtypeStruct((length, WIDTH), bf16),
        compiler_params=pltpu.CompilerParams(vmem_limit_bytes=VMEM_LIMIT),
        cost_estimate=pl.CostEstimate(
            flops=8 * length * WIDTH * slots * BLOCK, bytes_accessed=16 << 20, transcendentals=0
        ),
        name="attend",
    )(at, queries, mask, local, got)


def out_kernel(order, pieces, w_same, w_other, gain, out, acc):
    k = pl.program_id(0)
    half = pl.num_programs(0) // 2

    @pl.when(k == 0)
    def _():
        acc[...] = jnp.dot(pieces[0], w_same[0], preferred_element_type=f32)

    @pl.when((k > 0) & (k < half))
    def _():
        acc[...] += jnp.dot(pieces[0], w_same[0], preferred_element_type=f32)

    @pl.when((k >= half) & (k < 2 * half - 1))
    def _():
        acc[...] += jnp.dot(pieces[0], w_other[0], preferred_element_type=f32)

    @pl.when(k == 2 * half - 1)
    def _():
        mixed = acc[...] + jnp.dot(pieces[0], w_other[0], preferred_element_type=f32)
        width = mixed.shape[1]
        squares = jnp.sum(mixed * mixed, axis=-1, keepdims=True)
        factor = lax.rsqrt(squares * (1.0 / width) + norm_eps)
        normed = (mixed * factor * gain[...]).astype(bf16)
        for j in range(out.shape[0]):
            out[j] = normed[:, j * WIDTH : (j + 1) * WIDTH]


def project_out(order, pieces, w_same, w_other, gain):
    count, rows, _ = pieces.shape
    half = count // 2
    width = w_same.shape[2]
    return pl.pallas_call(
        out_kernel,
        grid_spec=pltpu.PrefetchScalarGridSpec(
            num_scalar_prefetch=1,
            grid=(count,),
            in_specs=[
                pl.BlockSpec((1, rows, WIDTH), lambda k, order: (order[k], 0, 0)),
                pl.BlockSpec((1, WIDTH, width), lambda k, order: (jnp.minimum(k, half - 1), 0, 0)),
                pl.BlockSpec((1, WIDTH, width), lambda k, order: (jnp.maximum(k - half, 0), 0, 0)),
                pl.BlockSpec((1, width), lambda k, order: (0, 0)),
            ],
            out_specs=pl.BlockSpec((count, rows, WIDTH), lambda k, order: (0, 0, 0)),
            scratch_shapes=[pltpu.VMEM((rows, width), f32)],
        ),
        out_shape=jax.ShapeDtypeStruct((count, rows, WIDTH), bf16),
        compiler_params=pltpu.CompilerParams(vmem_limit_bytes=VMEM_LIMIT),
        cost_estimate=pl.CostEstimate(
            flops=2 * rows * width * width, bytes_accessed=12 << 20, transcendentals=0
        ),
        name="project_out",
    )(order, pieces, w_same, w_other, gain)


def exchange(pieces, axes):
    return lax.all_to_all(pieces, axes, split_axis=0, concat_axis=0, tiled=True)


def gather_w_out(w_out):
    ring = lax.axis_size(TP[0])
    parts = [w_out]
    for shift in range(1, ring):
        parts.append(lax.ppermute(w_out, TP[0], [(i, (i + shift) % ring) for i in range(ring)]))
    same = jnp.stack(parts)
    other = lax.ppermute(same, TP[1], [(0, 1), (1, 0)])
    y = lax.axis_index(TP[0])
    c = lax.axis_index(TP[1])
    rows = (y - jnp.arange(ring, dtype=jnp.int32)) % ring
    order = jnp.concatenate([2 * rows + c, 2 * rows + 1 - c]).astype(jnp.int32)
    return same, other, order


def local(tokens, w_query, w_key, w_value, w_out, query_gain, key_gain, out_gain, chosen):
    length, model_width = tokens.shape
    blocks_here = length // BLOCK
    devices = lax.axis_size(KV)
    position = lax.axis_index(KV)
    ranks = lax.axis_size(TP)

    usable = chosen >= 0
    pick = jnp.where(usable, chosen, 0)
    owner_of = pick // blocks_here
    all_blocks = jnp.arange(devices * blocks_here, dtype=jnp.int32)
    marked = jnp.where(usable & (owner_of != position), chosen, -1)
    wanted = jnp.any(marked[:, :, None] == all_blocks[None, None, :], axis=(0, 1)).reshape(
        devices, blocks_here
    )
    rank_of = jnp.cumsum(wanted.astype(jnp.int32), axis=1) - 1
    local_ids = jnp.arange(blocks_here, dtype=jnp.int32)
    places = wanted[:, :, None] & (
        rank_of[:, :, None] == jnp.arange(HOT, dtype=jnp.int32)[None, None, :]
    )
    requests = jnp.sum(jnp.where(places, local_ids[None, :, None], 0), axis=1).astype(jnp.int32)
    asked_for = exchange(requests, KV)
    flat_rank = rank_of.reshape(-1)
    slot_rank = jnp.sum(
        jnp.where(pick[:, :, None] == all_blocks[None, None, :], flat_rank[None, None, :], 0), axis=-1
    )
    at = jnp.where(
        owner_of == position, pick % blocks_here, blocks_here + owner_of * HOT + slot_rank
    )
    at = jnp.where(usable, at, 0).astype(jnp.int32).reshape(-1)
    mask = jnp.repeat(usable.astype(f32), BLOCK, axis=1)

    w_same, w_other, order = gather_w_out(w_out)

    key_row = key_gain[None, :]
    query_row = (query_gain * (HEAD_DIM ** (-0.5) * LOG2E))[None, :]
    pairs = project_kv(tokens, w_key, w_value, key_row)
    sent = pairs[asked_for.reshape(-1)].reshape(devices, HOT, PAIR, BLOCK, WIDTH)
    got = exchange(sent, KV).reshape(devices * HOT, PAIR, BLOCK, WIDTH)
    queries = project_q(tokens, w_query, query_row)
    attended = attend(at, queries, mask, pairs, got)
    pieces = exchange(attended.reshape(ranks, length // ranks, WIDTH), TP)
    normed = project_out(order, pieces, w_same, w_other, out_gain[None, :])
    return exchange(normed, TP).reshape(length, WIDTH)


def solution(mesh):
    split = Mesh(mesh.devices.reshape(4, 4, 4, 2), KV + TP)
    return jax.shard_map(
        local,
        mesh=split,
        in_specs=(
            P(KV, None),
            P(None, TP),
            P(None, TP),
            P(None, TP),
            P(TP, None),
            P(),
            P(),
            P(),
            P(KV, None),
        ),
        out_specs=P(KV, TP),
        check_vma=False,
    )
```

```python
import jax
import jax.numpy as jnp
from jax import lax
from jax.experimental import pallas as pl
from jax.experimental.pallas import tpu as pltpu
from jax.sharding import Mesh
from jax.sharding import PartitionSpec as P

HEAD_DIM = 128
BLOCK = 64
HOT = 8
REACH = 2
KV = ("kv_0", "kv_1")
TP = ("tp_0", "tp_1")
WIDTH = 256
PAIR = 2
norm_eps = 1e-06
LOG2E = 1.4426950408889634
bf16 = jnp.bfloat16
f32 = jnp.float32
VMEM_LIMIT = 60 * 1024 * 1024


def head_norm(values, gain_row):
    factor = lax.rsqrt(jnp.mean(values * values, axis=-1, keepdims=True) + norm_eps)
    return (values * factor * gain_row).astype(bf16)


def kv_kernel(tok, wk, wv, gain, out):
    rows = tok[...]
    keys = jnp.dot(rows, wk[...], preferred_element_type=f32)
    blocks = out.shape[0]
    for h in range(2):
        lanes = slice(h * HEAD_DIM, (h + 1) * HEAD_DIM)
        normed = head_norm(keys[:, lanes], gain[...])
        out[:, 0, :, lanes] = normed.reshape(blocks, BLOCK, HEAD_DIM)
    vals = jnp.dot(rows, wv[...], preferred_element_type=f32).astype(bf16)
    out[:, 1, :, :] = vals.reshape(blocks, BLOCK, WIDTH)


def project_kv(tokens, w_key, w_value, gain):
    length, depth = tokens.shape
    tile = min(512, length)
    blocks = tile // BLOCK
    return pl.pallas_call(
        kv_kernel,
        grid=(length // tile,),
        in_specs=[
            pl.BlockSpec((tile, depth), lambda i: (i, 0)),
            pl.BlockSpec((depth, WIDTH), lambda i: (0, 0)),
            pl.BlockSpec((depth, WIDTH), lambda i: (0, 0)),
            pl.BlockSpec((1, HEAD_DIM), lambda i: (0, 0)),
        ],
        out_specs=pl.BlockSpec((blocks, PAIR, BLOCK, WIDTH), lambda i: (i, 0, 0, 0)),
        out_shape=jax.ShapeDtypeStruct((length // BLOCK, PAIR, BLOCK, WIDTH), bf16),
        compiler_params=pltpu.CompilerParams(vmem_limit_bytes=VMEM_LIMIT),
        cost_estimate=pl.CostEstimate(
            flops=4 * length * depth * WIDTH, bytes_accessed=2 * length * depth, transcendentals=0
        ),
        name="project_kv",
    )(tokens, w_key, w_value, gain)


def hot_kernel(asked, order, same, other, wk, wv, gain, out, keep):
    keys = jnp.zeros((same.shape[1], WIDTH), f32)
    vals = jnp.zeros((same.shape[1], WIDTH), f32)
    count = same.shape[0]
    for k in range(2 * count):
        rows = same[k] if k < count else other[k - count]
        span = pl.ds(pl.multiple_of(order[k] * WIDTH, WIDTH), WIDTH)
        keys += jnp.dot(rows, wk[span, :], preferred_element_type=f32)
        vals += jnp.dot(rows, wv[span, :], preferred_element_type=f32)
    part = out.shape[1] // 2
    groups = keep.shape[0]
    for h in range(2):
        lanes = slice(h * HEAD_DIM, (h + 1) * HEAD_DIM)
        x = keys[:, lanes]
        factor = lax.rsqrt(jnp.mean(x * x, axis=-1, keepdims=True) + norm_eps)
        keep[:, :part, lanes] = (x * factor * gain[...]).reshape(groups, part, HEAD_DIM)
    keep[:, part:, :] = vals.reshape(groups, part, WIDTH)

    def one(m, carry):
        out[m] = keep[asked[m]].astype(bf16)
        return carry

    lax.fori_loop(0, out.shape[0], one, 0, unroll=8)


def project_hot(asked, order, same, other, w_key, w_value, gain):
    count, rows, _ = same.shape
    groups = 64
    part = rows // groups
    depth = w_key.shape[0]
    sends = asked.shape[0]
    whole = lambda *shape: pl.BlockSpec(shape, lambda i, a, o: (0,) * len(shape))
    return pl.pallas_call(
        hot_kernel,
        grid_spec=pltpu.PrefetchScalarGridSpec(
            num_scalar_prefetch=2,
            grid=(1,),
            in_specs=[
                whole(count, rows, WIDTH),
                whole(count, rows, WIDTH),
                whole(depth, WIDTH),
                whole(depth, WIDTH),
                whole(1, HEAD_DIM),
            ],
            out_specs=whole(sends, 2 * part, WIDTH),
            scratch_shapes=[pltpu.VMEM((groups, 2 * part, WIDTH), f32)],
        ),
        out_shape=jax.ShapeDtypeStruct((sends, 2 * part, WIDTH), bf16),
        compiler_params=pltpu.CompilerParams(vmem_limit_bytes=VMEM_LIMIT),
        cost_estimate=pl.CostEstimate(
            flops=4 * rows * depth * WIDTH, bytes_accessed=4 << 20, transcendentals=0
        ),
        name="project_hot",
    )(asked, order, same, other, w_key, w_value, gain)


def q_kernel(tok, wq, gain, out):
    values = jnp.dot(tok[...], wq[...], preferred_element_type=f32)
    for h in range(2):
        lanes = slice(h * HEAD_DIM, (h + 1) * HEAD_DIM)
        out[:, lanes] = head_norm(values[:, lanes], gain[...])


def project_q(tokens, w_query, gain):
    length, depth = tokens.shape
    tile = 512
    return pl.pallas_call(
        q_kernel,
        grid=(length // tile,),
        in_specs=[
            pl.BlockSpec((tile, depth), lambda i: (i, 0)),
            pl.BlockSpec((depth, WIDTH), lambda i: (0, 0)),
            pl.BlockSpec((1, HEAD_DIM), lambda i: (0, 0)),
        ],
        out_specs=pl.BlockSpec((tile, WIDTH), lambda i: (i, 0)),
        out_shape=jax.ShapeDtypeStruct((length, WIDTH), bf16),
        compiler_params=pltpu.CompilerParams(vmem_limit_bytes=VMEM_LIMIT),
        cost_estimate=pl.CostEstimate(
            flops=2 * length * depth * WIDTH, bytes_accessed=2 * length * depth, transcendentals=0
        ),
        name="project_q",
    )(tokens, w_query, gain)


def attention_kernel(at, q, mask, local, near, hot, out, table, sems):
    step = pl.program_id(0)

    @pl.when(step == 0)
    def _():
        copies = []
        start = 0
        for n, part in enumerate((local, near, hot)):
            span = table.at[pl.ds(start, part.shape[0])]
            copies.append(pltpu.make_async_copy(part, span, sems.at[n]))
            start += part.shape[0]
        for copy in copies:
            copy.start()
        for copy in copies:
            copy.wait()

    blocks = q.shape[0] // BLOCK
    slots = mask.shape[1] // BLOCK

    def one(i, carry):
        row = pl.multiple_of(i * BLOCK, BLOCK)
        rows = q[pl.ds(row, BLOCK), :]
        blank = jnp.zeros((BLOCK, HEAD_DIM), bf16)
        both = jnp.concatenate(
            [
                jnp.concatenate([rows[:, :HEAD_DIM], blank], axis=1),
                jnp.concatenate([blank, rows[:, HEAD_DIM:]], axis=1),
            ],
            axis=0,
        )
        base = (step * blocks + i) * slots
        picks = [at[base + j] for j in range(slots)]
        keys = jnp.concatenate([table[p, 0] for p in picks], axis=0)
        logits = lax.dot_general(both, keys, (((1,), (1,)), ((), ())), preferred_element_type=f32)
        weights = jnp.exp2(logits) * mask[pl.ds(i, 1), :]
        totals = jnp.sum(weights, axis=-1, keepdims=True)
        values = jnp.concatenate([table[p, 1] for p in picks], axis=0)
        sums = jnp.dot(weights.astype(bf16), values, preferred_element_type=f32)
        scale = 1.0 / totals
        out[pl.ds(row, BLOCK), :HEAD_DIM] = (
            sums[:BLOCK, :HEAD_DIM] * scale[:BLOCK]
        ).astype(bf16)
        out[pl.ds(row, BLOCK), HEAD_DIM:] = (
            sums[BLOCK:, HEAD_DIM:] * scale[BLOCK:]
        ).astype(bf16)
        return carry

    lax.fori_loop(0, blocks, one, 0, unroll=4)


def attend(at, queries, mask, local, near, hot):
    length = queries.shape[0]
    slots = mask.shape[1] // BLOCK
    per = 16
    steps = length // (per * BLOCK)
    return pl.pallas_call(
        attention_kernel,
        grid_spec=pltpu.PrefetchScalarGridSpec(
            num_scalar_prefetch=1,
            grid=(steps,),
            in_specs=[
                pl.BlockSpec((per * BLOCK, WIDTH), lambda i, at: (i, 0)),
                pl.BlockSpec((per, slots * BLOCK), lambda i, at: (i, 0)),
                pl.BlockSpec(memory_space=pl.ANY),
                pl.BlockSpec(memory_space=pl.ANY),
                pl.BlockSpec(memory_space=pl.ANY),
            ],
            out_specs=pl.BlockSpec((per * BLOCK, WIDTH), lambda i, at: (i, 0)),
            scratch_shapes=[
                pltpu.VMEM(
                    (local.shape[0] + near.shape[0] + hot.shape[0],) + local.shape[1:], bf16
                ),
                pltpu.SemaphoreType.DMA((3,)),
            ],
        ),
        out_shape=jax.ShapeDtypeStruct((length, WIDTH), bf16),
        compiler_params=pltpu.CompilerParams(vmem_limit_bytes=VMEM_LIMIT),
        cost_estimate=pl.CostEstimate(
            flops=8 * length * WIDTH * slots * BLOCK, bytes_accessed=16 << 20, transcendentals=0
        ),
        name="attend",
    )(at, queries, mask, local, near, hot)


def out_kernel(order, pieces, w_same, w_other, gain, out, acc):
    k = pl.program_id(0)
    half = pl.num_programs(0) // 2

    @pl.when(k == 0)
    def _():
        acc[...] = jnp.dot(pieces[0], w_same[0], preferred_element_type=f32)

    @pl.when((k > 0) & (k < half))
    def _():
        acc[...] += jnp.dot(pieces[0], w_same[0], preferred_element_type=f32)

    @pl.when((k >= half) & (k < 2 * half - 1))
    def _():
        acc[...] += jnp.dot(pieces[0], w_other[0], preferred_element_type=f32)

    @pl.when(k == 2 * half - 1)
    def _():
        mixed = acc[...] + jnp.dot(pieces[0], w_other[0], preferred_element_type=f32)
        width = mixed.shape[1]
        squares = jnp.sum(mixed * mixed, axis=-1, keepdims=True)
        factor = lax.rsqrt(squares * (1.0 / width) + norm_eps)
        normed = (mixed * factor * gain[...]).astype(bf16)
        for j in range(out.shape[0]):
            out[j] = normed[:, j * WIDTH : (j + 1) * WIDTH]


def project_out(order, pieces, w_same, w_other, gain):
    count, rows, _ = pieces.shape
    half = count // 2
    width = w_same.shape[2]
    return pl.pallas_call(
        out_kernel,
        grid_spec=pltpu.PrefetchScalarGridSpec(
            num_scalar_prefetch=1,
            grid=(count,),
            in_specs=[
                pl.BlockSpec((1, rows, WIDTH), lambda k, order: (order[k], 0, 0)),
                pl.BlockSpec((1, WIDTH, width), lambda k, order: (jnp.minimum(k, half - 1), 0, 0)),
                pl.BlockSpec((1, WIDTH, width), lambda k, order: (jnp.maximum(k - half, 0), 0, 0)),
                pl.BlockSpec((1, width), lambda k, order: (0, 0)),
            ],
            out_specs=pl.BlockSpec((count, rows, WIDTH), lambda k, order: (0, 0, 0)),
            scratch_shapes=[pltpu.VMEM((rows, width), f32)],
        ),
        out_shape=jax.ShapeDtypeStruct((count, rows, WIDTH), bf16),
        compiler_params=pltpu.CompilerParams(vmem_limit_bytes=VMEM_LIMIT),
        cost_estimate=pl.CostEstimate(
            flops=2 * rows * width * width, bytes_accessed=12 << 20, transcendentals=0
        ),
        name="project_out",
    )(order, pieces, w_same, w_other, gain)


def exchange(pieces, axes):
    return lax.all_to_all(pieces, axes, split_axis=0, concat_axis=0, tiled=True)


def along_y(piece, shift):
    ring = lax.axis_size(TP[0])
    return lax.ppermute(piece, TP[0], [(i, (i + shift) % ring) for i in range(ring)])


def both_cores(parts):
    same = jnp.stack(parts)
    return same, lax.ppermute(same, TP[1], [(0, 1), (1, 0)])


def gather_w_out(w_out):
    half = w_out.shape[0] // 2
    after = along_y(w_out, 1)
    before = along_y(w_out, -1)
    far = jnp.concatenate([along_y(after[:half], 1), along_y(before[half:], -1)], axis=0)
    return both_cores([w_out, after, before, far])


def gather_rows(rows):
    return both_cores([rows, along_y(rows, 1), along_y(rows, -1), along_y(rows, 2)])


def piece_order():
    ring = lax.axis_size(TP[0])
    y = lax.axis_index(TP[0])
    c = lax.axis_index(TP[1])
    rows = jnp.stack([y, (y + ring - 1) % ring, (y + 1) % ring, (y + 2) % ring])
    return jnp.concatenate([2 * rows + c, 2 * rows + 1 - c]).astype(jnp.int32)


def local(tokens, w_query, w_key, w_value, w_out, query_gain, key_gain, out_gain, chosen):
    length, model_width = tokens.shape
    blocks_here = length // BLOCK
    devices = lax.axis_size(KV)
    position = lax.axis_index(KV)
    ranks = lax.axis_size(TP)
    part = BLOCK // devices
    key_row = key_gain[None, :]
    query_row = (query_gain * (HEAD_DIM ** (-0.5) * LOG2E))[None, :]

    columns = lax.dynamic_slice_in_dim(tokens, lax.axis_index(TP) * WIDTH, WIDTH, 1)
    shares = columns.reshape(blocks_here, devices, part, WIDTH).transpose(1, 0, 2, 3)
    shares = exchange(shares.reshape(devices, blocks_here * part, WIDTH), KV)[0]

    usable = chosen >= 0
    pick = jnp.where(usable, chosen, 0)
    owner_of = pick // blocks_here
    all_blocks = jnp.arange(devices * blocks_here, dtype=jnp.int32)
    marked = jnp.where(usable & (owner_of != position), chosen, -1)
    wanted = jnp.any(marked[:, :, None] == all_blocks[None, None, :], axis=(0, 1)).reshape(
        devices, blocks_here
    )
    rank_of = jnp.cumsum(wanted.astype(jnp.int32), axis=1) - 1
    local_ids = jnp.arange(blocks_here, dtype=jnp.int32)
    places = wanted[:, :, None] & (
        rank_of[:, :, None] == jnp.arange(HOT, dtype=jnp.int32)[None, None, :]
    )
    named = jnp.sum(jnp.where(places, local_ids[None, :, None], 0), axis=1).astype(jnp.int32)
    requests = jnp.concatenate([named, jnp.broadcast_to(named[:1], named.shape)], axis=1)
    asked = exchange(requests, KV)
    asked_near = asked[:, :REACH].reshape(-1)
    asked_hot = asked[:, HOT:].reshape(-1)

    order = piece_order()
    w_same, w_other = gather_w_out(w_out)
    rows_same, rows_other = gather_rows(shares)

    pairs = project_kv(tokens, w_key, w_value, key_row)
    sent = pairs[asked_near].reshape(devices, REACH, PAIR, BLOCK, WIDTH)
    near = exchange(sent, KV).reshape(devices * REACH, PAIR, BLOCK, WIDTH)
    sent_hot = project_hot(asked_hot, order, rows_same, rows_other, w_key, w_value, key_row)
    hot = exchange(sent_hot.reshape(devices, HOT * 2 * part, WIDTH), KV)
    hot = hot.reshape(devices, HOT, PAIR, part, WIDTH).transpose(1, 2, 0, 3, 4)
    hot = hot.reshape(HOT, PAIR, BLOCK, WIDTH)
    queries = project_q(tokens, w_query, query_row)

    flat_rank = rank_of.reshape(-1)
    slot_rank = jnp.sum(
        jnp.where(pick[:, :, None] == all_blocks[None, None, :], flat_rank[None, None, :], 0), axis=-1
    )
    near_at = blocks_here + owner_of * REACH + slot_rank
    hot_at = blocks_here + devices * REACH + slot_rank
    at = jnp.where(
        owner_of == position, pick % blocks_here, jnp.where(owner_of == 0, hot_at, near_at)
    )
    at = jnp.where(usable, at, 0).astype(jnp.int32).reshape(-1)
    mask = jnp.repeat(usable.astype(f32), BLOCK, axis=1)

    attended = attend(at, queries, mask, pairs, near, hot)
    pieces = exchange(attended.reshape(ranks, length // ranks, WIDTH), TP)
    normed = project_out(order, pieces, w_same, w_other, out_gain[None, :])
    return exchange(normed, TP).reshape(length, WIDTH)


def solution(mesh):
    split = Mesh(mesh.devices.reshape(4, 4, 4, 2), KV + TP)
    return jax.shard_map(
        local,
        mesh=split,
        in_specs=(
            P(KV, None),
            P(None, TP),
            P(None, TP),
            P(None, TP),
            P(TP, None),
            P(),
            P(),
            P(),
            P(KV, None),
        ),
        out_specs=P(KV, TP),
        check_vma=False,
    )
```

```python
import functools

import jax
import jax.numpy as jnp
from jax import lax
from jax.experimental import pallas as pl
from jax.experimental.pallas import tpu as pltpu
from jax.sharding import Mesh
from jax.sharding import PartitionSpec as P

HEAD_DIM = 128
BLOCK = 64
HOT = 8
REACH = 2
CHUNKS = 1
KV = ("kv_0", "kv_1")
TP = ("tp_0", "tp_1")
WIDTH = 256
PAIR = 2
norm_eps = 1e-06
LOG2E = 1.4426950408889634
bf16 = jnp.bfloat16
f32 = jnp.float32
VMEM_LIMIT = 60 * 1024 * 1024


def head_norm(values, gain_row):
    factor = lax.rsqrt(jnp.mean(values * values, axis=-1, keepdims=True) + norm_eps)
    return (values * factor * gain_row).astype(bf16)


def share_kernel(rank, tok, asks, out):
    rows = tok[...].astype(f32)
    devices = out.shape[0]
    part = BLOCK // devices
    small = rows.shape[0] // devices
    step = pl.program_id(0)
    for k in range(small // 16):
        parts = []
        for b in range(16 // part):
            first = (k * (16 // part) + b) * BLOCK
            parts.append(rows[first : first + BLOCK].reshape(devices, part, WIDTH))
        at = pl.ds(pl.multiple_of(step * small + k * 16, 16), 16)
        out[:, at, :] = jnp.concatenate(parts, axis=1).astype(bf16)

    @pl.when(step == 0)
    def _():
        out[:, -16:, :] = asks[...]


def token_shares(rank, tokens, asks):
    length = tokens.shape[0]
    devices = asks.shape[0]
    tile = 1024
    shape = (devices, length // devices + 16, WIDTH)
    return pl.pallas_call(
        share_kernel,
        grid_spec=pltpu.PrefetchScalarGridSpec(
            num_scalar_prefetch=1,
            grid=(length // tile,),
            in_specs=[
                pl.BlockSpec((tile, WIDTH), lambda i, rank: (i, rank[0])),
                pl.BlockSpec(asks.shape, lambda i, rank: (0, 0, 0)),
            ],
            out_specs=pl.BlockSpec(shape, lambda i, rank: (0, 0, 0)),
        ),
        out_shape=jax.ShapeDtypeStruct(shape, bf16),
        compiler_params=pltpu.CompilerParams(vmem_limit_bytes=VMEM_LIMIT),
        cost_estimate=pl.CostEstimate(flops=1 << 20, bytes_accessed=4 << 20, transcendentals=0),
        name="token_shares",
    )(rank, tokens, asks)


def qkv_kernel(tok, wq, wk, wv, q_gain, k_gain, queries, pairs, weights, sems):
    @pl.when(pl.program_id(0) == 0)
    def _():
        copies = []
        for n, w in enumerate((wq, wk, wv)):
            span = weights.at[:, pl.ds(n * WIDTH, WIDTH)]
            copies.append(pltpu.make_async_copy(w, span, sems.at[n]))
        for copy in copies:
            copy.start()
        for copy in copies:
            copy.wait()

    sums = jnp.dot(tok[...], weights[...], preferred_element_type=f32)
    blocks = pairs.shape[0]
    for h in range(2):
        lanes = slice(h * HEAD_DIM, (h + 1) * HEAD_DIM)
        queries[:, lanes] = head_norm(sums[:, lanes], q_gain[...])
        key_lanes = slice(WIDTH + h * HEAD_DIM, WIDTH + (h + 1) * HEAD_DIM)
        normed = head_norm(sums[:, key_lanes], k_gain[...])
        pairs[:, 0, :, lanes] = normed.reshape(blocks, BLOCK, HEAD_DIM)
    pairs[:, 1, :, :] = sums[:, 2 * WIDTH :].astype(bf16).reshape(blocks, BLOCK, WIDTH)


def project_qkv(tokens, w_query, w_key, w_value, q_gain, k_gain):
    length, depth = tokens.shape
    tile = 512
    blocks = tile // BLOCK
    anywhere = pl.BlockSpec(memory_space=pl.ANY)
    gain_spec = pl.BlockSpec((1, HEAD_DIM), lambda i: (0, 0))
    return pl.pallas_call(
        qkv_kernel,
        grid=(length // tile,),
        in_specs=[
            pl.BlockSpec((tile, depth), lambda i: (i, 0)),
            anywhere,
            anywhere,
            anywhere,
            gain_spec,
            gain_spec,
        ],
        out_specs=[
            pl.BlockSpec((tile, WIDTH), lambda i: (i, 0)),
            pl.BlockSpec((blocks, PAIR, BLOCK, WIDTH), lambda i: (i, 0, 0, 0)),
        ],
        out_shape=[
            jax.ShapeDtypeStruct((length, WIDTH), bf16),
            jax.ShapeDtypeStruct((length // BLOCK, PAIR, BLOCK, WIDTH), bf16),
        ],
        scratch_shapes=[pltpu.VMEM((depth, 3 * WIDTH), bf16), pltpu.SemaphoreType.DMA((3,))],
        compiler_params=pltpu.CompilerParams(vmem_limit_bytes=VMEM_LIMIT),
        cost_estimate=pl.CostEstimate(
            flops=6 * length * depth * WIDTH, bytes_accessed=2 * length * depth, transcendentals=0
        ),
        name="project_qkv",
    )(tokens, w_query, w_key, w_value, q_gain, k_gain)


def hot_kernel(asked, order, same, other, wk, wv, gain, out, keep):
    keys = jnp.zeros((same.shape[1], WIDTH), f32)
    vals = jnp.zeros((same.shape[1], WIDTH), f32)
    count = same.shape[0]
    for k in range(2 * count):
        rows = same[k] if k < count else other[k - count]
        span = pl.ds(pl.multiple_of(order[k] * WIDTH, WIDTH), WIDTH)
        keys += jnp.dot(rows, wk[span, :], preferred_element_type=f32)
        vals += jnp.dot(rows, wv[span, :], preferred_element_type=f32)
    part = out.shape[1] // 2
    groups = keep.shape[0]
    for h in range(2):
        lanes = slice(h * HEAD_DIM, (h + 1) * HEAD_DIM)
        x = keys[:, lanes]
        factor = lax.rsqrt(jnp.mean(x * x, axis=-1, keepdims=True) + norm_eps)
        keep[:, :part, lanes] = (x * factor * gain[...]).reshape(groups, part, HEAD_DIM)
    keep[:, part:, :] = vals.reshape(groups, part, WIDTH)

    def one(m, carry):
        out[m] = keep[asked[m]].astype(bf16)
        return carry

    lax.fori_loop(0, out.shape[0], one, 0, unroll=8)


def project_hot(asked, order, same, other, w_key, w_value, gain):
    count, rows, _ = same.shape
    groups = 64
    part = rows // groups
    depth = w_key.shape[0]
    sends = asked.shape[0]
    whole = lambda *shape: pl.BlockSpec(shape, lambda i, a, o: (0,) * len(shape))
    return pl.pallas_call(
        hot_kernel,
        grid_spec=pltpu.PrefetchScalarGridSpec(
            num_scalar_prefetch=2,
            grid=(1,),
            in_specs=[
                whole(count, rows, WIDTH),
                whole(count, rows, WIDTH),
                whole(depth, WIDTH),
                whole(depth, WIDTH),
                whole(1, HEAD_DIM),
            ],
            out_specs=whole(sends, 2 * part, WIDTH),
            scratch_shapes=[pltpu.VMEM((groups, 2 * part, WIDTH), f32)],
        ),
        out_shape=jax.ShapeDtypeStruct((sends, 2 * part, WIDTH), bf16),
        compiler_params=pltpu.CompilerParams(vmem_limit_bytes=VMEM_LIMIT),
        cost_estimate=pl.CostEstimate(
            flops=4 * rows * depth * WIDTH, bytes_accessed=4 << 20, transcendentals=0
        ),
        name="project_hot",
    )(asked, order, same, other, w_key, w_value, gain)


def attention_kernel(first, at, q, mask, local, near, hot, out, table, sems):
    step = pl.program_id(0)

    @pl.when(step == 0)
    def _():
        copies = []
        start = 0
        for n, part in enumerate((local, near, hot)):
            span = table.at[pl.ds(start, part.shape[0])]
            copies.append(pltpu.make_async_copy(part, span, sems.at[n]))
            start += part.shape[0]
        for copy in copies:
            copy.start()
        for copy in copies:
            copy.wait()

    blocks = q.shape[0] // BLOCK
    slots = mask.shape[1] // BLOCK

    def one(i, carry):
        row = pl.multiple_of(i * BLOCK, BLOCK)
        rows = q[pl.ds(row, BLOCK), :]
        blank = jnp.zeros((BLOCK, HEAD_DIM), bf16)
        both = jnp.concatenate(
            [
                jnp.concatenate([rows[:, :HEAD_DIM], blank], axis=1),
                jnp.concatenate([blank, rows[:, HEAD_DIM:]], axis=1),
            ],
            axis=0,
        )
        base = (first * blocks + step * blocks + i) * slots
        picks = [at[base + j] for j in range(slots)]
        keys = jnp.concatenate([table[p, 0] for p in picks], axis=0)
        logits = lax.dot_general(both, keys, (((1,), (1,)), ((), ())), preferred_element_type=f32)
        weights = jnp.exp2(logits) * mask[pl.ds(i, 1), :]
        totals = jnp.sum(weights, axis=-1, keepdims=True)
        values = jnp.concatenate([table[p, 1] for p in picks], axis=0)
        sums = jnp.dot(weights.astype(bf16), values, preferred_element_type=f32)
        scale = 1.0 / totals
        out[pl.ds(row, BLOCK), :HEAD_DIM] = (
            sums[:BLOCK, :HEAD_DIM] * scale[:BLOCK]
        ).astype(bf16)
        out[pl.ds(row, BLOCK), HEAD_DIM:] = (
            sums[BLOCK:, HEAD_DIM:] * scale[BLOCK:]
        ).astype(bf16)
        return carry

    lax.fori_loop(0, blocks, one, 0, unroll=4)


def attend(chunk, chunks, at, queries, mask, local, near, hot):
    length = queries.shape[0] // chunks
    slots = mask.shape[1] // BLOCK
    per = 16
    steps = length // (per * BLOCK)
    first = chunk * steps
    return pl.pallas_call(
        functools.partial(attention_kernel, first),
        grid_spec=pltpu.PrefetchScalarGridSpec(
            num_scalar_prefetch=1,
            grid=(steps,),
            in_specs=[
                pl.BlockSpec((per * BLOCK, WIDTH), lambda i, at: (i + first, 0)),
                pl.BlockSpec((per, slots * BLOCK), lambda i, at: (i + first, 0)),
                pl.BlockSpec(memory_space=pl.ANY),
                pl.BlockSpec(memory_space=pl.ANY),
                pl.BlockSpec(memory_space=pl.ANY),
            ],
            out_specs=pl.BlockSpec((per * BLOCK, WIDTH), lambda i, at: (i, 0)),
            scratch_shapes=[
                pltpu.VMEM(
                    (local.shape[0] + near.shape[0] + hot.shape[0],) + local.shape[1:], bf16
                ),
                pltpu.SemaphoreType.DMA((3,)),
            ],
        ),
        out_shape=jax.ShapeDtypeStruct((length, WIDTH), bf16),
        compiler_params=pltpu.CompilerParams(vmem_limit_bytes=VMEM_LIMIT),
        cost_estimate=pl.CostEstimate(
            flops=8 * length * WIDTH * slots * BLOCK, bytes_accessed=16 << 20, transcendentals=0
        ),
        name="attend",
    )(at, queries, mask, local, near, hot)


def out_kernel(order, pieces, w_same, w_other, gain, out, acc):
    k = pl.program_id(0)
    half = pl.num_programs(0) // 2

    @pl.when(k == 0)
    def _():
        acc[...] = jnp.dot(pieces[0], w_same[0], preferred_element_type=f32)

    @pl.when((k > 0) & (k < half))
    def _():
        acc[...] += jnp.dot(pieces[0], w_same[0], preferred_element_type=f32)

    @pl.when((k >= half) & (k < 2 * half - 1))
    def _():
        acc[...] += jnp.dot(pieces[0], w_other[0], preferred_element_type=f32)

    @pl.when(k == 2 * half - 1)
    def _():
        mixed = acc[...] + jnp.dot(pieces[0], w_other[0], preferred_element_type=f32)
        width = mixed.shape[1]
        squares = jnp.sum(mixed * mixed, axis=-1, keepdims=True)
        factor = lax.rsqrt(squares * (1.0 / width) + norm_eps)
        normed = (mixed * factor * gain[...]).astype(bf16)
        for j in range(out.shape[0]):
            out[j] = normed[:, j * WIDTH : (j + 1) * WIDTH]


def project_out(order, pieces, w_same, w_other, gain):
    count, rows, _ = pieces.shape
    half = count // 2
    width = w_same.shape[2]
    return pl.pallas_call(
        out_kernel,
        grid_spec=pltpu.PrefetchScalarGridSpec(
            num_scalar_prefetch=1,
            grid=(count,),
            in_specs=[
                pl.BlockSpec((1, rows, WIDTH), lambda k, order: (order[k], 0, 0)),
                pl.BlockSpec((1, WIDTH, width), lambda k, order: (jnp.minimum(k, half - 1), 0, 0)),
                pl.BlockSpec((1, WIDTH, width), lambda k, order: (jnp.maximum(k - half, 0), 0, 0)),
                pl.BlockSpec((1, width), lambda k, order: (0, 0)),
            ],
            out_specs=pl.BlockSpec((count, rows, WIDTH), lambda k, order: (0, 0, 0)),
            scratch_shapes=[pltpu.VMEM((rows, width), f32)],
        ),
        out_shape=jax.ShapeDtypeStruct((count, rows, WIDTH), bf16),
        compiler_params=pltpu.CompilerParams(vmem_limit_bytes=VMEM_LIMIT),
        cost_estimate=pl.CostEstimate(
            flops=2 * rows * width * width, bytes_accessed=12 << 20, transcendentals=0
        ),
        name="project_out",
    )(order, pieces, w_same, w_other, gain)


def exchange(pieces, axes):
    return lax.all_to_all(pieces, axes, split_axis=0, concat_axis=0, tiled=True)


def tied(*arrays):
    return lax.optimization_barrier(arrays)


def along_y(piece, shift):
    ring = lax.axis_size(TP[0])
    return lax.ppermute(piece, TP[0], [(i, (i + shift) % ring) for i in range(ring)])


def both_cores(parts):
    same = jnp.stack(parts)
    return same, lax.ppermute(same, TP[1], [(0, 1), (1, 0)])


def piece_order():
    ring = lax.axis_size(TP[0])
    y = lax.axis_index(TP[0])
    c = lax.axis_index(TP[1])
    rows = jnp.stack([y, (y + ring - 1) % ring, (y + 1) % ring, (y + 2) % ring])
    return jnp.concatenate([2 * rows + c, 2 * rows + 1 - c]).astype(jnp.int32)


def local(tokens, w_query, w_key, w_value, w_out, query_gain, key_gain, out_gain, chosen):
    length, model_width = tokens.shape
    blocks_here = length // BLOCK
    devices = lax.axis_size(KV)
    position = lax.axis_index(KV)
    ranks = lax.axis_size(TP)
    part = BLOCK // devices
    key_row = key_gain[None, :]
    query_row = (query_gain * (HEAD_DIM ** (-0.5) * LOG2E))[None, :]

    usable = chosen >= 0
    pick = jnp.where(usable, chosen, 0)
    owner_of = pick // blocks_here
    all_blocks = jnp.arange(devices * blocks_here, dtype=jnp.int32)
    marked = jnp.where(usable & (owner_of != position), chosen, -1)
    wanted = jnp.any(marked[:, :, None] == all_blocks[None, None, :], axis=(0, 1)).reshape(
        devices, blocks_here
    )
    rank_of = jnp.cumsum(wanted.astype(jnp.int32), axis=1) - 1
    local_ids = jnp.arange(blocks_here, dtype=jnp.int32)
    places = wanted[:, :, None] & (
        rank_of[:, :, None] == jnp.arange(HOT, dtype=jnp.int32)[None, None, :]
    )
    named = jnp.sum(jnp.where(places, local_ids[None, :, None], 0), axis=1).astype(jnp.int32)
    requests = jnp.concatenate([named, jnp.broadcast_to(named[:1], named.shape)], axis=1)
    asks = jnp.pad(requests.astype(bf16)[:, None, :], ((0, 0), (0, 15), (0, WIDTH - 2 * HOT)))
    rank = lax.axis_index(TP).astype(jnp.int32).reshape(1)
    arrived = exchange(token_shares(rank, tokens, asks), KV)
    shares = arrived[0, :-16]
    asked = arrived[:, -16, : 2 * HOT].astype(jnp.int32)
    asked_near = asked[:, :REACH].reshape(-1)
    asked_hot = asked[:, HOT:].reshape(-1)

    order = piece_order()
    w_after = along_y(w_out, 1)
    w_before = along_y(w_out, -1)

    queries, pairs = project_qkv(tokens, w_query, w_key, w_value, query_row, key_row)
    shares, asked_near, asked_hot, pairs = tied(shares, asked_near, asked_hot, pairs)
    parts = [along_y(shares, shift) for shift in (1, -1, 2)]
    sent = pairs[asked_near].reshape(devices, REACH, PAIR, BLOCK, WIDTH)
    sent, *parts = tied(sent, *parts)
    near = exchange(sent, KV).reshape(devices * REACH, PAIR, BLOCK, WIDTH)
    rows_same, rows_other = both_cores([shares] + parts)
    sent_hot = project_hot(asked_hot, order, rows_same, rows_other, w_key, w_value, key_row)
    w_after, w_before, near, sent_hot = tied(w_after, w_before, near, sent_hot)
    hot = exchange(sent_hot.reshape(devices, HOT * 2 * part, WIDTH), KV)
    half = w_out.shape[0] // 2
    w_far = [along_y(w_after[:half], 1), along_y(w_before[half:], -1)]
    hot = hot.reshape(devices, HOT, PAIR, part, WIDTH).transpose(1, 2, 0, 3, 4)
    hot = hot.reshape(HOT, PAIR, BLOCK, WIDTH)

    flat_rank = rank_of.reshape(-1)
    slot_rank = jnp.sum(
        jnp.where(pick[:, :, None] == all_blocks[None, None, :], flat_rank[None, None, :], 0), axis=-1
    )
    near_at = blocks_here + owner_of * REACH + slot_rank
    hot_at = blocks_here + devices * REACH + slot_rank
    at = jnp.where(
        owner_of == position, pick % blocks_here, jnp.where(owner_of == 0, hot_at, near_at)
    )
    at = jnp.where(usable, at, 0).astype(jnp.int32).reshape(-1)
    mask = jnp.repeat(usable.astype(f32), BLOCK, axis=1)

    gain_row = out_gain[None, :]
    span = length // CHUNKS
    shape = (ranks, span // ranks, WIDTH)
    attended = [attend(0, CHUNKS, at, queries, mask, pairs, near, hot)]
    tied_parts = tied(attended[0], w_after, w_before, *w_far)
    pieces = [exchange(tied_parts[0].reshape(shape), TP)]
    w_same, w_other = both_cores(
        [w_out, tied_parts[1], tied_parts[2], jnp.concatenate(tied_parts[3:], axis=0)]
    )
    for chunk in range(1, CHUNKS):
        attended.append(attend(chunk, CHUNKS, at, queries, mask, pairs, near, hot))
        pieces.append(exchange(attended[chunk].reshape(shape), TP))
    outs = []
    for chunk in range(CHUNKS):
        normed = project_out(order, pieces[chunk], w_same, w_other, gain_row)
        outs.append(exchange(normed, TP).reshape(span, WIDTH))
    return jnp.concatenate(outs, axis=0)


def solution(mesh):
    split = Mesh(mesh.devices.reshape(4, 4, 4, 2), KV + TP)
    return jax.shard_map(
        local,
        mesh=split,
        in_specs=(
            P(KV, None),
            P(None, TP),
            P(None, TP),
            P(None, TP),
            P(TP, None),
            P(),
            P(),
            P(),
            P(KV, None),
        ),
        out_specs=P(KV, TP),
        check_vma=False,
    )
```

```python
import functools

import jax
import jax.numpy as jnp
from jax import lax
from jax.experimental import pallas as pl
from jax.experimental.pallas import tpu as pltpu
from jax.sharding import Mesh
from jax.sharding import PartitionSpec as P

HEAD_DIM = 128
BLOCK = 64
HOT = 8
REACH = 2
CHUNKS = 2
KV = ("kv_0", "kv_1")
TP = ("tp_0", "tp_1")
WIDTH = 256
PAIR = 2
norm_eps = 1e-06
LOG2E = 1.4426950408889634
bf16 = jnp.bfloat16
f32 = jnp.float32
VMEM_LIMIT = 60 * 1024 * 1024


def head_norm(values, gain_row):
    factor = lax.rsqrt(jnp.mean(values * values, axis=-1, keepdims=True) + norm_eps)
    return (values * factor * gain_row).astype(bf16)


def share_kernel(rank, tok, out):
    rows = tok[...].astype(f32)
    devices = out.shape[0]
    part = BLOCK // devices
    for k in range(out.shape[1] // 16):
        parts = []
        for b in range(16 // part):
            first = (k * (16 // part) + b) * BLOCK
            parts.append(rows[first : first + BLOCK].reshape(devices, part, WIDTH))
        out[:, k * 16 : (k + 1) * 16, :] = jnp.concatenate(parts, axis=1).astype(bf16)


def token_shares(rank, tokens, devices):
    length = tokens.shape[0]
    tile = 1024
    small = tile // devices
    return pl.pallas_call(
        share_kernel,
        grid_spec=pltpu.PrefetchScalarGridSpec(
            num_scalar_prefetch=1,
            grid=(length // tile,),
            in_specs=[pl.BlockSpec((tile, WIDTH), lambda i, rank: (i, rank[0]))],
            out_specs=pl.BlockSpec((devices, small, WIDTH), lambda i, rank: (0, i, 0)),
        ),
        out_shape=jax.ShapeDtypeStruct((devices, length // devices, WIDTH), bf16),
        compiler_params=pltpu.CompilerParams(vmem_limit_bytes=VMEM_LIMIT),
        cost_estimate=pl.CostEstimate(flops=1 << 20, bytes_accessed=4 << 20, transcendentals=0),
        name="token_shares",
    )(rank, tokens)


def kv_kernel(tok, wk, wv, gain, out):
    rows = tok[...]
    keys = jnp.dot(rows, wk[...], preferred_element_type=f32)
    blocks = out.shape[0]
    for h in range(2):
        lanes = slice(h * HEAD_DIM, (h + 1) * HEAD_DIM)
        normed = head_norm(keys[:, lanes], gain[...])
        out[:, 0, :, lanes] = normed.reshape(blocks, BLOCK, HEAD_DIM)
    vals = jnp.dot(rows, wv[...], preferred_element_type=f32).astype(bf16)
    out[:, 1, :, :] = vals.reshape(blocks, BLOCK, WIDTH)


def project_kv(tokens, w_key, w_value, gain):
    length, depth = tokens.shape
    tile = 1024
    blocks = tile // BLOCK
    return pl.pallas_call(
        kv_kernel,
        grid=(length // tile,),
        in_specs=[
            pl.BlockSpec((tile, depth), lambda i: (i, 0)),
            pl.BlockSpec((depth, WIDTH), lambda i: (0, 0)),
            pl.BlockSpec((depth, WIDTH), lambda i: (0, 0)),
            pl.BlockSpec((1, HEAD_DIM), lambda i: (0, 0)),
        ],
        out_specs=pl.BlockSpec((blocks, PAIR, BLOCK, WIDTH), lambda i: (i, 0, 0, 0)),
        out_shape=jax.ShapeDtypeStruct((length // BLOCK, PAIR, BLOCK, WIDTH), bf16),
        compiler_params=pltpu.CompilerParams(vmem_limit_bytes=VMEM_LIMIT),
        cost_estimate=pl.CostEstimate(
            flops=4 * length * depth * WIDTH, bytes_accessed=2 * length * depth, transcendentals=0
        ),
        name="project_kv",
    )(tokens, w_key, w_value, gain)


def q_kernel(tok, wq, gain, out):
    values = jnp.dot(tok[...], wq[...], preferred_element_type=f32)
    for h in range(2):
        lanes = slice(h * HEAD_DIM, (h + 1) * HEAD_DIM)
        out[:, lanes] = head_norm(values[:, lanes], gain[...])


def project_q(tokens, w_query, gain):
    length, depth = tokens.shape
    tile = 1024
    return pl.pallas_call(
        q_kernel,
        grid=(length // tile,),
        in_specs=[
            pl.BlockSpec((tile, depth), lambda i: (i, 0)),
            pl.BlockSpec((depth, WIDTH), lambda i: (0, 0)),
            pl.BlockSpec((1, HEAD_DIM), lambda i: (0, 0)),
        ],
        out_specs=pl.BlockSpec((tile, WIDTH), lambda i: (i, 0)),
        out_shape=jax.ShapeDtypeStruct((length, WIDTH), bf16),
        compiler_params=pltpu.CompilerParams(vmem_limit_bytes=VMEM_LIMIT),
        cost_estimate=pl.CostEstimate(
            flops=2 * length * depth * WIDTH, bytes_accessed=2 * length * depth, transcendentals=0
        ),
        name="project_q",
    )(tokens, w_query, gain)


def hot_kernel(asked, order, same, other, wk, wv, gain, out, keep):
    keys = jnp.zeros((same.shape[1], WIDTH), f32)
    vals = jnp.zeros((same.shape[1], WIDTH), f32)
    count = same.shape[0]
    for k in range(2 * count):
        rows = same[k] if k < count else other[k - count]
        span = pl.ds(pl.multiple_of(order[k] * WIDTH, WIDTH), WIDTH)
        keys += jnp.dot(rows, wk[span, :], preferred_element_type=f32)
        vals += jnp.dot(rows, wv[span, :], preferred_element_type=f32)
    part = out.shape[1] // 2
    groups = keep.shape[0]
    for h in range(2):
        lanes = slice(h * HEAD_DIM, (h + 1) * HEAD_DIM)
        x = keys[:, lanes]
        factor = lax.rsqrt(jnp.mean(x * x, axis=-1, keepdims=True) + norm_eps)
        keep[:, :part, lanes] = (x * factor * gain[...]).reshape(groups, part, HEAD_DIM)
    keep[:, part:, :] = vals.reshape(groups, part, WIDTH)

    def one(m, carry):
        out[m] = keep[asked[m]].astype(bf16)
        return carry

    lax.fori_loop(0, out.shape[0], one, 0, unroll=8)


def project_hot(asked, order, same, other, w_key, w_value, gain):
    count, rows, _ = same.shape
    groups = 64
    part = rows // groups
    depth = w_key.shape[0]
    sends = asked.shape[0]
    whole = lambda *shape: pl.BlockSpec(shape, lambda i, a, o: (0,) * len(shape))
    return pl.pallas_call(
        hot_kernel,
        grid_spec=pltpu.PrefetchScalarGridSpec(
            num_scalar_prefetch=2,
            grid=(1,),
            in_specs=[
                whole(count, rows, WIDTH),
                whole(count, rows, WIDTH),
                whole(depth, WIDTH),
                whole(depth, WIDTH),
                whole(1, HEAD_DIM),
            ],
            out_specs=whole(sends, 2 * part, WIDTH),
            scratch_shapes=[pltpu.VMEM((groups, 2 * part, WIDTH), f32)],
        ),
        out_shape=jax.ShapeDtypeStruct((sends, 2 * part, WIDTH), bf16),
        compiler_params=pltpu.CompilerParams(vmem_limit_bytes=VMEM_LIMIT),
        cost_estimate=pl.CostEstimate(
            flops=4 * rows * depth * WIDTH, bytes_accessed=4 << 20, transcendentals=0
        ),
        name="project_hot",
    )(asked, order, same, other, w_key, w_value, gain)


def attention_kernel(first, at, q, mask, local, near, hot, out, table, sems):
    step = pl.program_id(0)

    @pl.when(step == 0)
    def _():
        copies = []
        start = 0
        for n, part in enumerate((local, near, hot)):
            span = table.at[pl.ds(start, part.shape[0])]
            copies.append(pltpu.make_async_copy(part, span, sems.at[n]))
            start += part.shape[0]
        for copy in copies:
            copy.start()
        for copy in copies:
            copy.wait()

    blocks = q.shape[0] // BLOCK
    slots = mask.shape[1] // BLOCK

    def one(i, carry):
        row = pl.multiple_of(i * BLOCK, BLOCK)
        rows = q[pl.ds(row, BLOCK), :]
        blank = jnp.zeros((BLOCK, HEAD_DIM), bf16)
        both = jnp.concatenate(
            [
                jnp.concatenate([rows[:, :HEAD_DIM], blank], axis=1),
                jnp.concatenate([blank, rows[:, HEAD_DIM:]], axis=1),
            ],
            axis=0,
        )
        base = (first * blocks + step * blocks + i) * slots
        picks = [at[base + j] for j in range(slots)]
        keys = jnp.concatenate([table[p, 0] for p in picks], axis=0)
        logits = lax.dot_general(both, keys, (((1,), (1,)), ((), ())), preferred_element_type=f32)
        weights = jnp.exp2(logits) * mask[pl.ds(i, 1), :]
        totals = jnp.sum(weights, axis=-1, keepdims=True)
        values = jnp.concatenate([table[p, 1] for p in picks], axis=0)
        sums = jnp.dot(weights.astype(bf16), values, preferred_element_type=f32)
        scale = 1.0 / totals
        out[pl.ds(row, BLOCK), :HEAD_DIM] = (
            sums[:BLOCK, :HEAD_DIM] * scale[:BLOCK]
        ).astype(bf16)
        out[pl.ds(row, BLOCK), HEAD_DIM:] = (
            sums[BLOCK:, HEAD_DIM:] * scale[BLOCK:]
        ).astype(bf16)
        return carry

    lax.fori_loop(0, blocks, one, 0, unroll=4)


def attend(chunk, chunks, at, queries, mask, local, near, hot):
    length = queries.shape[0] // chunks
    slots = mask.shape[1] // BLOCK
    per = 16
    steps = length // (per * BLOCK)
    first = chunk * steps
    return pl.pallas_call(
        functools.partial(attention_kernel, first),
        grid_spec=pltpu.PrefetchScalarGridSpec(
            num_scalar_prefetch=1,
            grid=(steps,),
            in_specs=[
                pl.BlockSpec((per * BLOCK, WIDTH), lambda i, at: (i + first, 0)),
                pl.BlockSpec((per, slots * BLOCK), lambda i, at: (i + first, 0)),
                pl.BlockSpec(memory_space=pl.ANY),
                pl.BlockSpec(memory_space=pl.ANY),
                pl.BlockSpec(memory_space=pl.ANY),
            ],
            out_specs=pl.BlockSpec((per * BLOCK, WIDTH), lambda i, at: (i, 0)),
            scratch_shapes=[
                pltpu.VMEM(
                    (local.shape[0] + near.shape[0] + hot.shape[0],) + local.shape[1:], bf16
                ),
                pltpu.SemaphoreType.DMA((3,)),
            ],
        ),
        out_shape=jax.ShapeDtypeStruct((length, WIDTH), bf16),
        compiler_params=pltpu.CompilerParams(vmem_limit_bytes=VMEM_LIMIT),
        cost_estimate=pl.CostEstimate(
            flops=8 * length * WIDTH * slots * BLOCK, bytes_accessed=16 << 20, transcendentals=0
        ),
        name="attend",
    )(at, queries, mask, local, near, hot)


def out_kernel(order, pieces, w_same, w_other, gain, out, acc):
    k = pl.program_id(0)
    half = pl.num_programs(0) // 2

    @pl.when(k == 0)
    def _():
        acc[...] = jnp.dot(pieces[0], w_same[0], preferred_element_type=f32)

    @pl.when((k > 0) & (k < half))
    def _():
        acc[...] += jnp.dot(pieces[0], w_same[0], preferred_element_type=f32)

    @pl.when((k >= half) & (k < 2 * half - 1))
    def _():
        acc[...] += jnp.dot(pieces[0], w_other[0], preferred_element_type=f32)

    @pl.when(k == 2 * half - 1)
    def _():
        mixed = acc[...] + jnp.dot(pieces[0], w_other[0], preferred_element_type=f32)
        width = mixed.shape[1]
        squares = jnp.sum(mixed * mixed, axis=-1, keepdims=True)
        factor = lax.rsqrt(squares * (1.0 / width) + norm_eps)
        normed = (mixed * factor * gain[...]).astype(bf16)
        for j in range(out.shape[0]):
            out[j] = normed[:, j * WIDTH : (j + 1) * WIDTH]


def project_out(order, pieces, w_same, w_other, gain):
    count, rows, _ = pieces.shape
    half = count // 2
    width = w_same.shape[2]
    return pl.pallas_call(
        out_kernel,
        grid_spec=pltpu.PrefetchScalarGridSpec(
            num_scalar_prefetch=1,
            grid=(count,),
            in_specs=[
                pl.BlockSpec((1, rows, WIDTH), lambda k, order: (order[k], 0, 0)),
                pl.BlockSpec((1, WIDTH, width), lambda k, order: (jnp.minimum(k, half - 1), 0, 0)),
                pl.BlockSpec((1, WIDTH, width), lambda k, order: (jnp.maximum(k - half, 0), 0, 0)),
                pl.BlockSpec((1, width), lambda k, order: (0, 0)),
            ],
            out_specs=pl.BlockSpec((count, rows, WIDTH), lambda k, order: (0, 0, 0)),
            scratch_shapes=[pltpu.VMEM((rows, width), f32)],
        ),
        out_shape=jax.ShapeDtypeStruct((count, rows, WIDTH), bf16),
        compiler_params=pltpu.CompilerParams(vmem_limit_bytes=VMEM_LIMIT),
        cost_estimate=pl.CostEstimate(
            flops=2 * rows * width * width, bytes_accessed=12 << 20, transcendentals=0
        ),
        name="project_out",
    )(order, pieces, w_same, w_other, gain)


def exchange(pieces, axes):
    return lax.all_to_all(pieces, axes, split_axis=0, concat_axis=0, tiled=True)


def tied(*arrays):
    return lax.optimization_barrier(arrays)


def along_y(piece, shift):
    ring = lax.axis_size(TP[0])
    return lax.ppermute(piece, TP[0], [(i, (i + shift) % ring) for i in range(ring)])


def both_cores(parts):
    same = jnp.stack(parts)
    return same, lax.ppermute(same, TP[1], [(0, 1), (1, 0)])


def chosen_of(options, index):
    result = options[0]
    for n, option in enumerate(options[1:], 1):
        result = jnp.where(index == n, option, result)
    return result


def piece_order():
    ring = lax.axis_size(TP[0])
    y = lax.axis_index(TP[0])
    c = lax.axis_index(TP[1])
    rows = jnp.stack([y, (y + ring - 1) % ring, (y + 1) % ring, (y + 2) % ring])
    return jnp.concatenate([2 * rows + c, 2 * rows + 1 - c]).astype(jnp.int32)


def local(tokens, w_query, w_key, w_value, w_out, query_gain, key_gain, out_gain, chosen):
    length, _ = tokens.shape
    blocks_here = length // BLOCK
    devices = lax.axis_size(KV)
    position = lax.axis_index(KV)
    ranks = lax.axis_size(TP)
    part = BLOCK // devices
    key_row = key_gain[None, :]
    query_row = (query_gain * (HEAD_DIM ** (-0.5) * LOG2E))[None, :]

    usable = chosen >= 0
    pick = jnp.where(usable, chosen, 0)
    owner_of = pick // blocks_here
    all_blocks = jnp.arange(devices * blocks_here, dtype=jnp.int32)
    marked = jnp.where(usable & (owner_of != position), chosen, -1)
    wanted = jnp.any(marked[:, :, None] == all_blocks[None, None, :], axis=(0, 1)).reshape(
        devices, blocks_here
    )
    rank_of = jnp.cumsum(wanted.astype(jnp.int32), axis=1) - 1
    local_ids = jnp.arange(blocks_here, dtype=jnp.int32)
    places = wanted[:, :, None] & (
        rank_of[:, :, None] == jnp.arange(HOT, dtype=jnp.int32)[None, None, :]
    )
    named = jnp.sum(jnp.where(places, local_ids[None, :, None], 0), axis=1).astype(jnp.int32)
    requests = jnp.concatenate([named, jnp.broadcast_to(named[:1], named.shape)], axis=1)
    asked = exchange(requests, KV)
    asked_near = asked[:, :REACH].reshape(-1)
    asked_hot = asked[:, HOT:].reshape(-1)
    order = piece_order()

    rank = lax.axis_index(TP).astype(jnp.int32).reshape(1)
    shares = token_shares(rank, tokens, devices)
    side = lax.axis_size(KV[1])
    groups = shares.reshape((devices // side, side) + shares.shape[1:])
    columns = [groups[0]] + [
        lax.ppermute(groups[n], KV, [(0, n * side)]) for n in range(1, devices // side)
    ]
    w_after = along_y(w_out, 1)
    w_before = along_y(w_out, -1)

    pairs = project_kv(tokens, w_key, w_value, key_row)
    sent = pairs[asked_near].reshape(devices, REACH, PAIR, BLOCK, WIDTH)
    sent, w_after, w_before, *columns = tied(sent, w_after, w_before, *columns)
    near = exchange(sent, KV).reshape(devices * REACH, PAIR, BLOCK, WIDTH)
    held = chosen_of(columns, lax.axis_index(KV[0]))
    starts = range(0, devices, side)
    rows = [held[0]] + [
        lax.ppermute(held[n], KV, [(z, z + n) for z in starts]) for n in range(1, side)
    ]
    half = w_out.shape[0] // 2
    w_far = [along_y(w_after[:half], 1), along_y(w_before[half:], -1)]
    again, held = tied(tokens, held)
    queries = project_q(again, w_query, query_row)
    queries, *rows = tied(queries, *rows)
    share = chosen_of(rows, lax.axis_index(KV[1]))
    parts = [share] + [along_y(share, shift) for shift in (1, -1, 2)]
    rows_same, rows_other = both_cores(parts)
    sent_hot = project_hot(asked_hot, order, rows_same, rows_other, w_key, w_value, key_row)
    near, sent_hot = tied(near, sent_hot)
    hot = exchange(sent_hot.reshape(devices, HOT * 2 * part, WIDTH), KV)
    hot = hot.reshape(devices, HOT, PAIR, part, WIDTH).transpose(1, 2, 0, 3, 4)
    hot = hot.reshape(HOT, PAIR, BLOCK, WIDTH)

    flat_rank = rank_of.reshape(-1)
    slot_rank = jnp.sum(
        jnp.where(pick[:, :, None] == all_blocks[None, None, :], flat_rank[None, None, :], 0), axis=-1
    )
    near_at = blocks_here + owner_of * REACH + slot_rank
    hot_at = blocks_here + devices * REACH + slot_rank
    at = jnp.where(
        owner_of == position, pick % blocks_here, jnp.where(owner_of == 0, hot_at, near_at)
    )
    at = jnp.where(usable, at, 0).astype(jnp.int32).reshape(-1)
    mask = jnp.repeat(usable.astype(f32), BLOCK, axis=1)

    gain_row = out_gain[None, :]
    span = length // CHUNKS
    shape = (ranks, span // ranks, WIDTH)
    attended, pieces, outs = [], [], []
    for chunk in range(CHUNKS):
        attended.append(attend(chunk, CHUNKS, at, queries, mask, pairs, near, hot))
        if chunk == 0:
            attended[0], w_after, w_before, *w_far = tied(attended[0], w_after, w_before, *w_far)
        pieces.append(exchange(attended[chunk].reshape(shape), TP))
    w_same, w_other = both_cores([w_out, w_after, w_before, jnp.concatenate(w_far, axis=0)])
    for chunk in range(CHUNKS):
        normed = project_out(order, pieces[chunk], w_same, w_other, gain_row)
        outs.append(exchange(normed, TP).reshape(span, WIDTH))
    return jnp.concatenate(outs, axis=0)


def solution(mesh):
    split = Mesh(mesh.devices.reshape(4, 4, 4, 2), KV + TP)
    return jax.shard_map(
        local,
        mesh=split,
        in_specs=(
            P(KV, None),
            P(None, TP),
            P(None, TP),
            P(None, TP),
            P(TP, None),
            P(),
            P(),
            P(),
            P(KV, None),
        ),
        out_specs=P(KV, TP),
        check_vma=False,
    )
```

```python
import jax
import jax.numpy as jnp
from jax import lax
from jax.experimental import pallas as pl
from jax.experimental.pallas import tpu as pltpu
from jax.sharding import Mesh
from jax.sharding import PartitionSpec as P

HEAD_DIM = 128
BLOCK = 64
HOT = 8
REACH = 2
KV = ("kv_0", "kv_1")
TP = ("tp_0", "tp_1")
WIDTH = 256
PAIR = 2
norm_eps = 1e-06
LOG2E = 1.4426950408889634
bf16 = jnp.bfloat16
f32 = jnp.float32
VMEM_LIMIT = 60 * 1024 * 1024


def head_norm(values, gain_row):
    factor = lax.rsqrt(jnp.mean(values * values, axis=-1, keepdims=True) + norm_eps)
    return (values * factor * gain_row).astype(bf16)


def share_kernel(rank, tok, out):
    rows = tok[...].astype(f32)
    devices = out.shape[0]
    part = BLOCK // devices
    for k in range(out.shape[1] // 16):
        parts = []
        for b in range(16 // part):
            first = (k * (16 // part) + b) * BLOCK
            parts.append(rows[first : first + BLOCK].reshape(devices, part, WIDTH))
        out[:, k * 16 : (k + 1) * 16, :] = jnp.concatenate(parts, axis=1).astype(bf16)


def token_shares(rank, tokens, devices):
    length = tokens.shape[0]
    tile = 1024
    small = tile // devices
    return pl.pallas_call(
        share_kernel,
        grid_spec=pltpu.PrefetchScalarGridSpec(
            num_scalar_prefetch=1,
            grid=(length // tile,),
            in_specs=[pl.BlockSpec((tile, WIDTH), lambda i, rank: (i, rank[0]))],
            out_specs=pl.BlockSpec((devices, small, WIDTH), lambda i, rank: (0, i, 0)),
        ),
        out_shape=jax.ShapeDtypeStruct((devices, length // devices, WIDTH), bf16),
        compiler_params=pltpu.CompilerParams(vmem_limit_bytes=VMEM_LIMIT),
        cost_estimate=pl.CostEstimate(flops=1 << 20, bytes_accessed=4 << 20, transcendentals=0),
        name="token_shares",
    )(rank, tokens)


def qkv_kernel(tok, wq, wk, wv, q_gain, k_gain, queries, pairs, weights, sems):
    @pl.when(pl.program_id(0) == 0)
    def _():
        copies = []
        for n, w in enumerate((wq, wk, wv)):
            span = weights.at[:, pl.ds(n * WIDTH, WIDTH)]
            copies.append(pltpu.make_async_copy(w, span, sems.at[n]))
        for copy in copies:
            copy.start()
        for copy in copies:
            copy.wait()

    sums = jnp.dot(tok[...], weights[...], preferred_element_type=f32)
    blocks = pairs.shape[0]
    for h in range(2):
        lanes = slice(h * HEAD_DIM, (h + 1) * HEAD_DIM)
        queries[:, lanes] = head_norm(sums[:, lanes], q_gain[...])
        key_lanes = slice(WIDTH + h * HEAD_DIM, WIDTH + (h + 1) * HEAD_DIM)
        normed = head_norm(sums[:, key_lanes], k_gain[...])
        pairs[:, 0, :, lanes] = normed.reshape(blocks, BLOCK, HEAD_DIM)
    pairs[:, 1, :, :] = sums[:, 2 * WIDTH :].astype(bf16).reshape(blocks, BLOCK, WIDTH)


def project_qkv(tokens, w_query, w_key, w_value, q_gain, k_gain):
    length, depth = tokens.shape
    tile = 512
    blocks = tile // BLOCK
    anywhere = pl.BlockSpec(memory_space=pl.ANY)
    gain_spec = pl.BlockSpec((1, HEAD_DIM), lambda i: (0, 0))
    return pl.pallas_call(
        qkv_kernel,
        grid=(length // tile,),
        in_specs=[
            pl.BlockSpec((tile, depth), lambda i: (i, 0)),
            anywhere,
            anywhere,
            anywhere,
            gain_spec,
            gain_spec,
        ],
        out_specs=[
            pl.BlockSpec((tile, WIDTH), lambda i: (i, 0)),
            pl.BlockSpec((blocks, PAIR, BLOCK, WIDTH), lambda i: (i, 0, 0, 0)),
        ],
        out_shape=[
            jax.ShapeDtypeStruct((length, WIDTH), bf16),
            jax.ShapeDtypeStruct((length // BLOCK, PAIR, BLOCK, WIDTH), bf16),
        ],
        scratch_shapes=[pltpu.VMEM((depth, 3 * WIDTH), bf16), pltpu.SemaphoreType.DMA((3,))],
        compiler_params=pltpu.CompilerParams(vmem_limit_bytes=VMEM_LIMIT),
        cost_estimate=pl.CostEstimate(
            flops=6 * length * depth * WIDTH, bytes_accessed=2 * length * depth, transcendentals=0
        ),
        name="project_qkv",
    )(tokens, w_query, w_key, w_value, q_gain, k_gain)


def hot_kernel(asked, order, same, other, wk, wv, gain, out, keep):
    keys = jnp.zeros((same.shape[1], WIDTH), f32)
    vals = jnp.zeros((same.shape[1], WIDTH), f32)
    count = same.shape[0]
    for k in range(2 * count):
        rows = same[k] if k < count else other[k - count]
        span = pl.ds(pl.multiple_of(order[k] * WIDTH, WIDTH), WIDTH)
        keys += jnp.dot(rows, wk[span, :], preferred_element_type=f32)
        vals += jnp.dot(rows, wv[span, :], preferred_element_type=f32)
    part = out.shape[1] // 2
    groups = keep.shape[0]
    for h in range(2):
        lanes = slice(h * HEAD_DIM, (h + 1) * HEAD_DIM)
        x = keys[:, lanes]
        factor = lax.rsqrt(jnp.mean(x * x, axis=-1, keepdims=True) + norm_eps)
        keep[:, :part, lanes] = (x * factor * gain[...]).reshape(groups, part, HEAD_DIM)
    keep[:, part:, :] = vals.reshape(groups, part, WIDTH)

    def one(m, carry):
        out[m] = keep[asked[m]].astype(bf16)
        return carry

    lax.fori_loop(0, out.shape[0], one, 0, unroll=8)


def project_hot(asked, order, same, other, w_key, w_value, gain):
    count, rows, _ = same.shape
    groups = 64
    part = rows // groups
    depth = w_key.shape[0]
    sends = asked.shape[0]
    whole = lambda *shape: pl.BlockSpec(shape, lambda i, a, o: (0,) * len(shape))
    return pl.pallas_call(
        hot_kernel,
        grid_spec=pltpu.PrefetchScalarGridSpec(
            num_scalar_prefetch=2,
            grid=(1,),
            in_specs=[
                whole(count, rows, WIDTH),
                whole(count, rows, WIDTH),
                whole(depth, WIDTH),
                whole(depth, WIDTH),
                whole(1, HEAD_DIM),
            ],
            out_specs=whole(sends, 2 * part, WIDTH),
            scratch_shapes=[pltpu.VMEM((groups, 2 * part, WIDTH), f32)],
        ),
        out_shape=jax.ShapeDtypeStruct((sends, 2 * part, WIDTH), bf16),
        compiler_params=pltpu.CompilerParams(vmem_limit_bytes=VMEM_LIMIT),
        cost_estimate=pl.CostEstimate(
            flops=4 * rows * depth * WIDTH, bytes_accessed=4 << 20, transcendentals=0
        ),
        name="project_hot",
    )(asked, order, same, other, w_key, w_value, gain)


def attention_kernel(at, where, q, mask, local, near, hot, out, table, sems):
    copies = []
    start = 0
    for n, part in enumerate((local, near, hot)):
        span = table.at[pl.ds(start, part.shape[0])]
        copies.append(pltpu.make_async_copy(part, span, sems.at[n]))
        start += part.shape[0]
    for copy in copies:
        copy.start()
    for copy in copies:
        copy.wait()

    count, rows_piece, _ = out.shape
    blocks = rows_piece // BLOCK
    slots = mask.shape[1] // BLOCK
    first = where[count]

    def one(n, carry):
        piece = where[n // blocks]
        inner = n % blocks
        block = piece * blocks + inner
        row = pl.multiple_of(block * BLOCK, BLOCK)
        to = pl.multiple_of(inner * BLOCK, BLOCK)
        rows = q[pl.ds(row, BLOCK), :]
        blank = jnp.zeros((BLOCK, HEAD_DIM), bf16)
        both = jnp.concatenate(
            [
                jnp.concatenate([rows[:, :HEAD_DIM], blank], axis=1),
                jnp.concatenate([blank, rows[:, HEAD_DIM:]], axis=1),
            ],
            axis=0,
        )
        base = (first + block) * slots
        picks = [at[base + j] for j in range(slots)]
        keys = jnp.concatenate([table[p, 0] for p in picks], axis=0)
        logits = lax.dot_general(both, keys, (((1,), (1,)), ((), ())), preferred_element_type=f32)
        weights = jnp.exp2(logits) * mask[pl.ds(block, 1), :]
        totals = jnp.sum(weights, axis=-1, keepdims=True)
        values = jnp.concatenate([table[p, 1] for p in picks], axis=0)
        sums = jnp.dot(weights.astype(bf16), values, preferred_element_type=f32)
        scale = 1.0 / totals
        out[n // blocks, pl.ds(to, BLOCK), :HEAD_DIM] = (
            sums[:BLOCK, :HEAD_DIM] * scale[:BLOCK]
        ).astype(bf16)
        out[n // blocks, pl.ds(to, BLOCK), HEAD_DIM:] = (
            sums[BLOCK:, HEAD_DIM:] * scale[BLOCK:]
        ).astype(bf16)
        return carry

    lax.fori_loop(0, count * blocks, one, 0, unroll=4)


def attend(chunk, chunks, ranks, at, where, queries, mask, local, near, hot):
    length = queries.shape[0] // chunks
    slots = mask.shape[1] // BLOCK
    blocks = length // BLOCK
    first = jnp.full((1,), chunk * blocks, jnp.int32)
    where = jnp.concatenate([where, first])
    anywhere = pl.BlockSpec(memory_space=pl.ANY)
    return pl.pallas_call(
        attention_kernel,
        grid_spec=pltpu.PrefetchScalarGridSpec(
            num_scalar_prefetch=2,
            grid=(1,),
            in_specs=[
                pl.BlockSpec((length, WIDTH), lambda i, at, where: (chunk, 0)),
                pl.BlockSpec((blocks, slots * BLOCK), lambda i, at, where: (chunk, 0)),
                anywhere,
                anywhere,
                anywhere,
            ],
            out_specs=pl.BlockSpec((ranks, length // ranks, WIDTH), lambda i, at, where: (0, 0, 0)),
            scratch_shapes=[
                pltpu.VMEM(
                    (local.shape[0] + near.shape[0] + hot.shape[0],) + local.shape[1:], bf16
                ),
                pltpu.SemaphoreType.DMA((3,)),
            ],
        ),
        out_shape=jax.ShapeDtypeStruct((ranks, length // ranks, WIDTH), bf16),
        compiler_params=pltpu.CompilerParams(vmem_limit_bytes=VMEM_LIMIT),
        cost_estimate=pl.CostEstimate(
            flops=8 * length * WIDTH * slots * BLOCK, bytes_accessed=16 << 20, transcendentals=0
        ),
        name="attend",
    )(at, where, queries, mask, local, near, hot)


def out_kernel(order, slot, pieces, w_same, w_other, gain, out, mixed, squares):
    n = pl.program_id(0)
    count = pieces.shape[0]
    half = count // 2
    rows = jnp.concatenate([pieces[order[k]] for k in range(count)], axis=1)
    weight = jnp.concatenate(
        [w_same[k] for k in range(half)] + [w_other[k] for k in range(half)], axis=0
    )
    sums = jnp.dot(rows, weight, preferred_element_type=f32)
    mixed[n] = sums
    tile = sums.shape[1]
    part = sum(sums[:, i : i + 128] * sums[:, i : i + 128] for i in range(0, tile, 128))

    @pl.when(n == 0)
    def _():
        squares[...] = part

    @pl.when(n > 0)
    def _():
        squares[...] += part

    @pl.when(n == pl.num_programs(0) - 1)
    def _():
        total = jnp.sum(squares[...], axis=-1, keepdims=True)
        factor = lax.rsqrt(total * (1.0 / (count * WIDTH)) + norm_eps)
        per = tile // WIDTH
        for j in range(count):
            lanes = slice((j % per) * WIDTH, (j % per + 1) * WIDTH)
            gains = gain[:, j * WIDTH : (j + 1) * WIDTH]
            out[slot[j]] = (mixed[j // per, :, lanes] * factor * gains).astype(bf16)


def project_out(order, slot, pieces, w_same, w_other, gain):
    count, rows, _ = pieces.shape
    half = count // 2
    width = w_same.shape[2]
    tile = 512
    return pl.pallas_call(
        out_kernel,
        grid_spec=pltpu.PrefetchScalarGridSpec(
            num_scalar_prefetch=2,
            grid=(width // tile,),
            in_specs=[
                pl.BlockSpec((count, rows, WIDTH), lambda n, order, slot: (0, 0, 0)),
                pl.BlockSpec((half, WIDTH, tile), lambda n, order, slot: (0, 0, n)),
                pl.BlockSpec((half, WIDTH, tile), lambda n, order, slot: (0, 0, n)),
                pl.BlockSpec((1, width), lambda n, order, slot: (0, 0)),
            ],
            out_specs=pl.BlockSpec((count, rows, WIDTH), lambda n, order, slot: (0, 0, 0)),
            scratch_shapes=[
                pltpu.VMEM((width // tile, rows, tile), f32),
                pltpu.VMEM((rows, 128), f32),
            ],
        ),
        out_shape=jax.ShapeDtypeStruct((count, rows, WIDTH), bf16),
        compiler_params=pltpu.CompilerParams(vmem_limit_bytes=VMEM_LIMIT),
        cost_estimate=pl.CostEstimate(
            flops=2 * rows * width * width, bytes_accessed=12 << 20, transcendentals=0
        ),
        name="project_out",
    )(order, slot, pieces, w_same, w_other, gain)


def place_kernel(order, whole, *rest):
    count = len(rest) - 2
    parts, out, sems = rest[:count], rest[count], rest[count + 1]
    copies = [pltpu.make_async_copy(whole, out.at[pl.ds(0, count)], sems.at[count])]
    for k in range(count):
        copies.append(pltpu.make_async_copy(parts[k], out.at[count + order[k]], sems.at[k]))
    for copy in copies:
        copy.start()
    for copy in copies:
        copy.wait()


def place(order, whole, parts):
    count = len(parts)
    shape = (2 * count,) + parts[0].shape
    anywhere = pl.BlockSpec(memory_space=pl.ANY)
    return pl.pallas_call(
        place_kernel,
        grid_spec=pltpu.PrefetchScalarGridSpec(
            num_scalar_prefetch=1,
            grid=(1,),
            in_specs=[anywhere] * (count + 1),
            out_specs=pl.BlockSpec(shape, lambda i, order: (0, 0, 0)),
            scratch_shapes=[pltpu.SemaphoreType.DMA((count + 1,))],
        ),
        out_shape=jax.ShapeDtypeStruct(shape, bf16),
        compiler_params=pltpu.CompilerParams(vmem_limit_bytes=VMEM_LIMIT),
        cost_estimate=pl.CostEstimate(flops=1 << 20, bytes_accessed=4 << 20, transcendentals=0),
        name="place",
    )(order, whole, *parts)


def exchange(pieces, axes):
    return lax.all_to_all(pieces, axes, split_axis=0, concat_axis=0, tiled=True)


def tied(*arrays):
    return lax.optimization_barrier(arrays)


def along_y(piece, shift):
    ring = lax.axis_size(TP[0])
    return lax.ppermute(piece, TP[0], [(i, (i + shift) % ring) for i in range(ring)])


def both_cores(parts):
    same = jnp.stack(parts)
    return same, lax.ppermute(same, TP[1], [(0, 1), (1, 0)])


OFFSETS = (0, -1, 1, 2)


def piece_order(sign):
    ring = lax.axis_size(TP[0])
    y = lax.axis_index(TP[0])
    c = lax.axis_index(TP[1])
    rows = jnp.stack([(y + ring + sign * d) % ring for d in OFFSETS])
    return jnp.concatenate([2 * rows + c, 2 * rows + 1 - c]).astype(jnp.int32)


def send_pieces(pieces):
    ring = lax.axis_size(TP[0])
    got = []
    for k in range(2 * ring):
        step, swap = OFFSETS[k % ring], k // ring
        pairs = [
            (2 * y + c, 2 * ((y - step) % ring) + (c + swap) % 2)
            for y in range(ring)
            for c in range(2)
        ]
        got.append(lax.ppermute(pieces[k], TP, pairs) if k else pieces[0])
    return got


def local(tokens, w_query, w_key, w_value, w_out, query_gain, key_gain, out_gain, chosen):
    length, _ = tokens.shape
    blocks_here = length // BLOCK
    devices = lax.axis_size(KV)
    position = lax.axis_index(KV)
    ranks = lax.axis_size(TP)
    part = BLOCK // devices
    key_row = key_gain[None, :]
    query_row = (query_gain * (HEAD_DIM ** (-0.5) * LOG2E))[None, :]

    usable = chosen >= 0
    pick = jnp.where(usable, chosen, 0)
    owner_of = pick // blocks_here
    all_blocks = jnp.arange(devices * blocks_here, dtype=jnp.int32)
    marked = jnp.where(usable & (owner_of != position), chosen, -1)
    wanted = jnp.any(marked[:, :, None] == all_blocks[None, None, :], axis=(0, 1)).reshape(
        devices, blocks_here
    )
    rank_of = jnp.cumsum(wanted.astype(jnp.int32), axis=1) - 1
    local_ids = jnp.arange(blocks_here, dtype=jnp.int32)
    places = wanted[:, :, None] & (
        rank_of[:, :, None] == jnp.arange(HOT, dtype=jnp.int32)[None, None, :]
    )
    named = jnp.sum(jnp.where(places, local_ids[None, :, None], 0), axis=1).astype(jnp.int32)
    requests = jnp.concatenate([named, jnp.broadcast_to(named[:1], named.shape)], axis=1)
    asked = exchange(requests, KV)
    asked_near = asked[:, :REACH].reshape(-1)
    asked_hot = asked[:, HOT:].reshape(-1)
    order = piece_order(1)
    toward = piece_order(-1)
    same_order = jnp.arange(ranks, dtype=jnp.int32)
    slot_for = jnp.sum(
        jnp.where(toward[None, :] == same_order[:, None], same_order[None, :], 0), axis=1
    ).astype(jnp.int32)

    rank = lax.axis_index(TP).astype(jnp.int32).reshape(1)
    shares = exchange(token_shares(rank, tokens, devices), KV)[0]
    w_after = along_y(w_out, 1)
    w_before = along_y(w_out, -1)

    queries, pairs = project_qkv(tokens, w_query, w_key, w_value, query_row, key_row)
    sent = pairs[asked_near].reshape(devices, REACH, PAIR, BLOCK, WIDTH)
    sent, w_after, w_before, shares = tied(sent, w_after, w_before, shares)
    near = exchange(sent, KV).reshape(devices * REACH, PAIR, BLOCK, WIDTH)
    parts = [shares] + [along_y(shares, shift) for shift in (1, -1, 2)]
    rows_same, rows_other = both_cores(parts)
    half = w_out.shape[0] // 2
    w_far = [along_y(w_after[:half], 1), along_y(w_before[half:], -1)]
    flat_rank = rank_of.reshape(-1)
    slot_rank = jnp.sum(
        jnp.where(pick[:, :, None] == all_blocks[None, None, :], flat_rank[None, None, :], 0), axis=-1
    )
    near_at = blocks_here + owner_of * REACH + slot_rank
    hot_at = blocks_here + devices * REACH + slot_rank
    at = jnp.where(
        owner_of == position, pick % blocks_here, jnp.where(owner_of == 0, hot_at, near_at)
    )
    at = jnp.where(usable, at, 0).astype(jnp.int32).reshape(-1)
    mask = jnp.repeat(usable.astype(f32), BLOCK, axis=1)

    asked_hot, at, mask, slot_for, toward = tied(asked_hot, at, mask, slot_for, toward)
    sent_hot = project_hot(asked_hot, order, rows_same, rows_other, w_key, w_value, key_row)
    w_same = jnp.concatenate([w_out, w_after, w_before, *w_far], axis=0)
    w_same = w_same.reshape((ranks // 2,) + w_out.shape)
    near, sent_hot, w_same = tied(near, sent_hot, w_same)
    hot = exchange(sent_hot.reshape(devices, HOT * 2 * part, WIDTH), KV)
    w_other = lax.ppermute(w_same, TP[1], [(0, 1), (1, 0)])
    hot = hot.reshape(devices, HOT, PAIR, part, WIDTH).transpose(1, 2, 0, 3, 4)
    hot = hot.reshape(HOT, PAIR, BLOCK, WIDTH)

    gain_row = out_gain[None, :]
    hot, w_same, w_other = tied(hot, w_same, w_other)
    first = attend(0, 2, ranks, at, same_order, queries, mask, pairs, near, hot)
    first = exchange(first, TP)
    second = attend(1, 2, ranks, at, toward, queries, mask, pairs, near, hot)
    second = send_pieces(second)
    first = project_out(order, same_order, first, w_same, w_other, gain_row)
    second = jnp.stack(tied(first, *second)[1:])
    first = exchange(first, TP)
    second = project_out(same_order, slot_for, second, w_same, w_other, gain_row)
    second = send_pieces(second)
    return place(order, first, second).reshape(length, WIDTH)


def solution(mesh):
    split = Mesh(mesh.devices.reshape(4, 4, 4, 2), KV + TP)
    return jax.shard_map(
        local,
        mesh=split,
        in_specs=(
            P(KV, None),
            P(None, TP),
            P(None, TP),
            P(None, TP),
            P(TP, None),
            P(),
            P(),
            P(),
            P(KV, None),
        ),
        out_specs=P(KV, TP),
        check_vma=False,
    )
```

```python
import functools

import jax
import jax.numpy as jnp
from jax import lax
from jax.experimental import pallas as pl
from jax.experimental.pallas import tpu as pltpu
from jax.sharding import Mesh
from jax.sharding import PartitionSpec as P

HEAD_DIM = 128
BLOCK = 64
HOT = 8
REACH = 2
KV = ("kv_0", "kv_1")
TP = ("tp_0", "tp_1")
WIDTH = 256
PAIR = 2
norm_eps = 1e-06
LOG2E = 1.4426950408889634
bf16 = jnp.bfloat16
f32 = jnp.float32
VMEM_LIMIT = 60 * 1024 * 1024


def head_norm(values, gain_row):
    factor = lax.rsqrt(jnp.mean(values * values, axis=-1, keepdims=True) + norm_eps)
    return (values * factor * gain_row).astype(bf16)


def share_kernel(rank, tok, out):
    rows = tok[...].astype(f32)
    devices = out.shape[0]
    part = BLOCK // devices
    for k in range(out.shape[1] // 16):
        parts = []
        for b in range(16 // part):
            first = (k * (16 // part) + b) * BLOCK
            parts.append(rows[first : first + BLOCK].reshape(devices, part, WIDTH))
        out[:, k * 16 : (k + 1) * 16, :] = jnp.concatenate(parts, axis=1).astype(bf16)


def token_shares(rank, tokens, devices):
    length = tokens.shape[0]
    tile = 1024
    small = tile // devices
    return pl.pallas_call(
        share_kernel,
        grid_spec=pltpu.PrefetchScalarGridSpec(
            num_scalar_prefetch=1,
            grid=(length // tile,),
            in_specs=[pl.BlockSpec((tile, WIDTH), lambda i, rank: (i, rank[0]))],
            out_specs=pl.BlockSpec((devices, small, WIDTH), lambda i, rank: (0, i, 0)),
        ),
        out_shape=jax.ShapeDtypeStruct((devices, length // devices, WIDTH), bf16),
        compiler_params=pltpu.CompilerParams(vmem_limit_bytes=VMEM_LIMIT),
        cost_estimate=pl.CostEstimate(flops=1 << 20, bytes_accessed=4 << 20, transcendentals=0),
        name="token_shares",
    )(rank, tokens)


def kv_kernel(asked, tok, wk, wv, gain, pairs, sent, keep, out_sem, sent_sem):
    step = pl.program_id(0)
    steps = pl.num_programs(0)
    rows = tok[...]
    blocks = keep.shape[0] // steps
    first = pl.multiple_of(step * blocks, blocks)
    here = pl.ds(first, blocks)
    keys = jnp.dot(rows, wk[...], preferred_element_type=f32)
    for h in range(2):
        lanes = slice(h * HEAD_DIM, (h + 1) * HEAD_DIM)
        normed = head_norm(keys[:, lanes], gain[...])
        keep[here, 0, :, lanes] = normed.reshape(blocks, BLOCK, HEAD_DIM)
    vals = jnp.dot(rows, wv[...], preferred_element_type=f32).astype(bf16)
    keep[here, 1, :, :] = vals.reshape(blocks, BLOCK, WIDTH)
    pltpu.make_async_copy(keep.at[here], pairs.at[here], out_sem).start()

    @pl.when(step == steps - 1)
    def _():
        def begin(m, carry):
            pltpu.make_async_copy(keep.at[asked[m]], sent.at[m], sent_sem).start()
            return carry

        lax.fori_loop(0, sent.shape[0], begin, 0)
        pltpu.make_async_copy(keep.at[pl.ds(0, sent.shape[0])], sent, sent_sem).wait()
        pltpu.make_async_copy(keep, pairs, out_sem).wait()


def project_kv(asked, tokens, w_key, w_value, gain):
    length, depth = tokens.shape
    tile = 1024
    sends = asked.shape[0]
    shape = (PAIR, BLOCK, WIDTH)
    anywhere = pl.BlockSpec(memory_space=pl.ANY)
    return pl.pallas_call(
        kv_kernel,
        grid_spec=pltpu.PrefetchScalarGridSpec(
            num_scalar_prefetch=1,
            grid=(length // tile,),
            in_specs=[
                pl.BlockSpec((tile, depth), lambda i, asked: (i, 0)),
                pl.BlockSpec((depth, WIDTH), lambda i, asked: (0, 0)),
                pl.BlockSpec((depth, WIDTH), lambda i, asked: (0, 0)),
                pl.BlockSpec((1, HEAD_DIM), lambda i, asked: (0, 0)),
            ],
            out_specs=[anywhere, anywhere],
            scratch_shapes=[
                pltpu.VMEM((length // BLOCK,) + shape, bf16),
                pltpu.SemaphoreType.DMA,
                pltpu.SemaphoreType.DMA,
            ],
        ),
        out_shape=[
            jax.ShapeDtypeStruct((length // BLOCK,) + shape, bf16),
            jax.ShapeDtypeStruct((sends,) + shape, bf16),
        ],
        compiler_params=pltpu.CompilerParams(vmem_limit_bytes=VMEM_LIMIT),
        cost_estimate=pl.CostEstimate(
            flops=4 * length * depth * WIDTH, bytes_accessed=2 * length * depth, transcendentals=0
        ),
        name="project_kv",
    )(asked, tokens, w_key, w_value, gain)


def q_kernel(tok, wq, gain, out):
    values = jnp.dot(tok[...], wq[...], preferred_element_type=f32)
    for h in range(2):
        lanes = slice(h * HEAD_DIM, (h + 1) * HEAD_DIM)
        out[:, lanes] = head_norm(values[:, lanes], gain[...])


def project_q(tokens, w_query, gain):
    length, depth = tokens.shape
    tile = 1024
    return pl.pallas_call(
        q_kernel,
        grid=(length // tile,),
        in_specs=[
            pl.BlockSpec((tile, depth), lambda i: (i, 0)),
            pl.BlockSpec((depth, WIDTH), lambda i: (0, 0)),
            pl.BlockSpec((1, HEAD_DIM), lambda i: (0, 0)),
        ],
        out_specs=pl.BlockSpec((tile, WIDTH), lambda i: (i, 0)),
        out_shape=jax.ShapeDtypeStruct((length, WIDTH), bf16),
        compiler_params=pltpu.CompilerParams(vmem_limit_bytes=VMEM_LIMIT),
        cost_estimate=pl.CostEstimate(
            flops=2 * length * depth * WIDTH, bytes_accessed=2 * length * depth, transcendentals=0
        ),
        name="project_q",
    )(tokens, w_query, gain)


def hot_kernel(asked, order, same, other, wk, wv, gain, out, keep):
    keys = jnp.zeros((same.shape[1], WIDTH), f32)
    vals = jnp.zeros((same.shape[1], WIDTH), f32)
    count = same.shape[0]
    for k in range(2 * count):
        rows = same[k] if k < count else other[k - count]
        span = pl.ds(pl.multiple_of(order[k] * WIDTH, WIDTH), WIDTH)
        keys += jnp.dot(rows, wk[span, :], preferred_element_type=f32)
        vals += jnp.dot(rows, wv[span, :], preferred_element_type=f32)
    part = out.shape[1] // 2
    groups = keep.shape[0]
    for h in range(2):
        lanes = slice(h * HEAD_DIM, (h + 1) * HEAD_DIM)
        x = keys[:, lanes]
        factor = lax.rsqrt(jnp.mean(x * x, axis=-1, keepdims=True) + norm_eps)
        keep[:, :part, lanes] = (x * factor * gain[...]).reshape(groups, part, HEAD_DIM)
    keep[:, part:, :] = vals.reshape(groups, part, WIDTH)

    def one(m, carry):
        out[m] = keep[asked[m]].astype(bf16)
        return carry

    lax.fori_loop(0, out.shape[0], one, 0, unroll=8)


def project_hot(asked, order, same, other, w_key, w_value, gain):
    count, rows, _ = same.shape
    groups = 64
    part = rows // groups
    depth = w_key.shape[0]
    sends = asked.shape[0]
    whole = lambda *shape: pl.BlockSpec(shape, lambda i, a, o: (0,) * len(shape))
    return pl.pallas_call(
        hot_kernel,
        grid_spec=pltpu.PrefetchScalarGridSpec(
            num_scalar_prefetch=2,
            grid=(1,),
            in_specs=[
                whole(count, rows, WIDTH),
                whole(count, rows, WIDTH),
                whole(depth, WIDTH),
                whole(depth, WIDTH),
                whole(1, HEAD_DIM),
            ],
            out_specs=whole(sends, 2 * part, WIDTH),
            scratch_shapes=[pltpu.VMEM((groups, 2 * part, WIDTH), f32)],
        ),
        out_shape=jax.ShapeDtypeStruct((sends, 2 * part, WIDTH), bf16),
        compiler_params=pltpu.CompilerParams(vmem_limit_bytes=VMEM_LIMIT),
        cost_estimate=pl.CostEstimate(
            flops=4 * rows * depth * WIDTH, bytes_accessed=4 << 20, transcendentals=0
        ),
        name="project_hot",
    )(asked, order, same, other, w_key, w_value, gain)


def attention_kernel(first, at, where, q, mask, local, near, hot, *rest):
    outs, (table, sems) = rest[:-2], rest[-2:]
    copies = []
    start = 0
    for n, part in enumerate((local, near, hot)):
        span = table.at[pl.ds(start, part.shape[0])]
        copies.append(pltpu.make_async_copy(part, span, sems.at[n]))
        start += part.shape[0]
    for copy in copies:
        copy.start()
    for copy in copies:
        copy.wait()
    slots = mask.shape[1] // BLOCK
    count = where.shape[0]
    whole = len(outs) == 1
    per_piece = mask.shape[0] // count
    blank = jnp.zeros((BLOCK, HEAD_DIM), bf16)

    def load(block):
        row = pl.multiple_of(block * BLOCK, BLOCK)
        rows = q[pl.ds(row, BLOCK), :]
        both = jnp.concatenate(
            [
                jnp.concatenate([rows[:, :HEAD_DIM], blank], axis=1),
                jnp.concatenate([blank, rows[:, HEAD_DIM:]], axis=1),
            ],
            axis=0,
        )
        base = (first + block) * slots
        return both, [at[base + j] for j in range(slots)]

    def piece_of(n, put):
        items = [load(where[n] * per_piece + i) for i in range(per_piece)]
        logits = []
        for both, picks in items:
            keys = jnp.concatenate([table[p, 0] for p in picks], axis=0)
            logits.append(
                lax.dot_general(both, keys, (((1,), (1,)), ((), ())), preferred_element_type=f32)
            )
        weights = []
        for i in range(per_piece):
            block = where[n] * per_piece + i
            weights.append(jnp.exp2(logits[i]) * mask[pl.ds(block, 1), :])
        for i, (both, picks) in enumerate(items):
            values = jnp.concatenate([table[p, 1] for p in picks], axis=0)
            sums = jnp.dot(weights[i].astype(bf16), values, preferred_element_type=f32)
            scale = 1.0 / jnp.sum(weights[i], axis=-1, keepdims=True)
            to = slice(i * BLOCK, (i + 1) * BLOCK)
            put(to, slice(0, HEAD_DIM), sums[:BLOCK, :HEAD_DIM] * scale[:BLOCK])
            put(to, slice(HEAD_DIM, WIDTH), sums[BLOCK:, HEAD_DIM:] * scale[BLOCK:])

    if whole:

        def one(n, carry):
            def put(rows, lanes, value):
                outs[0][n, rows, lanes] = value.astype(bf16)

            piece_of(n, put)
            return carry

        lax.fori_loop(0, count, one, 0)
    else:
        for n in range(count):

            def put(rows, lanes, value, n=n):
                outs[n][rows, lanes] = value.astype(bf16)

            piece_of(n, put)


def whole_block(*shape):
    return pl.BlockSpec(shape, lambda i, *_: (0,) * len(shape))


def attend(chunk, chunks, split, at, where, queries, mask, local, near, hot):
    ranks = where.shape[0]
    length = queries.shape[0] // chunks
    slots = mask.shape[1] // BLOCK
    blocks = length // BLOCK
    rows = length // ranks
    anywhere = pl.BlockSpec(memory_space=pl.ANY)
    shape = (rows, WIDTH) if split else (ranks, rows, WIDTH)
    count = ranks if split else 1
    parts = (local, near, hot)
    outs = pl.pallas_call(
        functools.partial(attention_kernel, chunk * blocks),
        grid_spec=pltpu.PrefetchScalarGridSpec(
            num_scalar_prefetch=2,
            grid=(1,),
            in_specs=[
                pl.BlockSpec((length, WIDTH), lambda i, *_: (chunk, 0)),
                pl.BlockSpec((blocks, slots * BLOCK), lambda i, *_: (chunk, 0)),
                anywhere,
                anywhere,
                anywhere,
            ],
            out_specs=[whole_block(*shape)] * count,
            scratch_shapes=[
                pltpu.VMEM((sum(p.shape[0] for p in parts),) + local.shape[1:], bf16),
                pltpu.SemaphoreType.DMA((3,)),
            ],
        ),
        out_shape=[jax.ShapeDtypeStruct(shape, bf16)] * count,
        compiler_params=pltpu.CompilerParams(vmem_limit_bytes=VMEM_LIMIT),
        cost_estimate=pl.CostEstimate(
            flops=8 * length * WIDTH * slots * BLOCK, bytes_accessed=10 << 20, transcendentals=0
        ),
        name="attend",
    )(at, where, queries, mask, *parts)
    return list(outs) if split else outs[0]


def out_kernel(order, slot, *refs):
    count = order.shape[0]
    n = pl.program_id(0)
    if len(refs) > 2 * count + 4:
        pieces, refs = refs[:count], refs[count:]
    else:
        pieces, refs = [refs[0].at[order[k]] for k in range(count)], refs[1:]
    weights, gain, refs = refs[:count], refs[count], refs[count + 1 :]
    outs, (mixed, squares) = refs[:-2], refs[-2:]
    rows = jnp.concatenate([piece[...] for piece in pieces], axis=1)
    weight = jnp.concatenate([w[...] for w in weights], axis=0)
    sums = jnp.dot(rows, weight, preferred_element_type=f32)
    tile = sums.shape[1]
    mixed[2 * n] = sums[:, :WIDTH]
    mixed[2 * n + 1] = sums[:, WIDTH:]
    part = sum(sums[:, i : i + 128] * sums[:, i : i + 128] for i in range(0, tile, 128))

    @pl.when(n == 0)
    def _():
        squares[...] = part

    @pl.when(n > 0)
    def _():
        squares[...] += part

    @pl.when(n == pl.num_programs(0) - 1)
    def _():
        total = jnp.sum(squares[...], axis=-1, keepdims=True)
        factor = lax.rsqrt(total * (1.0 / (count * WIDTH)) + norm_eps)
        for k in range(count):
            value = (mixed[slot[k]] * factor * gain[slot[k]]).astype(bf16)
            if len(outs) == 1:
                outs[0][k] = value
            else:
                outs[k][...] = value


def project_out(split, order, slot, pieces, weights, gain):
    count = len(weights)
    pieces = list(pieces) if split else [pieces]
    rows = pieces[0].shape[-2]
    depth, width = weights[0].shape
    tile = 2 * WIDTH
    shape = (rows, WIDTH) if split else (count, rows, WIDTH)
    outs = pl.pallas_call(
        out_kernel,
        grid_spec=pltpu.PrefetchScalarGridSpec(
            num_scalar_prefetch=2,
            grid=(width // tile,),
            in_specs=[whole_block(*shape)] * len(pieces)
            + [pl.BlockSpec((depth, tile), lambda n, *_: (0, n))] * count
            + [whole_block(*gain.shape)],
            out_specs=[whole_block(*shape)] * len(pieces),
            scratch_shapes=[
                pltpu.VMEM((count, rows, WIDTH), f32),
                pltpu.VMEM((rows, 128), f32),
            ],
        ),
        out_shape=[jax.ShapeDtypeStruct(shape, bf16)] * len(pieces),
        compiler_params=pltpu.CompilerParams(vmem_limit_bytes=VMEM_LIMIT),
        cost_estimate=pl.CostEstimate(
            flops=2 * rows * width * width, bytes_accessed=12 << 20, transcendentals=0
        ),
        name="project_out",
    )(order, slot, *pieces, *weights, gain)
    return list(outs) if split else outs[0]


def place_kernel(order, whole, *rest):
    count = len(rest) - 2
    parts, out, sems = rest[:count], rest[count], rest[count + 1]
    copies = [pltpu.make_async_copy(whole, out.at[pl.ds(0, count)], sems.at[count])]
    for k in range(count):
        copies.append(pltpu.make_async_copy(parts[k], out.at[count + order[k]], sems.at[k]))
    for copy in copies:
        copy.start()
    for copy in copies:
        copy.wait()


def place(order, whole, parts):
    count = len(parts)
    shape = (2 * count,) + parts[0].shape
    anywhere = pl.BlockSpec(memory_space=pl.ANY)
    return pl.pallas_call(
        place_kernel,
        grid_spec=pltpu.PrefetchScalarGridSpec(
            num_scalar_prefetch=1,
            grid=(1,),
            in_specs=[anywhere] * (count + 1),
            out_specs=pl.BlockSpec(shape, lambda i, order: (0, 0, 0)),
            scratch_shapes=[pltpu.SemaphoreType.DMA((count + 1,))],
        ),
        out_shape=jax.ShapeDtypeStruct(shape, bf16),
        compiler_params=pltpu.CompilerParams(vmem_limit_bytes=8 << 20),
        cost_estimate=pl.CostEstimate(flops=1 << 20, bytes_accessed=4 << 20, transcendentals=0),
        name="place",
    )(order, whole, *parts)


def exchange(pieces, axes):
    return lax.all_to_all(pieces, axes, split_axis=0, concat_axis=0, tiled=True)


def tied(*arrays):
    return lax.optimization_barrier(arrays)


def along_y(piece, shift):
    ring = lax.axis_size(TP[0])
    return lax.ppermute(piece, TP[0], [(i, (i + shift) % ring) for i in range(ring)])


def both_cores(parts):
    same = jnp.stack(parts)
    return same, lax.ppermute(same, TP[1], [(0, 1), (1, 0)])


OFFSETS = (0, -1, 1, 2)


def piece_order(sign):
    ring = lax.axis_size(TP[0])
    y = lax.axis_index(TP[0])
    c = lax.axis_index(TP[1])
    rows = jnp.stack([(y + ring + sign * d) % ring for d in OFFSETS])
    return jnp.concatenate([2 * rows + c, 2 * rows + 1 - c]).astype(jnp.int32)


def send_pieces(pieces):
    ring = lax.axis_size(TP[0])
    got = []
    for k in range(2 * ring):
        step, swap = OFFSETS[k % ring], k // ring
        pairs = [
            (2 * y + c, 2 * ((y - step) % ring) + (c + swap) % 2)
            for y in range(ring)
            for c in range(2)
        ]
        got.append(lax.ppermute(pieces[k], TP, pairs) if k else pieces[0])
    return got


def local(tokens, w_query, w_key, w_value, w_out, query_gain, key_gain, out_gain, chosen):
    length, _ = tokens.shape
    blocks_here = length // BLOCK
    devices = lax.axis_size(KV)
    position = lax.axis_index(KV)
    ranks = lax.axis_size(TP)
    part = BLOCK // devices
    key_row = key_gain[None, :]
    query_row = (query_gain * (HEAD_DIM ** (-0.5) * LOG2E))[None, :]

    usable = chosen >= 0
    pick = jnp.where(usable, chosen, 0)
    owner_of = pick // blocks_here
    all_blocks = jnp.arange(devices * blocks_here, dtype=jnp.int32)
    marked = jnp.where(usable & (owner_of != position), chosen, -1)
    wanted = jnp.any(marked[:, :, None] == all_blocks[None, None, :], axis=(0, 1)).reshape(
        devices, blocks_here
    )
    rank_of = jnp.cumsum(wanted.astype(jnp.int32), axis=1) - 1
    local_ids = jnp.arange(blocks_here, dtype=jnp.int32)
    places = wanted[:, :, None] & (
        rank_of[:, :, None] == jnp.arange(HOT, dtype=jnp.int32)[None, None, :]
    )
    named = jnp.sum(jnp.where(places, local_ids[None, :, None], 0), axis=1).astype(jnp.int32)
    requests = jnp.concatenate([named, jnp.broadcast_to(named[:1], named.shape)], axis=1)
    asked = exchange(requests, KV)
    asked_near = asked[:, :REACH].reshape(-1)
    asked_hot = asked[:, HOT:].reshape(-1)
    order = piece_order(1)
    toward = piece_order(-1)
    same_order = jnp.arange(ranks, dtype=jnp.int32)
    rank = lax.axis_index(TP).astype(jnp.int32).reshape(1)
    shares = exchange(token_shares(rank, tokens, devices), KV)[0]
    w_after = along_y(w_out, 1)
    w_before = along_y(w_out, -1)

    pairs, sent = project_kv(asked_near, tokens, w_key, w_value, key_row)
    sent, shares, w_after, w_before = tied(sent, shares, w_after, w_before)
    sent = sent.reshape(devices, REACH, PAIR, BLOCK, WIDTH)
    near = exchange(sent, KV).reshape(devices * REACH, PAIR, BLOCK, WIDTH)
    parts = [shares] + [along_y(shares, shift) for shift in (1, -1, 2)]
    again, sent = tied(tokens, sent)
    queries = project_q(again, w_query, query_row)
    queries, *parts = tied(queries, *parts)
    rows_same, rows_other = both_cores(parts)
    sent_hot = project_hot(asked_hot, order, rows_same, rows_other, w_key, w_value, key_row)

    pick, owner_of, rank_of, usable, sent_hot, w_after = tied(
        pick, owner_of, rank_of, usable, sent_hot, w_after
    )
    flat_rank = rank_of.reshape(-1)
    slot_rank = jnp.sum(
        jnp.where(pick[:, :, None] == all_blocks[None, None, :], flat_rank[None, None, :], 0), axis=-1
    )
    near_at = blocks_here + owner_of * REACH + slot_rank
    hot_at = blocks_here + devices * REACH + slot_rank
    at = jnp.where(
        owner_of == position, pick % blocks_here, jnp.where(owner_of == 0, hot_at, near_at)
    )
    at = jnp.where(usable, at, 0).astype(jnp.int32).reshape(-1)
    mask = jnp.repeat(usable.astype(f32), BLOCK, axis=1)
    w_far = along_y(w_after, 1)

    near, sent_hot = tied(near, sent_hot)
    hot = exchange(sent_hot.reshape(devices, HOT * 2 * part, WIDTH), KV)
    w_same = [w_out, w_after, w_before, w_far]
    w_other = [lax.ppermute(w, TP[1], [(0, 1), (1, 0)]) for w in w_same]
    weights = w_same + w_other
    hot = hot.reshape(devices, HOT, PAIR, part, WIDTH).transpose(1, 2, 0, 3, 4)
    hot = hot.reshape(HOT, PAIR, BLOCK, WIDTH)

    gains = out_gain.reshape(ranks, 1, WIDTH)
    first = attend(0, 2, False, at, same_order, queries, mask, pairs, near, hot)
    first = exchange(first, TP)
    second = attend(1, 2, True, at, toward, queries, mask, pairs, near, hot)
    second = send_pieces(second)
    first = project_out(False, order, same_order, first, weights, gains)
    moved = exchange(first, TP)
    second = tied(first, *second)[1:]
    second = project_out(True, order, toward, second, weights, gains)
    second = send_pieces(second)
    return place(order, moved, second).reshape(length, WIDTH)


def solution(mesh):
    split = Mesh(mesh.devices.reshape(4, 4, 4, 2), KV + TP)
    return jax.shard_map(
        local,
        mesh=split,
        in_specs=(
            P(KV, None),
            P(None, TP),
            P(None, TP),
            P(None, TP),
            P(TP, None),
            P(),
            P(),
            P(),
            P(KV, None),
        ),
        out_specs=P(KV, TP),
        check_vma=False,
    )
```

```python
import functools

import jax
import jax.numpy as jnp
from jax import lax
from jax.experimental import pallas as pl
from jax.experimental.pallas import tpu as pltpu
from jax.sharding import Mesh
from jax.sharding import PartitionSpec as P

HEAD_DIM = 128
BLOCK = 64
HOT = 8
REACH = 2
KV = ("kv_0", "kv_1")
TP = ("tp_0", "tp_1")
WIDTH = 256
PAIR = 2
norm_eps = 1e-06
LOG2E = 1.4426950408889634
bf16 = jnp.bfloat16
f32 = jnp.float32
VMEM_LIMIT = 60 * 1024 * 1024


def head_norm(values, gain_row):
    factor = lax.rsqrt(jnp.mean(values * values, axis=-1, keepdims=True) + norm_eps)
    return (values * factor * gain_row).astype(bf16)


def share_kernel(rank, tok, asks, out):
    rows = tok[...].astype(f32)
    devices = out.shape[0]
    part = BLOCK // devices
    small = rows.shape[0] // devices
    step = pl.program_id(0)
    for k in range(small // 16):
        parts = []
        for b in range(16 // part):
            first = (k * (16 // part) + b) * BLOCK
            parts.append(rows[first : first + BLOCK].reshape(devices, part, WIDTH))
        at = pl.ds(pl.multiple_of(step * small + k * 16, 16), 16)
        out[:, at, :] = jnp.concatenate(parts, axis=1).astype(bf16)

    @pl.when(step == 0)
    def _():
        out[:, -16:, :] = asks[...]


def token_shares(rank, tokens, asks):
    length = tokens.shape[0]
    devices = asks.shape[0]
    tile = 1024
    shape = (devices, length // devices + 16, WIDTH)
    return pl.pallas_call(
        share_kernel,
        grid_spec=pltpu.PrefetchScalarGridSpec(
            num_scalar_prefetch=1,
            grid=(length // tile,),
            in_specs=[
                pl.BlockSpec((tile, WIDTH), lambda i, rank: (i, rank[0])),
                pl.BlockSpec(asks.shape, lambda i, rank: (0, 0, 0)),
            ],
            out_specs=pl.BlockSpec(shape, lambda i, rank: (0, 0, 0)),
        ),
        out_shape=jax.ShapeDtypeStruct(shape, bf16),
        compiler_params=pltpu.CompilerParams(vmem_limit_bytes=VMEM_LIMIT),
        cost_estimate=pl.CostEstimate(flops=1 << 20, bytes_accessed=4 << 20, transcendentals=0),
        name="token_shares",
    )(rank, tokens, asks)


def kv_kernel(tok, wk, wv, gain, out):
    rows = tok[...]
    keys = jnp.dot(rows, wk[...], preferred_element_type=f32)
    blocks = out.shape[0]
    for h in range(2):
        lanes = slice(h * HEAD_DIM, (h + 1) * HEAD_DIM)
        normed = head_norm(keys[:, lanes], gain[...])
        out[:, 0, :, lanes] = normed.reshape(blocks, BLOCK, HEAD_DIM)
    vals = jnp.dot(rows, wv[...], preferred_element_type=f32).astype(bf16)
    out[:, 1, :, :] = vals.reshape(blocks, BLOCK, WIDTH)


def project_kv(tokens, w_key, w_value, gain):
    length, depth = tokens.shape
    tile = 1024
    blocks = tile // BLOCK
    return pl.pallas_call(
        kv_kernel,
        grid=(length // tile,),
        in_specs=[
            pl.BlockSpec((tile, depth), lambda i: (i, 0)),
            pl.BlockSpec((depth, WIDTH), lambda i: (0, 0)),
            pl.BlockSpec((depth, WIDTH), lambda i: (0, 0)),
            pl.BlockSpec((1, HEAD_DIM), lambda i: (0, 0)),
        ],
        out_specs=pl.BlockSpec((blocks, PAIR, BLOCK, WIDTH), lambda i: (i, 0, 0, 0)),
        out_shape=jax.ShapeDtypeStruct((length // BLOCK, PAIR, BLOCK, WIDTH), bf16),
        compiler_params=pltpu.CompilerParams(vmem_limit_bytes=VMEM_LIMIT),
        cost_estimate=pl.CostEstimate(
            flops=4 * length * depth * WIDTH, bytes_accessed=2 * length * depth, transcendentals=0
        ),
        name="project_kv",
    )(tokens, w_key, w_value, gain)


def q_kernel(tok, wq, gain, out):
    values = jnp.dot(tok[...], wq[...], preferred_element_type=f32)
    for h in range(2):
        lanes = slice(h * HEAD_DIM, (h + 1) * HEAD_DIM)
        out[:, lanes] = head_norm(values[:, lanes], gain[...])


def project_q(tokens, w_query, gain):
    length, depth = tokens.shape
    tile = 1024
    return pl.pallas_call(
        q_kernel,
        grid=(length // tile,),
        in_specs=[
            pl.BlockSpec((tile, depth), lambda i: (i, 0)),
            pl.BlockSpec((depth, WIDTH), lambda i: (0, 0)),
            pl.BlockSpec((1, HEAD_DIM), lambda i: (0, 0)),
        ],
        out_specs=pl.BlockSpec((tile, WIDTH), lambda i: (i, 0)),
        out_shape=jax.ShapeDtypeStruct((length, WIDTH), bf16),
        compiler_params=pltpu.CompilerParams(vmem_limit_bytes=VMEM_LIMIT),
        cost_estimate=pl.CostEstimate(
            flops=2 * length * depth * WIDTH, bytes_accessed=2 * length * depth, transcendentals=0
        ),
        name="project_q",
    )(tokens, w_query, gain)


def send_kernel(near, asked, order, same, other, wk, wv, gain, pairs, out, keep, sems):
    devices, rows, _ = out.shape
    reach = near.shape[0] // devices
    plain = reach * PAIR * BLOCK
    copies = []
    for m in range(near.shape[0]):
        first = pl.multiple_of(near[m] * PAIR * BLOCK, PAIR * BLOCK)
        to = pl.ds((m % reach) * PAIR * BLOCK, PAIR * BLOCK)
        copies.append(
            pltpu.make_async_copy(
                pairs.at[pl.ds(first, PAIR * BLOCK)], out.at[m // reach, to], sems.at[m]
            )
        )
    for copy in copies:
        copy.start()

    keys = jnp.zeros((same.shape[1], WIDTH), f32)
    vals = jnp.zeros((same.shape[1], WIDTH), f32)
    count = same.shape[0]
    for k in range(2 * count):
        tokens = same[k] if k < count else other[k - count]
        span = pl.ds(pl.multiple_of(order[k] * WIDTH, WIDTH), WIDTH)
        keys += jnp.dot(tokens, wk[span, :], preferred_element_type=f32)
        vals += jnp.dot(tokens, wv[span, :], preferred_element_type=f32)
    groups, unit, _ = keep.shape
    part = unit // 2
    for h in range(2):
        lanes = slice(h * HEAD_DIM, (h + 1) * HEAD_DIM)
        x = keys[:, lanes]
        factor = lax.rsqrt(jnp.mean(x * x, axis=-1, keepdims=True) + norm_eps)
        keep[:, :part, lanes] = (x * factor * gain[...]).reshape(groups, part, HEAD_DIM)
    keep[:, part:, :] = vals.reshape(groups, part, WIDTH)

    twos = (rows - plain) // (2 * unit)

    def one(m, carry):
        both = jnp.concatenate([keep[asked[2 * m]], keep[asked[2 * m + 1]]], axis=0)
        at = pl.multiple_of(plain + (m % twos) * 2 * unit, 2 * unit)
        out[m // twos, pl.ds(at, 2 * unit), :] = both.astype(bf16)
        return carry

    lax.fori_loop(0, devices * twos, one, 0, unroll=4)
    for copy in copies:
        copy.wait()


def whole_block(*shape):
    return pl.BlockSpec(shape, lambda i, *_: (0,) * len(shape))


def project_sent(near, asked, order, same, other, w_key, w_value, gain, pairs, devices):
    count, rows, _ = same.shape
    groups = 64
    unit = 2 * rows // groups
    depth = w_key.shape[0]
    length = (near.shape[0] // devices) * PAIR * BLOCK + (asked.shape[0] // devices) * unit
    shape = (devices, length, WIDTH)
    return pl.pallas_call(
        send_kernel,
        grid_spec=pltpu.PrefetchScalarGridSpec(
            num_scalar_prefetch=3,
            grid=(1,),
            in_specs=[
                whole_block(count, rows, WIDTH),
                whole_block(count, rows, WIDTH),
                whole_block(depth, WIDTH),
                whole_block(depth, WIDTH),
                whole_block(1, HEAD_DIM),
                pl.BlockSpec(memory_space=pl.ANY),
            ],
            out_specs=whole_block(*shape),
            scratch_shapes=[
                pltpu.VMEM((groups, unit, WIDTH), f32),
                pltpu.SemaphoreType.DMA((near.shape[0],)),
            ],
        ),
        out_shape=jax.ShapeDtypeStruct(shape, bf16),
        compiler_params=pltpu.CompilerParams(vmem_limit_bytes=VMEM_LIMIT),
        cost_estimate=pl.CostEstimate(
            flops=4 * rows * depth * WIDTH, bytes_accessed=8 << 20, transcendentals=0
        ),
        name="project_sent",
    )(near, asked, order, same, other, w_key, w_value, gain, pairs)


def attention_kernel(first, at, where, q, mask, pairs, got, *rest):
    outs, (table, raw, sems) = rest[:-3], rest[-3:]
    devices, rows, _ = got.shape
    here = pairs.shape[0]
    hot_rows = raw.shape[1]
    plain = rows - hot_rows
    copies = [
        pltpu.make_async_copy(got.at[:, pl.ds(plain, hot_rows)], raw, sems.at[devices]),
        pltpu.make_async_copy(pairs, table.at[pl.ds(0, here)], sems.at[devices + 1]),
    ]
    for n in range(devices):
        span = table.at[pl.ds(here + n * plain, plain)]
        copies.append(pltpu.make_async_copy(got.at[n, pl.ds(0, plain)], span, sems.at[n]))
    for copy in copies:
        copy.start()
    copies[0].wait()
    part = BLOCK // devices
    for n in range(hot_rows // 16):
        both = raw[:, n * 16 : (n + 1) * 16, :].astype(f32)
        for m in range(2):
            start = here + devices * plain + (2 * n + m) * PAIR * BLOCK
            for kind in range(PAIR):
                low = m * 2 * part + kind * part
                piece = both[:, low : low + part, :].reshape(BLOCK, WIDTH).astype(bf16)
                table[start + kind * BLOCK : start + (kind + 1) * BLOCK, :] = piece
    for copy in copies[1:]:
        copy.wait()
    slots = mask.shape[1] // BLOCK
    count = where.shape[0]
    whole = len(outs) == 1
    per_piece = mask.shape[0] // count
    blank = jnp.zeros((BLOCK, HEAD_DIM), bf16)

    def load(block):
        row = pl.multiple_of(block * BLOCK, BLOCK)
        rows = q[pl.ds(row, BLOCK), :]
        both = jnp.concatenate(
            [
                jnp.concatenate([rows[:, :HEAD_DIM], blank], axis=1),
                jnp.concatenate([blank, rows[:, HEAD_DIM:]], axis=1),
            ],
            axis=0,
        )
        base = (first + block) * slots
        return both, [
            pl.multiple_of(at[base + j] * PAIR * BLOCK, PAIR * BLOCK) for j in range(slots)
        ]

    def piece_of(n, put):
        items = [load(where[n] * per_piece + i) for i in range(per_piece)]
        logits = []
        for both, picks in items:
            keys = jnp.concatenate([table[pl.ds(p, BLOCK), :] for p in picks], axis=0)
            logits.append(
                lax.dot_general(both, keys, (((1,), (1,)), ((), ())), preferred_element_type=f32)
            )
        weights = []
        for i in range(per_piece):
            block = where[n] * per_piece + i
            weights.append(jnp.exp2(logits[i]) * mask[pl.ds(block, 1), :])
        for i, (both, picks) in enumerate(items):
            values = jnp.concatenate(
                [table[pl.ds(p + BLOCK, BLOCK), :] for p in picks], axis=0
            )
            sums = jnp.dot(weights[i].astype(bf16), values, preferred_element_type=f32)
            scale = 1.0 / jnp.sum(weights[i], axis=-1, keepdims=True)
            to = slice(i * BLOCK, (i + 1) * BLOCK)
            put(to, slice(0, HEAD_DIM), sums[:BLOCK, :HEAD_DIM] * scale[:BLOCK])
            put(to, slice(HEAD_DIM, WIDTH), sums[BLOCK:, HEAD_DIM:] * scale[BLOCK:])

    if whole:

        def one(n, carry):
            def put(rows, lanes, value):
                outs[0][n, rows, lanes] = value.astype(bf16)

            piece_of(n, put)
            return carry

        lax.fori_loop(0, count, one, 0)
    else:
        for n in range(count):

            def put(rows, lanes, value, n=n):
                outs[n][rows, lanes] = value.astype(bf16)

            piece_of(n, put)


def attend(chunk, chunks, split, at, where, queries, mask, pairs, got):
    ranks = where.shape[0]
    length = queries.shape[0] // chunks
    slots = mask.shape[1] // BLOCK
    blocks = length // BLOCK
    rows = length // ranks
    devices, arrived, _ = got.shape
    plain = REACH * PAIR * BLOCK
    anywhere = pl.BlockSpec(memory_space=pl.ANY)
    shape = (rows, WIDTH) if split else (ranks, rows, WIDTH)
    count = ranks if split else 1
    height = pairs.shape[0] + devices * plain + HOT * PAIR * BLOCK
    outs = pl.pallas_call(
        functools.partial(attention_kernel, chunk * blocks),
        grid_spec=pltpu.PrefetchScalarGridSpec(
            num_scalar_prefetch=2,
            grid=(1,),
            in_specs=[
                pl.BlockSpec((length, WIDTH), lambda i, *_: (chunk, 0)),
                pl.BlockSpec((blocks, slots * BLOCK), lambda i, *_: (chunk, 0)),
                anywhere,
                anywhere,
            ],
            out_specs=[whole_block(*shape)] * count,
            scratch_shapes=[
                pltpu.VMEM((height, WIDTH), bf16),
                pltpu.VMEM((devices, arrived - plain, WIDTH), bf16),
                pltpu.SemaphoreType.DMA((devices + 2,)),
            ],
        ),
        out_shape=[jax.ShapeDtypeStruct(shape, bf16)] * count,
        compiler_params=pltpu.CompilerParams(vmem_limit_bytes=VMEM_LIMIT),
        cost_estimate=pl.CostEstimate(
            flops=8 * length * WIDTH * slots * BLOCK, bytes_accessed=10 << 20, transcendentals=0
        ),
        name="attend",
    )(at, where, queries, mask, pairs, got)
    return list(outs) if split else outs[0]


def out_kernel(order, slot, *refs):
    count = order.shape[0]
    n = pl.program_id(0)
    if len(refs) > 2 * count + 4:
        pieces, refs = refs[:count], refs[count:]
    else:
        pieces, refs = [refs[0].at[order[k]] for k in range(count)], refs[1:]
    weights, gain, refs = refs[:count], refs[count], refs[count + 1 :]
    outs, (mixed, squares) = refs[:-2], refs[-2:]
    rows = jnp.concatenate([piece[...] for piece in pieces], axis=1)
    weight = jnp.concatenate([w[...] for w in weights], axis=0)
    sums = jnp.dot(rows, weight, preferred_element_type=f32)
    tile = sums.shape[1]
    mixed[2 * n] = sums[:, :WIDTH]
    mixed[2 * n + 1] = sums[:, WIDTH:]
    part = sum(sums[:, i : i + 128] * sums[:, i : i + 128] for i in range(0, tile, 128))

    @pl.when(n == 0)
    def _():
        squares[...] = part

    @pl.when(n > 0)
    def _():
        squares[...] += part

    @pl.when(n == pl.num_programs(0) - 1)
    def _():
        total = jnp.sum(squares[...], axis=-1, keepdims=True)
        factor = lax.rsqrt(total * (1.0 / (count * WIDTH)) + norm_eps)
        for k in range(count):
            value = (mixed[slot[k]] * factor * gain[slot[k]]).astype(bf16)
            if len(outs) == 1:
                outs[0][k] = value
            else:
                outs[k][...] = value


def project_out(split, order, slot, pieces, weights, gain):
    count = len(weights)
    pieces = list(pieces) if split else [pieces]
    rows = pieces[0].shape[-2]
    depth, width = weights[0].shape
    tile = 2 * WIDTH
    shape = (rows, WIDTH) if split else (count, rows, WIDTH)
    outs = pl.pallas_call(
        out_kernel,
        grid_spec=pltpu.PrefetchScalarGridSpec(
            num_scalar_prefetch=2,
            grid=(width // tile,),
            in_specs=[whole_block(*shape)] * len(pieces)
            + [pl.BlockSpec((depth, tile), lambda n, *_: (0, n))] * count
            + [whole_block(*gain.shape)],
            out_specs=[whole_block(*shape)] * len(pieces),
            scratch_shapes=[
                pltpu.VMEM((count, rows, WIDTH), f32),
                pltpu.VMEM((rows, 128), f32),
            ],
        ),
        out_shape=[jax.ShapeDtypeStruct(shape, bf16)] * len(pieces),
        compiler_params=pltpu.CompilerParams(vmem_limit_bytes=VMEM_LIMIT),
        cost_estimate=pl.CostEstimate(
            flops=2 * rows * width * width, bytes_accessed=12 << 20, transcendentals=0
        ),
        name="project_out",
    )(order, slot, *pieces, *weights, gain)
    return list(outs) if split else outs[0]


def place_kernel(order, whole, *rest):
    count = len(rest) - 2
    parts, out, sems = rest[:count], rest[count], rest[count + 1]
    copies = [pltpu.make_async_copy(whole, out.at[pl.ds(0, count)], sems.at[count])]
    for k in range(count):
        copies.append(pltpu.make_async_copy(parts[k], out.at[count + order[k]], sems.at[k]))
    for copy in copies:
        copy.start()
    for copy in copies:
        copy.wait()


def place(order, whole, parts):
    count = len(parts)
    shape = (2 * count,) + parts[0].shape
    anywhere = pl.BlockSpec(memory_space=pl.ANY)
    return pl.pallas_call(
        place_kernel,
        grid_spec=pltpu.PrefetchScalarGridSpec(
            num_scalar_prefetch=1,
            grid=(1,),
            in_specs=[anywhere] * (count + 1),
            out_specs=pl.BlockSpec(shape, lambda i, order: (0, 0, 0)),
            scratch_shapes=[pltpu.SemaphoreType.DMA((count + 1,))],
        ),
        out_shape=jax.ShapeDtypeStruct(shape, bf16),
        compiler_params=pltpu.CompilerParams(vmem_limit_bytes=8 << 20),
        cost_estimate=pl.CostEstimate(flops=1 << 20, bytes_accessed=4 << 20, transcendentals=0),
        name="place",
    )(order, whole, *parts)


def exchange(pieces, axes):
    return lax.all_to_all(pieces, axes, split_axis=0, concat_axis=0, tiled=True)


def tied(*arrays):
    return lax.optimization_barrier(arrays)


def along_y(piece, shift):
    ring = lax.axis_size(TP[0])
    return lax.ppermute(piece, TP[0], [(i, (i + shift) % ring) for i in range(ring)])


def across(piece):
    return lax.ppermute(piece, TP[1], [(0, 1), (1, 0)])


def both_cores(parts):
    same = jnp.stack(parts)
    return same, across(same)


OFFSETS = (0, -1, 1, 2)


def piece_order(sign):
    ring = lax.axis_size(TP[0])
    y = lax.axis_index(TP[0])
    c = lax.axis_index(TP[1])
    rows = jnp.stack([(y + ring + sign * d) % ring for d in OFFSETS])
    return jnp.concatenate([2 * rows + c, 2 * rows + 1 - c]).astype(jnp.int32)


def send_pieces(pieces):
    ring = lax.axis_size(TP[0])
    got = []
    for k in range(2 * ring):
        step, swap = OFFSETS[k % ring], k // ring
        pairs = [
            (2 * y + c, 2 * ((y - step) % ring) + (c + swap) % 2)
            for y in range(ring)
            for c in range(2)
        ]
        got.append(lax.ppermute(pieces[k], TP, pairs) if k else pieces[0])
    return got


def local(tokens, w_query, w_key, w_value, w_out, query_gain, key_gain, out_gain, chosen):
    length, _ = tokens.shape
    blocks_here = length // BLOCK
    devices = lax.axis_size(KV)
    position = lax.axis_index(KV)
    ranks = lax.axis_size(TP)
    key_row = key_gain[None, :]
    query_row = (query_gain * (HEAD_DIM ** (-0.5) * LOG2E))[None, :]

    usable = chosen >= 0
    pick = jnp.where(usable, chosen, 0)
    owner_of = pick // blocks_here
    all_blocks = jnp.arange(devices * blocks_here, dtype=jnp.int32)
    marked = jnp.where(usable & (owner_of != position), chosen, -1)
    wanted = jnp.any(marked[:, :, None] == all_blocks[None, None, :], axis=(0, 1)).reshape(
        devices, blocks_here
    )
    rank_of = jnp.cumsum(wanted.astype(jnp.int32), axis=1) - 1
    local_ids = jnp.arange(blocks_here, dtype=jnp.int32)
    places = wanted[:, :, None] & (
        rank_of[:, :, None] == jnp.arange(HOT, dtype=jnp.int32)[None, None, :]
    )
    named = jnp.sum(jnp.where(places, local_ids[None, :, None], 0), axis=1).astype(jnp.int32)
    requests = jnp.concatenate([named, jnp.broadcast_to(named[:1], named.shape)], axis=1)
    asks = jnp.pad(requests.astype(bf16)[:, None, :], ((0, 0), (0, 15), (0, WIDTH - 2 * HOT)))
    order = piece_order(1)
    toward = piece_order(-1)
    same_order = jnp.arange(ranks, dtype=jnp.int32)

    rank = lax.axis_index(TP).astype(jnp.int32).reshape(1)
    arrived = exchange(token_shares(rank, tokens, asks), KV)
    shares = arrived[0, :-16]
    asked = arrived[:, -16, : 2 * HOT].astype(jnp.int32)
    asked_near = asked[:, :REACH].reshape(-1)
    asked_hot = asked[:, HOT:].reshape(-1)
    w_after = along_y(w_out, 1)
    w_before = along_y(w_out, -1)
    w_own = across(w_out)

    pairs = project_kv(tokens, w_key, w_value, key_row).reshape(-1, WIDTH)
    again, pairs = tied(tokens, pairs)
    queries = project_q(again, w_query, query_row)
    flat_rank = rank_of.reshape(-1)
    slot_rank = jnp.sum(
        jnp.where(pick[:, :, None] == all_blocks[None, None, :], flat_rank[None, None, :], 0), axis=-1
    )
    near_at = blocks_here + owner_of * REACH + slot_rank
    hot_at = blocks_here + devices * REACH + slot_rank
    at = jnp.where(
        owner_of == position, pick % blocks_here, jnp.where(owner_of == 0, hot_at, near_at)
    )
    at = jnp.where(usable, at, 0).astype(jnp.int32).reshape(-1)
    mask = jnp.repeat(usable.astype(f32), BLOCK, axis=1)

    shares, asked_near, asked_hot, queries, at, mask, order, w_after, w_before = tied(
        shares, asked_near, asked_hot, queries, at, mask, order, w_after, w_before
    )
    parts = [shares] + [along_y(shares, shift) for shift in (1, -1, 2)]
    w_far = along_y(w_after, 1)
    w_swapped = [across(w_after), across(w_before)]
    rows_same, rows_other = both_cores(parts)
    sent = project_sent(
        asked_near, asked_hot, order, rows_same, rows_other, w_key, w_value, key_row, pairs, devices
    )
    got = exchange(sent, KV)
    w_swapped.append(across(w_far))
    weights = [w_out, w_after, w_before, w_far, w_own] + w_swapped

    gains = out_gain.reshape(ranks, 1, WIDTH)
    first = attend(0, 2, False, at, same_order, queries, mask, pairs, got)
    first = exchange(first, TP)
    second = attend(1, 2, True, at, toward, queries, mask, pairs, got)
    second = send_pieces(second)
    first = project_out(False, order, same_order, first, weights, gains)
    moved = exchange(first, TP)
    second = tied(first, *second)[1:]
    second = project_out(True, order, toward, second, weights, gains)
    second = send_pieces(second)
    return place(order, moved, second).reshape(length, WIDTH)


def solution(mesh):
    split = Mesh(mesh.devices.reshape(4, 4, 4, 2), KV + TP)
    return jax.shard_map(
        local,
        mesh=split,
        in_specs=(
            P(KV, None),
            P(None, TP),
            P(None, TP),
            P(None, TP),
            P(TP, None),
            P(),
            P(),
            P(),
            P(KV, None),
        ),
        out_specs=P(KV, TP),
        check_vma=False,
    )
```

```python
import functools

import jax
import jax.numpy as jnp
from jax import lax
from jax.experimental import pallas as pl
from jax.experimental.pallas import tpu as pltpu
from jax.sharding import Mesh
from jax.sharding import PartitionSpec as P

HEAD_DIM = 128
BLOCK = 64
HOT = 8
REACH = 2
KV = ("kv_0", "kv_1")
TP = ("tp_0", "tp_1")
WIDTH = 256
PAIR = 2
norm_eps = 1e-06
LOG2E = 1.4426950408889634
bf16 = jnp.bfloat16
f32 = jnp.float32
VMEM_LIMIT = 60 * 1024 * 1024


def head_norm(values, gain_row):
    factor = lax.rsqrt(jnp.mean(values * values, axis=-1, keepdims=True) + norm_eps)
    return (values * factor * gain_row).astype(bf16)


def share_kernel(rank, tok, asks, out):
    rows = tok[...].astype(f32)
    devices = out.shape[0]
    part = BLOCK // devices
    small = rows.shape[0] // devices
    step = pl.program_id(0)
    for k in range(small // 16):
        parts = []
        for b in range(16 // part):
            first = (k * (16 // part) + b) * BLOCK
            parts.append(rows[first : first + BLOCK].reshape(devices, part, WIDTH))
        at = pl.ds(pl.multiple_of(step * small + k * 16, 16), 16)
        out[:, at, :] = jnp.concatenate(parts, axis=1).astype(bf16)

    @pl.when(step == 0)
    def _():
        out[:, -16:, :] = asks[...]


def token_shares(rank, tokens, asks):
    length = tokens.shape[0]
    devices = asks.shape[0]
    tile = 1024
    shape = (devices, length // devices + 16, WIDTH)
    return pl.pallas_call(
        share_kernel,
        grid_spec=pltpu.PrefetchScalarGridSpec(
            num_scalar_prefetch=1,
            grid=(length // tile,),
            in_specs=[
                pl.BlockSpec((tile, WIDTH), lambda i, rank: (i, rank[0])),
                pl.BlockSpec(asks.shape, lambda i, rank: (0, 0, 0)),
            ],
            out_specs=pl.BlockSpec(shape, lambda i, rank: (0, 0, 0)),
        ),
        out_shape=jax.ShapeDtypeStruct(shape, bf16),
        compiler_params=pltpu.CompilerParams(vmem_limit_bytes=VMEM_LIMIT),
        cost_estimate=pl.CostEstimate(flops=1 << 20, bytes_accessed=4 << 20, transcendentals=0),
        name="token_shares",
    )(rank, tokens, asks)


def kv_kernel(tok, wk, wv, gain, out):
    rows = tok[...]
    keys = jnp.dot(rows, wk[...], preferred_element_type=f32)
    blocks = out.shape[0]
    for h in range(2):
        lanes = slice(h * HEAD_DIM, (h + 1) * HEAD_DIM)
        normed = head_norm(keys[:, lanes], gain[...])
        out[:, 0, :, lanes] = normed.reshape(blocks, BLOCK, HEAD_DIM)
    vals = jnp.dot(rows, wv[...], preferred_element_type=f32).astype(bf16)
    out[:, 1, :, :] = vals.reshape(blocks, BLOCK, WIDTH)


def project_kv(tokens, w_key, w_value, gain):
    length, depth = tokens.shape
    tile = 1024
    blocks = tile // BLOCK
    return pl.pallas_call(
        kv_kernel,
        grid=(length // tile,),
        in_specs=[
            pl.BlockSpec((tile, depth), lambda i: (i, 0)),
            pl.BlockSpec((depth, WIDTH), lambda i: (0, 0)),
            pl.BlockSpec((depth, WIDTH), lambda i: (0, 0)),
            pl.BlockSpec((1, HEAD_DIM), lambda i: (0, 0)),
        ],
        out_specs=pl.BlockSpec((blocks, PAIR, BLOCK, WIDTH), lambda i: (i, 0, 0, 0)),
        out_shape=jax.ShapeDtypeStruct((length // BLOCK, PAIR, BLOCK, WIDTH), bf16),
        compiler_params=pltpu.CompilerParams(vmem_limit_bytes=VMEM_LIMIT),
        cost_estimate=pl.CostEstimate(
            flops=4 * length * depth * WIDTH, bytes_accessed=2 * length * depth, transcendentals=0
        ),
        name="project_kv",
    )(tokens, w_key, w_value, gain)


def q_kernel(tok, wq, gain, out):
    values = jnp.dot(tok[...], wq[...], preferred_element_type=f32)
    for h in range(2):
        lanes = slice(h * HEAD_DIM, (h + 1) * HEAD_DIM)
        out[:, lanes] = head_norm(values[:, lanes], gain[...])


def project_q(tokens, w_query, gain):
    length, depth = tokens.shape
    tile = 1024
    return pl.pallas_call(
        q_kernel,
        grid=(length // tile,),
        in_specs=[
            pl.BlockSpec((tile, depth), lambda i: (i, 0)),
            pl.BlockSpec((depth, WIDTH), lambda i: (0, 0)),
            pl.BlockSpec((1, HEAD_DIM), lambda i: (0, 0)),
        ],
        out_specs=pl.BlockSpec((tile, WIDTH), lambda i: (i, 0)),
        out_shape=jax.ShapeDtypeStruct((length, WIDTH), bf16),
        compiler_params=pltpu.CompilerParams(vmem_limit_bytes=VMEM_LIMIT),
        cost_estimate=pl.CostEstimate(
            flops=2 * length * depth * WIDTH, bytes_accessed=2 * length * depth, transcendentals=0
        ),
        name="project_q",
    )(tokens, w_query, gain)


def near_kernel(near, pairs, out, room, in_sems, out_sems):
    devices = out.shape[0]
    reach = near.shape[0] // devices
    unit = PAIR * BLOCK
    coming, going = [], []
    for m in range(near.shape[0]):
        first = pl.multiple_of(near[m] * unit, unit)
        coming.append(
            pltpu.make_async_copy(pairs.at[pl.ds(first, unit)], room.at[m], in_sems.at[m])
        )
        to = out.at[m // reach, pl.ds((m % reach) * unit, unit)]
        going.append(pltpu.make_async_copy(room.at[m], to, out_sems.at[m]))
    for copy in coming:
        copy.start()
    for n, copy in enumerate(coming):
        copy.wait()
        going[n].start()
    for copy in going:
        copy.wait()


def gather_near(near, pairs, devices, length):
    anywhere = pl.BlockSpec(memory_space=pl.ANY)
    sends = near.shape[0]
    return pl.pallas_call(
        near_kernel,
        grid_spec=pltpu.PrefetchScalarGridSpec(
            num_scalar_prefetch=1,
            grid=(1,),
            in_specs=[anywhere],
            out_specs=anywhere,
            scratch_shapes=[
                pltpu.VMEM((sends, PAIR * BLOCK, WIDTH), bf16),
                pltpu.SemaphoreType.DMA((sends,)),
                pltpu.SemaphoreType.DMA((sends,)),
            ],
        ),
        out_shape=jax.ShapeDtypeStruct((devices, length, WIDTH), bf16),
        compiler_params=pltpu.CompilerParams(vmem_limit_bytes=VMEM_LIMIT),
        cost_estimate=pl.CostEstimate(flops=1 << 20, bytes_accessed=4 << 20, transcendentals=0),
        name="gather_near",
    )(near, pairs)


def send_kernel(asked, order, same, other, wk, wv, gain, _, out, keep):
    devices, rows, _ = out.shape
    keys = jnp.zeros((same.shape[1], WIDTH), f32)
    vals = jnp.zeros((same.shape[1], WIDTH), f32)
    count = same.shape[0]
    for k in range(2 * count):
        tokens = same[k] if k < count else other[k - count]
        span = pl.ds(pl.multiple_of(order[k] * WIDTH, WIDTH), WIDTH)
        keys += jnp.dot(tokens, wk[span, :], preferred_element_type=f32)
        vals += jnp.dot(tokens, wv[span, :], preferred_element_type=f32)
    groups, unit, _ = keep.shape
    part = unit // 2
    for h in range(2):
        lanes = slice(h * HEAD_DIM, (h + 1) * HEAD_DIM)
        x = keys[:, lanes]
        factor = lax.rsqrt(jnp.mean(x * x, axis=-1, keepdims=True) + norm_eps)
        keep[:, :part, lanes] = (x * factor * gain[...]).reshape(groups, part, HEAD_DIM)
    keep[:, part:, :] = vals.reshape(groups, part, WIDTH)

    twos = rows // (2 * unit)

    def one(m, carry):
        both = jnp.concatenate([keep[asked[2 * m]], keep[asked[2 * m + 1]]], axis=0)
        at = pl.multiple_of((m % twos) * 2 * unit, 2 * unit)
        out[m // twos, pl.ds(at, 2 * unit), :] = both.astype(bf16)
        return carry

    lax.fori_loop(0, devices * twos, one, 0, unroll=4)


def whole_block(*shape):
    return pl.BlockSpec(shape, lambda i, *_: (0,) * len(shape))


def project_sent(asked, order, same, other, w_key, w_value, gain, sent):
    count, rows, _ = same.shape
    groups = 64
    unit = 2 * rows // groups
    depth = w_key.shape[0]
    devices, length, _ = sent.shape
    hot_rows = (asked.shape[0] // devices) * unit
    last = length // hot_rows - 1
    return pl.pallas_call(
        send_kernel,
        grid_spec=pltpu.PrefetchScalarGridSpec(
            num_scalar_prefetch=2,
            grid=(1,),
            in_specs=[
                whole_block(count, rows, WIDTH),
                whole_block(count, rows, WIDTH),
                whole_block(depth, WIDTH),
                whole_block(depth, WIDTH),
                whole_block(1, HEAD_DIM),
                pl.BlockSpec(memory_space=pl.ANY),
            ],
            out_specs=pl.BlockSpec((devices, hot_rows, WIDTH), lambda i, *_: (0, last, 0)),
            scratch_shapes=[pltpu.VMEM((groups, unit, WIDTH), f32)],
        ),
        out_shape=jax.ShapeDtypeStruct(sent.shape, bf16),
        input_output_aliases={7: 0},
        compiler_params=pltpu.CompilerParams(vmem_limit_bytes=VMEM_LIMIT),
        cost_estimate=pl.CostEstimate(
            flops=4 * rows * depth * WIDTH, bytes_accessed=8 << 20, transcendentals=0
        ),
        name="project_sent",
    )(asked, order, same, other, w_key, w_value, gain, sent)


def attention_kernel(first, at, where, q, mask, pairs, got, *rest):
    outs, (table, raw, sems) = rest[:-3], rest[-3:]
    devices, rows, _ = got.shape
    here = pairs.shape[0]
    hot_rows = raw.shape[1]
    plain = rows - hot_rows
    copies = [
        pltpu.make_async_copy(got.at[:, pl.ds(plain, hot_rows)], raw, sems.at[devices]),
        pltpu.make_async_copy(pairs, table.at[pl.ds(0, here)], sems.at[devices + 1]),
    ]
    for n in range(devices):
        span = table.at[pl.ds(here + n * plain, plain)]
        copies.append(pltpu.make_async_copy(got.at[n, pl.ds(0, plain)], span, sems.at[n]))
    for copy in copies:
        copy.start()
    copies[0].wait()
    part = BLOCK // devices
    for n in range(hot_rows // 16):
        both = raw[:, n * 16 : (n + 1) * 16, :].astype(f32)
        for m in range(2):
            start = here + devices * plain + (2 * n + m) * PAIR * BLOCK
            for kind in range(PAIR):
                low = m * 2 * part + kind * part
                piece = both[:, low : low + part, :].reshape(BLOCK, WIDTH).astype(bf16)
                table[start + kind * BLOCK : start + (kind + 1) * BLOCK, :] = piece
    for copy in copies[1:]:
        copy.wait()
    slots = mask.shape[1] // BLOCK
    count = where.shape[0]
    whole = len(outs) == 1
    per_piece = mask.shape[0] // count
    blank = jnp.zeros((BLOCK, HEAD_DIM), bf16)

    def load(block):
        row = pl.multiple_of(block * BLOCK, BLOCK)
        rows = q[pl.ds(row, BLOCK), :]
        both = jnp.concatenate(
            [
                jnp.concatenate([rows[:, :HEAD_DIM], blank], axis=1),
                jnp.concatenate([blank, rows[:, HEAD_DIM:]], axis=1),
            ],
            axis=0,
        )
        base = (first + block) * slots
        return both, [
            pl.multiple_of(at[base + j] * PAIR * BLOCK, PAIR * BLOCK) for j in range(slots)
        ]

    def piece_of(n, put):
        items = [load(where[n] * per_piece + i) for i in range(per_piece)]
        logits = []
        for both, picks in items:
            keys = jnp.concatenate([table[pl.ds(p, BLOCK), :] for p in picks], axis=0)
            logits.append(
                lax.dot_general(both, keys, (((1,), (1,)), ((), ())), preferred_element_type=f32)
            )
        weights = []
        for i in range(per_piece):
            block = where[n] * per_piece + i
            weights.append(jnp.exp2(logits[i]) * mask[pl.ds(block, 1), :])
        for i, (both, picks) in enumerate(items):
            values = jnp.concatenate(
                [table[pl.ds(p + BLOCK, BLOCK), :] for p in picks], axis=0
            )
            sums = jnp.dot(weights[i].astype(bf16), values, preferred_element_type=f32)
            scale = 1.0 / jnp.sum(weights[i], axis=-1, keepdims=True)
            to = slice(i * BLOCK, (i + 1) * BLOCK)
            put(to, slice(0, HEAD_DIM), sums[:BLOCK, :HEAD_DIM] * scale[:BLOCK])
            put(to, slice(HEAD_DIM, WIDTH), sums[BLOCK:, HEAD_DIM:] * scale[BLOCK:])

    if whole:

        def one(n, carry):
            def put(rows, lanes, value):
                outs[0][n, rows, lanes] = value.astype(bf16)

            piece_of(n, put)
            return carry

        lax.fori_loop(0, count, one, 0)
    else:
        for n in range(count):

            def put(rows, lanes, value, n=n):
                outs[n][rows, lanes] = value.astype(bf16)

            piece_of(n, put)


def attend(chunk, chunks, split, at, where, queries, mask, pairs, got):
    ranks = where.shape[0]
    length = queries.shape[0] // chunks
    slots = mask.shape[1] // BLOCK
    blocks = length // BLOCK
    rows = length // ranks
    devices, arrived, _ = got.shape
    plain = REACH * PAIR * BLOCK
    anywhere = pl.BlockSpec(memory_space=pl.ANY)
    shape = (rows, WIDTH) if split else (ranks, rows, WIDTH)
    count = ranks if split else 1
    height = pairs.shape[0] + devices * plain + HOT * PAIR * BLOCK
    outs = pl.pallas_call(
        functools.partial(attention_kernel, chunk * blocks),
        grid_spec=pltpu.PrefetchScalarGridSpec(
            num_scalar_prefetch=2,
            grid=(1,),
            in_specs=[
                pl.BlockSpec((length, WIDTH), lambda i, *_: (chunk, 0)),
                pl.BlockSpec((blocks, slots * BLOCK), lambda i, *_: (chunk, 0)),
                anywhere,
                anywhere,
            ],
            out_specs=[whole_block(*shape)] * count,
            scratch_shapes=[
                pltpu.VMEM((height, WIDTH), bf16),
                pltpu.VMEM((devices, arrived - plain, WIDTH), bf16),
                pltpu.SemaphoreType.DMA((devices + 2,)),
            ],
        ),
        out_shape=[jax.ShapeDtypeStruct(shape, bf16)] * count,
        compiler_params=pltpu.CompilerParams(vmem_limit_bytes=VMEM_LIMIT),
        cost_estimate=pl.CostEstimate(
            flops=8 * length * WIDTH * slots * BLOCK, bytes_accessed=10 << 20, transcendentals=0
        ),
        name="attend",
    )(at, where, queries, mask, pairs, got)
    return list(outs) if split else outs[0]


def out_kernel(order, slot, *refs):
    count = order.shape[0]
    n = pl.program_id(0)
    if len(refs) > 2 * count + 4:
        pieces, refs = refs[:count], refs[count:]
    else:
        pieces, refs = [refs[0].at[order[k]] for k in range(count)], refs[1:]
    weights, gain, refs = refs[:count], refs[count], refs[count + 1 :]
    outs, (mixed, squares) = refs[:-2], refs[-2:]
    rows = jnp.concatenate([piece[...] for piece in pieces], axis=1)
    weight = jnp.concatenate([w[...] for w in weights], axis=0)
    sums = jnp.dot(rows, weight, preferred_element_type=f32)
    tile = sums.shape[1]
    mixed[2 * n] = sums[:, :WIDTH]
    mixed[2 * n + 1] = sums[:, WIDTH:]
    part = sum(sums[:, i : i + 128] * sums[:, i : i + 128] for i in range(0, tile, 128))

    @pl.when(n == 0)
    def _():
        squares[...] = part

    @pl.when(n > 0)
    def _():
        squares[...] += part

    @pl.when(n == pl.num_programs(0) - 1)
    def _():
        total = jnp.sum(squares[...], axis=-1, keepdims=True)
        factor = lax.rsqrt(total * (1.0 / (count * WIDTH)) + norm_eps)
        for k in range(count):
            value = (mixed[slot[k]] * factor * gain[slot[k]]).astype(bf16)
            if len(outs) == 1:
                outs[0][k] = value
            else:
                outs[k][...] = value


def project_out(split, order, slot, pieces, weights, gain):
    count = len(weights)
    pieces = list(pieces) if split else [pieces]
    rows = pieces[0].shape[-2]
    depth, width = weights[0].shape
    tile = 2 * WIDTH
    shape = (rows, WIDTH) if split else (count, rows, WIDTH)
    outs = pl.pallas_call(
        out_kernel,
        grid_spec=pltpu.PrefetchScalarGridSpec(
            num_scalar_prefetch=2,
            grid=(width // tile,),
            in_specs=[whole_block(*shape)] * len(pieces)
            + [pl.BlockSpec((depth, tile), lambda n, *_: (0, n))] * count
            + [whole_block(*gain.shape)],
            out_specs=[whole_block(*shape)] * len(pieces),
            scratch_shapes=[
                pltpu.VMEM((count, rows, WIDTH), f32),
                pltpu.VMEM((rows, 128), f32),
            ],
        ),
        out_shape=[jax.ShapeDtypeStruct(shape, bf16)] * len(pieces),
        compiler_params=pltpu.CompilerParams(vmem_limit_bytes=VMEM_LIMIT),
        cost_estimate=pl.CostEstimate(
            flops=2 * rows * width * width, bytes_accessed=12 << 20, transcendentals=0
        ),
        name="project_out",
    )(order, slot, *pieces, *weights, gain)
    return list(outs) if split else outs[0]


def place_kernel(order, whole, *rest):
    count = len(rest) - 2
    parts, out, sems = rest[:count], rest[count], rest[count + 1]
    copies = [pltpu.make_async_copy(whole, out.at[pl.ds(0, count)], sems.at[count])]
    for k in range(count):
        copies.append(pltpu.make_async_copy(parts[k], out.at[count + order[k]], sems.at[k]))
    for copy in copies:
        copy.start()
    for copy in copies:
        copy.wait()


def place(order, whole, parts):
    count = len(parts)
    shape = (2 * count,) + parts[0].shape
    anywhere = pl.BlockSpec(memory_space=pl.ANY)
    return pl.pallas_call(
        place_kernel,
        grid_spec=pltpu.PrefetchScalarGridSpec(
            num_scalar_prefetch=1,
            grid=(1,),
            in_specs=[anywhere] * (count + 1),
            out_specs=anywhere,
            scratch_shapes=[pltpu.SemaphoreType.DMA((count + 1,))],
        ),
        out_shape=jax.ShapeDtypeStruct(shape, bf16),
        compiler_params=pltpu.CompilerParams(vmem_limit_bytes=8 << 20),
        cost_estimate=pl.CostEstimate(flops=1 << 20, bytes_accessed=4 << 20, transcendentals=0),
        name="place",
    )(order, whole, *parts)


def exchange(pieces, axes):
    return lax.all_to_all(pieces, axes, split_axis=0, concat_axis=0, tiled=True)


def tied(*arrays):
    return lax.optimization_barrier(arrays)


def along_y(piece, shift):
    ring = lax.axis_size(TP[0])
    return lax.ppermute(piece, TP[0], [(i, (i + shift) % ring) for i in range(ring)])


def across(piece):
    return lax.ppermute(piece, TP[1], [(0, 1), (1, 0)])


def both_cores(parts):
    same = jnp.stack(parts)
    return same, across(same)


OFFSETS = (0, -1, 1, 2)


def piece_order(sign):
    ring = lax.axis_size(TP[0])
    y = lax.axis_index(TP[0])
    c = lax.axis_index(TP[1])
    rows = jnp.stack([(y + ring + sign * d) % ring for d in OFFSETS])
    return jnp.concatenate([2 * rows + c, 2 * rows + 1 - c]).astype(jnp.int32)


def send_pieces(pieces):
    ring = lax.axis_size(TP[0])
    got = []
    for k in range(2 * ring):
        step, swap = OFFSETS[k % ring], k // ring
        pairs = [
            (2 * y + c, 2 * ((y - step) % ring) + (c + swap) % 2)
            for y in range(ring)
            for c in range(2)
        ]
        got.append(lax.ppermute(pieces[k], TP, pairs) if k else pieces[0])
    return got


def local(tokens, w_query, w_key, w_value, w_out, query_gain, key_gain, out_gain, chosen):
    length, _ = tokens.shape
    blocks_here = length // BLOCK
    devices = lax.axis_size(KV)
    position = lax.axis_index(KV)
    ranks = lax.axis_size(TP)
    part = BLOCK // devices
    key_row = key_gain[None, :]
    query_row = (query_gain * (HEAD_DIM ** (-0.5) * LOG2E))[None, :]

    usable = chosen >= 0
    pick = jnp.where(usable, chosen, 0)
    owner_of = pick // blocks_here
    all_blocks = jnp.arange(devices * blocks_here, dtype=jnp.int32)
    marked = jnp.where(usable & (owner_of != position), chosen, -1)
    wanted = jnp.any(marked[:, :, None] == all_blocks[None, None, :], axis=(0, 1)).reshape(
        devices, blocks_here
    )
    rank_of = jnp.cumsum(wanted.astype(jnp.int32), axis=1) - 1
    local_ids = jnp.arange(blocks_here, dtype=jnp.int32)
    places = wanted[:, :, None] & (
        rank_of[:, :, None] == jnp.arange(HOT, dtype=jnp.int32)[None, None, :]
    )
    named = jnp.sum(jnp.where(places, local_ids[None, :, None], 0), axis=1).astype(jnp.int32)
    requests = jnp.concatenate([named, jnp.broadcast_to(named[:1], named.shape)], axis=1)
    asks = jnp.pad(requests.astype(bf16)[:, None, :], ((0, 0), (0, 15), (0, WIDTH - 2 * HOT)))
    order = piece_order(1)
    toward = piece_order(-1)
    same_order = jnp.arange(ranks, dtype=jnp.int32)

    rank = lax.axis_index(TP).astype(jnp.int32).reshape(1)
    arrived = exchange(token_shares(rank, tokens, asks), KV)
    w_after = along_y(w_out, 1)
    w_before = along_y(w_out, -1)
    w_own = across(w_out)

    pairs = project_kv(tokens, w_key, w_value, key_row).reshape(-1, WIDTH)
    again, pairs = tied(tokens, pairs)
    queries = project_q(again, w_query, query_row)
    flat_rank = rank_of.reshape(-1)
    slot_rank = jnp.sum(
        jnp.where(pick[:, :, None] == all_blocks[None, None, :], flat_rank[None, None, :], 0), axis=-1
    )
    near_at = blocks_here + owner_of * REACH + slot_rank
    hot_at = blocks_here + devices * REACH + slot_rank
    at = jnp.where(
        owner_of == position, pick % blocks_here, jnp.where(owner_of == 0, hot_at, near_at)
    )
    at = jnp.where(usable, at, 0).astype(jnp.int32).reshape(-1)
    mask = jnp.repeat(usable.astype(f32), BLOCK, axis=1)

    arrived, queries, at, mask, order, w_after, w_before = tied(
        arrived, queries, at, mask, order, w_after, w_before
    )
    shares = arrived[0, :-16]
    parts = [shares] + [along_y(shares, shift) for shift in (1, -1, 2)]
    w_far = along_y(w_after, 1)
    w_swapped = [across(w_after), across(w_before)]
    asked = arrived[:, -16, : 2 * HOT].astype(jnp.int32)
    asked_near = asked[:, :REACH].reshape(-1)
    asked_hot = asked[:, HOT:].reshape(-1)
    length_sent = REACH * PAIR * BLOCK + HOT * 2 * part
    sent = gather_near(asked_near, pairs, devices, length_sent)
    asked_hot, sent, *parts = tied(asked_hot, sent, *parts)
    rows_same, rows_other = both_cores(parts)
    sent = project_sent(asked_hot, order, rows_same, rows_other, w_key, w_value, key_row, sent)
    got = exchange(sent, KV)
    w_swapped.append(across(w_far))
    weights = [w_out, w_after, w_before, w_far, w_own] + w_swapped

    gains = out_gain.reshape(ranks, 1, WIDTH)
    first = attend(0, 2, False, at, same_order, queries, mask, pairs, got)
    first = exchange(first, TP)
    second = attend(1, 2, True, at, toward, queries, mask, pairs, got)
    second = send_pieces(second)
    first = project_out(False, order, same_order, first, weights, gains)
    moved = exchange(first, TP)
    second = tied(first, *second)[1:]
    second = project_out(True, order, toward, second, weights, gains)
    second = send_pieces(second)
    return place(order, moved, second).reshape(length, WIDTH)


def solution(mesh):
    split = Mesh(mesh.devices.reshape(4, 4, 4, 2), KV + TP)
    return jax.shard_map(
        local,
        mesh=split,
        in_specs=(
            P(KV, None),
            P(None, TP),
            P(None, TP),
            P(None, TP),
            P(TP, None),
            P(),
            P(),
            P(),
            P(KV, None),
        ),
        out_specs=P(KV, TP),
        check_vma=False,
    )
```

```python
import functools

import jax
import jax.numpy as jnp
from jax import lax
from jax.experimental import pallas as pl
from jax.experimental.pallas import tpu as pltpu
from jax.sharding import Mesh
from jax.sharding import PartitionSpec as P

HEAD_DIM = 128
BLOCK = 64
HOT = 8
REACH = 2
KV = ("kv_0", "kv_1")
TP = ("tp_0", "tp_1")
WIDTH = 256
PAIR = 2
norm_eps = 1e-06
LOG2E = 1.4426950408889634
bf16 = jnp.bfloat16
f32 = jnp.float32
VMEM_LIMIT = 60 * 1024 * 1024


def head_norm(values, gain_row):
    factor = lax.rsqrt(jnp.mean(values * values, axis=-1, keepdims=True) + norm_eps)
    return (values * factor * gain_row).astype(bf16)


def share_kernel(rank, tok, out):
    rows = tok[...].astype(f32)
    devices = out.shape[0]
    part = BLOCK // devices
    for k in range(out.shape[1] // 16):
        parts = []
        for b in range(16 // part):
            first = (k * (16 // part) + b) * BLOCK
            parts.append(rows[first : first + BLOCK].reshape(devices, part, WIDTH))
        out[:, k * 16 : (k + 1) * 16, :] = jnp.concatenate(parts, axis=1).astype(bf16)


def token_shares(rank, tokens, devices):
    length = tokens.shape[0]
    tile = 1024
    small = tile // devices
    return pl.pallas_call(
        share_kernel,
        grid_spec=pltpu.PrefetchScalarGridSpec(
            num_scalar_prefetch=1,
            grid=(length // tile,),
            in_specs=[pl.BlockSpec((tile, WIDTH), lambda i, rank: (i, rank[0]))],
            out_specs=pl.BlockSpec((devices, small, WIDTH), lambda i, rank: (0, i, 0)),
        ),
        out_shape=jax.ShapeDtypeStruct((devices, length // devices, WIDTH), bf16),
        compiler_params=pltpu.CompilerParams(vmem_limit_bytes=VMEM_LIMIT),
        cost_estimate=pl.CostEstimate(flops=1 << 20, bytes_accessed=4 << 20, transcendentals=0),
        name="token_shares",
    )(rank, tokens)


def kv_kernel(tok, wk, wv, gain, out):
    rows = tok[...]
    keys = jnp.dot(rows, wk[...], preferred_element_type=f32)
    blocks = out.shape[0]
    for h in range(2):
        lanes = slice(h * HEAD_DIM, (h + 1) * HEAD_DIM)
        normed = head_norm(keys[:, lanes], gain[...])
        out[:, 0, :, lanes] = normed.reshape(blocks, BLOCK, HEAD_DIM)
    vals = jnp.dot(rows, wv[...], preferred_element_type=f32).astype(bf16)
    out[:, 1, :, :] = vals.reshape(blocks, BLOCK, WIDTH)


def project_kv(tokens, w_key, w_value, gain):
    length, depth = tokens.shape
    tile = 1024
    blocks = tile // BLOCK
    return pl.pallas_call(
        kv_kernel,
        grid=(length // tile,),
        in_specs=[
            pl.BlockSpec((tile, depth), lambda i: (i, 0)),
            pl.BlockSpec((depth, WIDTH), lambda i: (0, 0)),
            pl.BlockSpec((depth, WIDTH), lambda i: (0, 0)),
            pl.BlockSpec((1, HEAD_DIM), lambda i: (0, 0)),
        ],
        out_specs=pl.BlockSpec((blocks, PAIR, BLOCK, WIDTH), lambda i: (i, 0, 0, 0)),
        out_shape=jax.ShapeDtypeStruct((length // BLOCK, PAIR, BLOCK, WIDTH), bf16),
        compiler_params=pltpu.CompilerParams(vmem_limit_bytes=VMEM_LIMIT),
        cost_estimate=pl.CostEstimate(
            flops=4 * length * depth * WIDTH, bytes_accessed=2 * length * depth, transcendentals=0
        ),
        name="project_kv",
    )(tokens, w_key, w_value, gain)


def q_kernel(tok, wq, gain, out):
    values = jnp.dot(tok[...], wq[...], preferred_element_type=f32)
    for h in range(2):
        lanes = slice(h * HEAD_DIM, (h + 1) * HEAD_DIM)
        out[:, lanes] = head_norm(values[:, lanes], gain[...])


def project_q(tokens, w_query, gain):
    length, depth = tokens.shape
    tile = 1024
    return pl.pallas_call(
        q_kernel,
        grid=(length // tile,),
        in_specs=[
            pl.BlockSpec((tile, depth), lambda i: (i, 0)),
            pl.BlockSpec((depth, WIDTH), lambda i: (0, 0)),
            pl.BlockSpec((1, HEAD_DIM), lambda i: (0, 0)),
        ],
        out_specs=pl.BlockSpec((tile, WIDTH), lambda i: (i, 0)),
        out_shape=jax.ShapeDtypeStruct((length, WIDTH), bf16),
        compiler_params=pltpu.CompilerParams(vmem_limit_bytes=VMEM_LIMIT),
        cost_estimate=pl.CostEstimate(
            flops=2 * length * depth * WIDTH, bytes_accessed=2 * length * depth, transcendentals=0
        ),
        name="project_q",
    )(tokens, w_query, gain)


def near_kernel(near, pairs, out, room, in_sems, out_sems):
    unit = PAIR * BLOCK
    coming, going = [], []
    for m in range(near.shape[0]):
        first = pl.multiple_of(near[m] * unit, unit)
        coming.append(
            pltpu.make_async_copy(pairs.at[pl.ds(first, unit)], room.at[m], in_sems.at[m])
        )
        going.append(pltpu.make_async_copy(room.at[m], out.at[m], out_sems.at[m]))
    for copy in coming:
        copy.start()
    for n, copy in enumerate(coming):
        copy.wait()
        going[n].start()
    for copy in going:
        copy.wait()


def gather_near(near, pairs):
    anywhere = pl.BlockSpec(memory_space=pl.ANY)
    sends = near.shape[0]
    return pl.pallas_call(
        near_kernel,
        grid_spec=pltpu.PrefetchScalarGridSpec(
            num_scalar_prefetch=1,
            grid=(1,),
            in_specs=[anywhere],
            out_specs=anywhere,
            scratch_shapes=[
                pltpu.VMEM((sends, PAIR * BLOCK, WIDTH), bf16),
                pltpu.SemaphoreType.DMA((sends,)),
                pltpu.SemaphoreType.DMA((sends,)),
            ],
        ),
        out_shape=jax.ShapeDtypeStruct((sends, PAIR * BLOCK, WIDTH), bf16),
        compiler_params=pltpu.CompilerParams(vmem_limit_bytes=VMEM_LIMIT),
        cost_estimate=pl.CostEstimate(flops=1 << 20, bytes_accessed=4 << 20, transcendentals=0),
        name="gather_near",
    )(near, pairs)


def send_kernel(asked, order, same, other, wk, wv, gain, out, keep):
    devices, rows, _ = out.shape
    keys = jnp.zeros((same.shape[1], WIDTH), f32)
    vals = jnp.zeros((same.shape[1], WIDTH), f32)
    count = same.shape[0]
    for k in range(2 * count):
        tokens = same[k] if k < count else other[k - count]
        span = pl.ds(pl.multiple_of(order[k] * WIDTH, WIDTH), WIDTH)
        keys += jnp.dot(tokens, wk[span, :], preferred_element_type=f32)
        vals += jnp.dot(tokens, wv[span, :], preferred_element_type=f32)
    groups, unit, _ = keep.shape
    part = unit // 2
    for h in range(2):
        lanes = slice(h * HEAD_DIM, (h + 1) * HEAD_DIM)
        x = keys[:, lanes]
        factor = lax.rsqrt(jnp.mean(x * x, axis=-1, keepdims=True) + norm_eps)
        keep[:, :part, lanes] = (x * factor * gain[...]).reshape(groups, part, HEAD_DIM)
    keep[:, part:, :] = vals.reshape(groups, part, WIDTH)

    twos = rows // (2 * unit)

    def one(m, carry):
        both = jnp.concatenate([keep[asked[2 * m]], keep[asked[2 * m + 1]]], axis=0)
        at = pl.multiple_of((m % twos) * 2 * unit, 2 * unit)
        out[m // twos, pl.ds(at, 2 * unit), :] = both.astype(bf16)
        return carry

    lax.fori_loop(0, devices * twos, one, 0, unroll=4)


def whole_block(*shape):
    return pl.BlockSpec(shape, lambda i, *_: (0,) * len(shape))


def project_sent(asked, order, same, other, w_key, w_value, gain, devices):
    count, rows, _ = same.shape
    groups = 64
    unit = 2 * rows // groups
    depth = w_key.shape[0]
    shape = (devices, (asked.shape[0] // devices) * unit, WIDTH)
    return pl.pallas_call(
        send_kernel,
        grid_spec=pltpu.PrefetchScalarGridSpec(
            num_scalar_prefetch=2,
            grid=(1,),
            in_specs=[
                whole_block(count, rows, WIDTH),
                whole_block(count, rows, WIDTH),
                whole_block(depth, WIDTH),
                whole_block(depth, WIDTH),
                whole_block(1, HEAD_DIM),
            ],
            out_specs=whole_block(*shape),
            scratch_shapes=[pltpu.VMEM((groups, unit, WIDTH), f32)],
        ),
        out_shape=jax.ShapeDtypeStruct(shape, bf16),
        compiler_params=pltpu.CompilerParams(vmem_limit_bytes=VMEM_LIMIT),
        cost_estimate=pl.CostEstimate(
            flops=4 * rows * depth * WIDTH, bytes_accessed=8 << 20, transcendentals=0
        ),
        name="project_sent",
    )(asked, order, same, other, w_key, w_value, gain)


def attention_kernel(first, at, where, q, mask, pairs, near, hot, *rest):
    outs, (table, raw, sems) = rest[:-3], rest[-3:]
    devices, hot_rows, _ = hot.shape
    here = pairs.shape[0]
    plain = near.shape[0]
    copies = [
        pltpu.make_async_copy(hot, raw, sems.at[0]),
        pltpu.make_async_copy(pairs, table.at[pl.ds(0, here)], sems.at[1]),
        pltpu.make_async_copy(near, table.at[pl.ds(here, plain)], sems.at[2]),
    ]
    for copy in copies:
        copy.start()
    copies[0].wait()
    part = BLOCK // devices
    for n in range(hot_rows // 16):
        both = raw[:, n * 16 : (n + 1) * 16, :].astype(f32)
        for m in range(2):
            start = here + plain + (2 * n + m) * PAIR * BLOCK
            for kind in range(PAIR):
                low = m * 2 * part + kind * part
                piece = both[:, low : low + part, :].reshape(BLOCK, WIDTH).astype(bf16)
                table[start + kind * BLOCK : start + (kind + 1) * BLOCK, :] = piece
    for copy in copies[1:]:
        copy.wait()
    slots = mask.shape[1] // BLOCK
    count = where.shape[0]
    whole = len(outs) == 1
    per_piece = mask.shape[0] // count
    blank = jnp.zeros((BLOCK, HEAD_DIM), bf16)

    def load(block):
        row = pl.multiple_of(block * BLOCK, BLOCK)
        rows = q[pl.ds(row, BLOCK), :]
        both = jnp.concatenate(
            [
                jnp.concatenate([rows[:, :HEAD_DIM], blank], axis=1),
                jnp.concatenate([blank, rows[:, HEAD_DIM:]], axis=1),
            ],
            axis=0,
        )
        base = (first + block) * slots
        return both, [
            pl.multiple_of(at[base + j] * PAIR * BLOCK, PAIR * BLOCK) for j in range(slots)
        ]

    def piece_of(n, put):
        items = [load(where[n] * per_piece + i) for i in range(per_piece)]
        logits = []
        for both, picks in items:
            keys = jnp.concatenate([table[pl.ds(p, BLOCK), :] for p in picks], axis=0)
            logits.append(
                lax.dot_general(both, keys, (((1,), (1,)), ((), ())), preferred_element_type=f32)
            )
        weights = []
        for i in range(per_piece):
            block = where[n] * per_piece + i
            weights.append(jnp.exp2(logits[i]) * mask[pl.ds(block, 1), :])
        for i, (both, picks) in enumerate(items):
            values = jnp.concatenate(
                [table[pl.ds(p + BLOCK, BLOCK), :] for p in picks], axis=0
            )
            sums = jnp.dot(weights[i].astype(bf16), values, preferred_element_type=f32)
            scale = 1.0 / jnp.sum(weights[i], axis=-1, keepdims=True)
            to = slice(i * BLOCK, (i + 1) * BLOCK)
            put(to, slice(0, HEAD_DIM), sums[:BLOCK, :HEAD_DIM] * scale[:BLOCK])
            put(to, slice(HEAD_DIM, WIDTH), sums[BLOCK:, HEAD_DIM:] * scale[BLOCK:])

    if whole:

        def one(n, carry):
            def put(rows, lanes, value):
                outs[0][n, rows, lanes] = value.astype(bf16)

            piece_of(n, put)
            return carry

        lax.fori_loop(0, count, one, 0)
    else:
        for n in range(count):

            def put(rows, lanes, value, n=n):
                outs[n][rows, lanes] = value.astype(bf16)

            piece_of(n, put)


def attend(chunk, chunks, split, at, where, queries, mask, pairs, near, hot):
    ranks = where.shape[0]
    length = queries.shape[0] // chunks
    slots = mask.shape[1] // BLOCK
    blocks = length // BLOCK
    rows = length // ranks
    anywhere = pl.BlockSpec(memory_space=pl.ANY)
    shape = (rows, WIDTH) if split else (ranks, rows, WIDTH)
    count = ranks if split else 1
    height = pairs.shape[0] + near.shape[0] + HOT * PAIR * BLOCK
    outs = pl.pallas_call(
        functools.partial(attention_kernel, chunk * blocks),
        grid_spec=pltpu.PrefetchScalarGridSpec(
            num_scalar_prefetch=2,
            grid=(1,),
            in_specs=[
                pl.BlockSpec((length, WIDTH), lambda i, *_: (chunk, 0)),
                pl.BlockSpec((blocks, slots * BLOCK), lambda i, *_: (chunk, 0)),
                anywhere,
                anywhere,
                anywhere,
            ],
            out_specs=[whole_block(*shape)] * count,
            scratch_shapes=[
                pltpu.VMEM((height, WIDTH), bf16),
                pltpu.VMEM(hot.shape, bf16),
                pltpu.SemaphoreType.DMA((3,)),
            ],
        ),
        out_shape=[jax.ShapeDtypeStruct(shape, bf16)] * count,
        compiler_params=pltpu.CompilerParams(vmem_limit_bytes=VMEM_LIMIT),
        cost_estimate=pl.CostEstimate(
            flops=8 * length * WIDTH * slots * BLOCK, bytes_accessed=10 << 20, transcendentals=0
        ),
        name="attend",
    )(at, where, queries, mask, pairs, near, hot)
    return list(outs) if split else outs[0]


def out_kernel(order, slot, *refs):
    count = order.shape[0]
    n = pl.program_id(0)
    if len(refs) > 2 * count + 4:
        pieces, refs = refs[:count], refs[count:]
    else:
        pieces, refs = [refs[0].at[order[k]] for k in range(count)], refs[1:]
    weights, gain, refs = refs[:count], refs[count], refs[count + 1 :]
    outs, (mixed, squares) = refs[:-2], refs[-2:]
    rows = jnp.concatenate([piece[...] for piece in pieces], axis=1)
    weight = jnp.concatenate([w[...] for w in weights], axis=0)
    sums = jnp.dot(rows, weight, preferred_element_type=f32)
    tile = sums.shape[1]
    mixed[2 * n] = sums[:, :WIDTH]
    mixed[2 * n + 1] = sums[:, WIDTH:]
    part = sum(sums[:, i : i + 128] * sums[:, i : i + 128] for i in range(0, tile, 128))

    @pl.when(n == 0)
    def _():
        squares[...] = part

    @pl.when(n > 0)
    def _():
        squares[...] += part

    @pl.when(n == pl.num_programs(0) - 1)
    def _():
        total = jnp.sum(squares[...], axis=-1, keepdims=True)
        factor = lax.rsqrt(total * (1.0 / (count * WIDTH)) + norm_eps)
        for k in range(count):
            value = (mixed[slot[k]] * factor * gain[slot[k]]).astype(bf16)
            if len(outs) == 1:
                outs[0][k] = value
            else:
                outs[k][...] = value


def project_out(split, order, slot, pieces, weights, gain):
    count = len(weights)
    pieces = list(pieces) if split else [pieces]
    rows = pieces[0].shape[-2]
    depth, width = weights[0].shape
    tile = 2 * WIDTH
    shape = (rows, WIDTH) if split else (count, rows, WIDTH)
    outs = pl.pallas_call(
        out_kernel,
        grid_spec=pltpu.PrefetchScalarGridSpec(
            num_scalar_prefetch=2,
            grid=(width // tile,),
            in_specs=[whole_block(*shape)] * len(pieces)
            + [pl.BlockSpec((depth, tile), lambda n, *_: (0, n))] * count
            + [whole_block(*gain.shape)],
            out_specs=[whole_block(*shape)] * len(pieces),
            scratch_shapes=[
                pltpu.VMEM((count, rows, WIDTH), f32),
                pltpu.VMEM((rows, 128), f32),
            ],
        ),
        out_shape=[jax.ShapeDtypeStruct(shape, bf16)] * len(pieces),
        compiler_params=pltpu.CompilerParams(vmem_limit_bytes=VMEM_LIMIT),
        cost_estimate=pl.CostEstimate(
            flops=2 * rows * width * width, bytes_accessed=12 << 20, transcendentals=0
        ),
        name="project_out",
    )(order, slot, *pieces, *weights, gain)
    return list(outs) if split else outs[0]


def place_kernel(order, whole, *rest):
    count = len(rest) - 2
    parts, out, sems = rest[:count], rest[count], rest[count + 1]
    copies = [pltpu.make_async_copy(whole, out.at[pl.ds(0, count)], sems.at[count])]
    for k in range(count):
        copies.append(pltpu.make_async_copy(parts[k], out.at[count + order[k]], sems.at[k]))
    for copy in copies:
        copy.start()
    for copy in copies:
        copy.wait()


def place(order, whole, parts):
    count = len(parts)
    shape = (2 * count,) + parts[0].shape
    anywhere = pl.BlockSpec(memory_space=pl.ANY)
    return pl.pallas_call(
        place_kernel,
        grid_spec=pltpu.PrefetchScalarGridSpec(
            num_scalar_prefetch=1,
            grid=(1,),
            in_specs=[anywhere] * (count + 1),
            out_specs=anywhere,
            scratch_shapes=[pltpu.SemaphoreType.DMA((count + 1,))],
        ),
        out_shape=jax.ShapeDtypeStruct(shape, bf16),
        compiler_params=pltpu.CompilerParams(vmem_limit_bytes=8 << 20),
        cost_estimate=pl.CostEstimate(flops=1 << 20, bytes_accessed=4 << 20, transcendentals=0),
        name="place",
    )(order, whole, *parts)


def exchange(pieces, axes):
    return lax.all_to_all(pieces, axes, split_axis=0, concat_axis=0, tiled=True)


def tied(*arrays):
    return lax.optimization_barrier(arrays)


def along_y(piece, shift):
    ring = lax.axis_size(TP[0])
    return lax.ppermute(piece, TP[0], [(i, (i + shift) % ring) for i in range(ring)])


def across(piece):
    return lax.ppermute(piece, TP[1], [(0, 1), (1, 0)])


def turned(blocks, here, step, axis):
    size = lax.axis_size(axis)
    mine = lax.dynamic_index_in_dim(blocks, (here + step) % size, 0, keepdims=False)
    if step == 0:
        return mine
    return lax.ppermute(mine, axis, [(i, (i + step) % size) for i in range(size)])


def both_cores(parts):
    same = jnp.stack(parts)
    return same, across(same)


OFFSETS = (0, -1, 1, 2)


def piece_order(sign):
    ring = lax.axis_size(TP[0])
    y = lax.axis_index(TP[0])
    c = lax.axis_index(TP[1])
    rows = jnp.stack([(y + ring + sign * d) % ring for d in OFFSETS])
    return jnp.concatenate([2 * rows + c, 2 * rows + 1 - c]).astype(jnp.int32)


def send_pieces(pieces):
    ring = lax.axis_size(TP[0])
    got = []
    for k in range(2 * ring):
        step, swap = OFFSETS[k % ring], k // ring
        pairs = [
            (2 * y + c, 2 * ((y - step) % ring) + (c + swap) % 2)
            for y in range(ring)
            for c in range(2)
        ]
        got.append(lax.ppermute(pieces[k], TP, pairs) if k else pieces[0])
    return got


def local(tokens, w_query, w_key, w_value, w_out, query_gain, key_gain, out_gain, chosen):
    length, _ = tokens.shape
    blocks_here = length // BLOCK
    devices = lax.axis_size(KV)
    position = lax.axis_index(KV)
    ranks = lax.axis_size(TP)
    key_row = key_gain[None, :]
    query_row = (query_gain * (HEAD_DIM ** (-0.5) * LOG2E))[None, :]

    rank = lax.axis_index(TP).astype(jnp.int32).reshape(1)
    shares = token_shares(rank, tokens, devices)
    chosen, shares = tied(chosen, shares)
    shares = exchange(shares, KV)[0]

    usable = chosen >= 0
    pick = jnp.where(usable, chosen, 0)
    owner_of = pick // blocks_here
    all_blocks = jnp.arange(devices * blocks_here, dtype=jnp.int32)
    marked = jnp.where(usable & (owner_of != position), chosen, -1)
    wanted = jnp.any(marked[:, :, None] == all_blocks[None, None, :], axis=(0, 1)).reshape(
        devices, blocks_here
    )
    rank_of = jnp.cumsum(wanted.astype(jnp.int32), axis=1) - 1
    local_ids = jnp.arange(blocks_here, dtype=jnp.int32)
    places = wanted[:, :, None] & (
        rank_of[:, :, None] == jnp.arange(HOT, dtype=jnp.int32)[None, None, :]
    )
    named = jnp.sum(jnp.where(places, local_ids[None, :, None], 0), axis=1).astype(jnp.int32)
    requests = jnp.concatenate([named, jnp.broadcast_to(named[:1], named.shape)], axis=1)
    order = piece_order(1)
    toward = piece_order(-1)
    same_order = jnp.arange(ranks, dtype=jnp.int32)

    long, side = lax.axis_size(KV[0]), lax.axis_size(KV[1])
    z, x = lax.axis_index(KV[0]), lax.axis_index(KV[1])
    by_row = requests.reshape(long, side, -1)
    rows_in = [turned(by_row, z, step, KV[0]) for step in range(long)]
    pairs = project_kv(tokens, w_key, w_value, key_row).reshape(-1, WIDTH)
    pairs, *rows_in = tied(pairs, *rows_in)
    by_side = jnp.stack(rows_in, axis=1)
    sides_in = [turned(by_side, x, step, KV[1]) for step in range(side)]
    asked = jnp.stack(sides_in, axis=1).reshape(devices, -1)
    sources = jnp.stack(
        [((z + long - s) % long) * side + (x + side - t) % side for s in range(long) for t in range(side)]
    )
    wheres = sources[None, :] == jnp.arange(devices, dtype=jnp.int32)[:, None]
    asked = jnp.sum(jnp.where(wheres[:, :, None], asked[None], 0), axis=1).astype(jnp.int32)
    asked_near = asked[:, :REACH].reshape(-1)
    asked_hot = asked[:, HOT:].reshape(-1)

    sent = gather_near(asked_near, pairs)
    sent, shares = tied(sent, shares)
    near = exchange(sent.reshape(devices, -1, WIDTH), KV).reshape(-1, WIDTH)
    parts = [shares] + [along_y(shares, shift) for shift in (1, -1, 2)]
    w_after = along_y(w_out, 1)
    w_before = along_y(w_out, -1)
    w_own = across(w_out)
    again, sent = tied(tokens, sent)
    queries = project_q(again, w_query, query_row)
    queries, *parts = tied(queries, *parts)
    rows_same, rows_other = both_cores(parts)
    sent_hot = project_sent(
        asked_hot, order, rows_same, rows_other, w_key, w_value, key_row, devices
    )
    pick, owner_of, rank_of, usable, sent_hot = tied(pick, owner_of, rank_of, usable, sent_hot)
    flat_rank = rank_of.reshape(-1)
    slot_rank = jnp.sum(
        jnp.where(pick[:, :, None] == all_blocks[None, None, :], flat_rank[None, None, :], 0), axis=-1
    )
    near_at = blocks_here + owner_of * REACH + slot_rank
    hot_at = blocks_here + devices * REACH + slot_rank
    at = jnp.where(
        owner_of == position, pick % blocks_here, jnp.where(owner_of == 0, hot_at, near_at)
    )
    at = jnp.where(usable, at, 0).astype(jnp.int32).reshape(-1)
    mask = jnp.repeat(usable.astype(f32), BLOCK, axis=1)

    near, sent_hot = tied(near, sent_hot)
    hot = exchange(sent_hot, KV)
    w_far = along_y(w_after, 1)
    w_swapped = [across(w_after), across(w_before)]
    w_swapped.append(across(w_far))
    weights = [w_out, w_after, w_before, w_far, w_own] + w_swapped

    gains = out_gain.reshape(ranks, 1, WIDTH)
    first = attend(0, 2, False, at, same_order, queries, mask, pairs, near, hot)
    first = exchange(first, TP)
    second = attend(1, 2, True, at, toward, queries, mask, pairs, near, hot)
    second = send_pieces(second)
    first = project_out(False, order, same_order, first, weights, gains)
    moved = exchange(first, TP)
    second = tied(first, *second)[1:]
    second = project_out(True, order, toward, second, weights, gains)
    second = send_pieces(second)
    return place(order, moved, second).reshape(length, WIDTH)


def solution(mesh):
    split = Mesh(mesh.devices.reshape(4, 4, 4, 2), KV + TP)
    return jax.shard_map(
        local,
        mesh=split,
        in_specs=(
            P(KV, None),
            P(None, TP),
            P(None, TP),
            P(None, TP),
            P(TP, None),
            P(),
            P(),
            P(),
            P(KV, None),
        ),
        out_specs=P(KV, TP),
        check_vma=False,
    )
```

```python
import functools

import jax
import jax.numpy as jnp
from jax import lax
from jax.experimental import pallas as pl
from jax.experimental.pallas import tpu as pltpu
from jax.sharding import Mesh
from jax.sharding import PartitionSpec as P

HEAD_DIM = 128
BLOCK = 64
HOT = 8
REACH = 2
FIRST_BLOCKS = 5
KV = ("kv_0", "kv_1")
TP = ("tp_0", "tp_1")
WIDTH = 256
PAIR = 2
norm_eps = 1e-06
LOG2E = 1.4426950408889634
bf16 = jnp.bfloat16
f32 = jnp.float32
VMEM_LIMIT = 60 * 1024 * 1024


def head_norm(values, gain_row):
    factor = lax.rsqrt(jnp.mean(values * values, axis=-1, keepdims=True) + norm_eps)
    return (values * factor * gain_row).astype(bf16)


def share_kernel(rank, tok, out):
    rows = tok[...].astype(f32)
    devices = out.shape[0]
    part = BLOCK // devices
    for k in range(out.shape[1] // 16):
        parts = []
        for b in range(16 // part):
            first = (k * (16 // part) + b) * BLOCK
            parts.append(rows[first : first + BLOCK].reshape(devices, part, WIDTH))
        out[:, k * 16 : (k + 1) * 16, :] = jnp.concatenate(parts, axis=1).astype(bf16)


def token_shares(rank, tokens, devices):
    length = tokens.shape[0]
    tile = 1024
    small = tile // devices
    return pl.pallas_call(
        share_kernel,
        grid_spec=pltpu.PrefetchScalarGridSpec(
            num_scalar_prefetch=1,
            grid=(length // tile,),
            in_specs=[pl.BlockSpec((tile, WIDTH), lambda i, rank: (i, rank[0]))],
            out_specs=pl.BlockSpec((devices, small, WIDTH), lambda i, rank: (0, i, 0)),
        ),
        out_shape=jax.ShapeDtypeStruct((devices, length // devices, WIDTH), bf16),
        compiler_params=pltpu.CompilerParams(vmem_limit_bytes=VMEM_LIMIT),
        cost_estimate=pl.CostEstimate(flops=1 << 20, bytes_accessed=4 << 20, transcendentals=0),
        name="token_shares",
    )(rank, tokens)


def kv_kernel(tok, wk, wv, gain, out):
    rows = tok[...]
    keys = jnp.dot(rows, wk[...], preferred_element_type=f32)
    blocks = out.shape[0]
    for h in range(2):
        lanes = slice(h * HEAD_DIM, (h + 1) * HEAD_DIM)
        normed = head_norm(keys[:, lanes], gain[...])
        out[:, 0, :, lanes] = normed.reshape(blocks, BLOCK, HEAD_DIM)
    vals = jnp.dot(rows, wv[...], preferred_element_type=f32).astype(bf16)
    out[:, 1, :, :] = vals.reshape(blocks, BLOCK, WIDTH)


def project_kv(tokens, w_key, w_value, gain):
    length, depth = tokens.shape
    tile = 1024
    blocks = tile // BLOCK
    return pl.pallas_call(
        kv_kernel,
        grid=(length // tile,),
        in_specs=[
            pl.BlockSpec((tile, depth), lambda i: (i, 0)),
            pl.BlockSpec((depth, WIDTH), lambda i: (0, 0)),
            pl.BlockSpec((depth, WIDTH), lambda i: (0, 0)),
            pl.BlockSpec((1, HEAD_DIM), lambda i: (0, 0)),
        ],
        out_specs=pl.BlockSpec((blocks, PAIR, BLOCK, WIDTH), lambda i: (i, 0, 0, 0)),
        out_shape=jax.ShapeDtypeStruct((length // BLOCK, PAIR, BLOCK, WIDTH), bf16),
        compiler_params=pltpu.CompilerParams(vmem_limit_bytes=VMEM_LIMIT),
        cost_estimate=pl.CostEstimate(
            flops=4 * length * depth * WIDTH, bytes_accessed=2 * length * depth, transcendentals=0
        ),
        name="project_kv",
    )(tokens, w_key, w_value, gain)


def q_kernel(tok, wq, gain, out):
    values = jnp.dot(tok[...], wq[...], preferred_element_type=f32)
    for h in range(2):
        lanes = slice(h * HEAD_DIM, (h + 1) * HEAD_DIM)
        out[:, lanes] = head_norm(values[:, lanes], gain[...])


def project_q(tokens, w_query, gain):
    length, depth = tokens.shape
    tile = 1024
    return pl.pallas_call(
        q_kernel,
        grid=(length // tile,),
        in_specs=[
            pl.BlockSpec((tile, depth), lambda i: (i, 0)),
            pl.BlockSpec((depth, WIDTH), lambda i: (0, 0)),
            pl.BlockSpec((1, HEAD_DIM), lambda i: (0, 0)),
        ],
        out_specs=pl.BlockSpec((tile, WIDTH), lambda i: (i, 0)),
        out_shape=jax.ShapeDtypeStruct((length, WIDTH), bf16),
        compiler_params=pltpu.CompilerParams(vmem_limit_bytes=VMEM_LIMIT),
        cost_estimate=pl.CostEstimate(
            flops=2 * length * depth * WIDTH, bytes_accessed=2 * length * depth, transcendentals=0
        ),
        name="project_q",
    )(tokens, w_query, gain)


def near_kernel(near, pairs, out, room, in_sems, out_sems):
    unit = PAIR * BLOCK
    coming, going = [], []
    for m in range(near.shape[0]):
        first = pl.multiple_of(near[m] * unit, unit)
        coming.append(
            pltpu.make_async_copy(pairs.at[pl.ds(first, unit)], room.at[m], in_sems.at[m])
        )
        going.append(pltpu.make_async_copy(room.at[m], out.at[m], out_sems.at[m]))
    for copy in coming:
        copy.start()
    for n, copy in enumerate(coming):
        copy.wait()
        going[n].start()
    for copy in going:
        copy.wait()


def gather_near(near, pairs):
    anywhere = pl.BlockSpec(memory_space=pl.ANY)
    sends = near.shape[0]
    return pl.pallas_call(
        near_kernel,
        grid_spec=pltpu.PrefetchScalarGridSpec(
            num_scalar_prefetch=1,
            grid=(1,),
            in_specs=[anywhere],
            out_specs=anywhere,
            scratch_shapes=[
                pltpu.VMEM((sends, PAIR * BLOCK, WIDTH), bf16),
                pltpu.SemaphoreType.DMA((sends,)),
                pltpu.SemaphoreType.DMA((sends,)),
            ],
        ),
        out_shape=jax.ShapeDtypeStruct((sends, PAIR * BLOCK, WIDTH), bf16),
        compiler_params=pltpu.CompilerParams(vmem_limit_bytes=VMEM_LIMIT),
        cost_estimate=pl.CostEstimate(flops=1 << 20, bytes_accessed=4 << 20, transcendentals=0),
        name="gather_near",
    )(near, pairs)


def send_kernel(asked, order, same, other, wk, wv, gain, out, keep):
    devices, rows, _ = out.shape
    keys = jnp.zeros((same.shape[1], WIDTH), f32)
    vals = jnp.zeros((same.shape[1], WIDTH), f32)
    count = same.shape[0]
    for k in range(2 * count):
        tokens = same[k] if k < count else other[k - count]
        span = pl.ds(pl.multiple_of(order[k] * WIDTH, WIDTH), WIDTH)
        keys += jnp.dot(tokens, wk[span, :], preferred_element_type=f32)
        vals += jnp.dot(tokens, wv[span, :], preferred_element_type=f32)
    groups, unit, _ = keep.shape
    part = unit // 2
    for h in range(2):
        lanes = slice(h * HEAD_DIM, (h + 1) * HEAD_DIM)
        x = keys[:, lanes]
        factor = lax.rsqrt(jnp.mean(x * x, axis=-1, keepdims=True) + norm_eps)
        keep[:, :part, lanes] = (x * factor * gain[...]).reshape(groups, part, HEAD_DIM)
    keep[:, part:, :] = vals.reshape(groups, part, WIDTH)

    twos = rows // (2 * unit)

    def one(m, carry):
        both = jnp.concatenate([keep[asked[2 * m]], keep[asked[2 * m + 1]]], axis=0)
        at = pl.multiple_of((m % twos) * 2 * unit, 2 * unit)
        out[m // twos, pl.ds(at, 2 * unit), :] = both.astype(bf16)
        return carry

    lax.fori_loop(0, devices * twos, one, 0, unroll=4)


def whole_block(*shape):
    return pl.BlockSpec(shape, lambda i, *_: (0,) * len(shape))


def project_sent(asked, order, same, other, w_key, w_value, gain, devices):
    count, rows, _ = same.shape
    groups = 64
    unit = 2 * rows // groups
    depth = w_key.shape[0]
    shape = (devices, (asked.shape[0] // devices) * unit, WIDTH)
    return pl.pallas_call(
        send_kernel,
        grid_spec=pltpu.PrefetchScalarGridSpec(
            num_scalar_prefetch=2,
            grid=(1,),
            in_specs=[
                whole_block(count, rows, WIDTH),
                whole_block(count, rows, WIDTH),
                whole_block(depth, WIDTH),
                whole_block(depth, WIDTH),
                whole_block(1, HEAD_DIM),
            ],
            out_specs=whole_block(*shape),
            scratch_shapes=[pltpu.VMEM((groups, unit, WIDTH), f32)],
        ),
        out_shape=jax.ShapeDtypeStruct(shape, bf16),
        compiler_params=pltpu.CompilerParams(vmem_limit_bytes=VMEM_LIMIT),
        cost_estimate=pl.CostEstimate(
            flops=4 * rows * depth * WIDTH, bytes_accessed=8 << 20, transcendentals=0
        ),
        name="project_sent",
    )(asked, order, same, other, w_key, w_value, gain)


def attention_kernel(first, at, where, queries, masks, pairs, near, hot, *rest):
    outs, (q, mask, table, raw, sems) = rest[:-5], rest[-5:]
    devices, hot_rows, _ = hot.shape
    here = pairs.shape[0]
    plain = near.shape[0]
    copies = [
        pltpu.make_async_copy(hot, raw, sems.at[0]),
        pltpu.make_async_copy(pairs, table.at[pl.ds(0, here)], sems.at[1]),
        pltpu.make_async_copy(near, table.at[pl.ds(here, plain)], sems.at[2]),
        pltpu.make_async_copy(queries.at[pl.ds(first * BLOCK, q.shape[0])], q, sems.at[3]),
        pltpu.make_async_copy(masks.at[pl.ds(first, mask.shape[0])], mask, sems.at[4]),
    ]
    for copy in copies:
        copy.start()
    copies[0].wait()
    part = BLOCK // devices
    for n in range(hot_rows // 16):
        both = raw[:, n * 16 : (n + 1) * 16, :].astype(f32)
        for m in range(2):
            start = here + plain + (2 * n + m) * PAIR * BLOCK
            for kind in range(PAIR):
                low = m * 2 * part + kind * part
                piece = both[:, low : low + part, :].reshape(BLOCK, WIDTH).astype(bf16)
                table[start + kind * BLOCK : start + (kind + 1) * BLOCK, :] = piece
    for copy in copies[1:]:
        copy.wait()
    slots = mask.shape[1] // BLOCK
    count = where.shape[0]
    whole = len(outs) == 1
    per_piece = mask.shape[0] // count
    blank = jnp.zeros((BLOCK, HEAD_DIM), bf16)

    def load(block):
        row = pl.multiple_of(block * BLOCK, BLOCK)
        rows = q[pl.ds(row, BLOCK), :]
        both = jnp.concatenate(
            [
                jnp.concatenate([rows[:, :HEAD_DIM], blank], axis=1),
                jnp.concatenate([blank, rows[:, HEAD_DIM:]], axis=1),
            ],
            axis=0,
        )
        base = (first + block) * slots
        return both, [
            pl.multiple_of(at[base + j] * PAIR * BLOCK, PAIR * BLOCK) for j in range(slots)
        ]

    def piece_of(n, put):
        items = [load(where[n] * per_piece + i) for i in range(per_piece)]
        logits = []
        for both, picks in items:
            keys = jnp.concatenate([table[pl.ds(p, BLOCK), :] for p in picks], axis=0)
            logits.append(
                lax.dot_general(both, keys, (((1,), (1,)), ((), ())), preferred_element_type=f32)
            )
        weights = []
        for i in range(per_piece):
            block = where[n] * per_piece + i
            weights.append(jnp.exp2(logits[i]) * mask[pl.ds(block, 1), :])
        for i, (both, picks) in enumerate(items):
            values = jnp.concatenate(
                [table[pl.ds(p + BLOCK, BLOCK), :] for p in picks], axis=0
            )
            sums = jnp.dot(weights[i].astype(bf16), values, preferred_element_type=f32)
            scale = 1.0 / jnp.sum(weights[i], axis=-1, keepdims=True)
            to = slice(i * BLOCK, (i + 1) * BLOCK)
            put(to, slice(0, HEAD_DIM), sums[:BLOCK, :HEAD_DIM] * scale[:BLOCK])
            put(to, slice(HEAD_DIM, WIDTH), sums[BLOCK:, HEAD_DIM:] * scale[BLOCK:])

    if whole:

        def one(n, carry):
            def put(rows, lanes, value):
                outs[0][n, rows, lanes] = value.astype(bf16)

            piece_of(n, put)
            return carry

        lax.fori_loop(0, count, one, 0)
    else:
        for n in range(count):

            def put(rows, lanes, value, n=n):
                outs[n][rows, lanes] = value.astype(bf16)

            piece_of(n, put)


def attend(first, blocks, split, at, where, queries, mask, pairs, near, hot):
    ranks = where.shape[0]
    length = blocks * BLOCK
    slots = mask.shape[1] // BLOCK
    rows = length // ranks
    anywhere = pl.BlockSpec(memory_space=pl.ANY)
    shape = (rows, WIDTH) if split else (ranks, rows, WIDTH)
    count = ranks if split else 1
    height = pairs.shape[0] + near.shape[0] + HOT * PAIR * BLOCK
    outs = pl.pallas_call(
        functools.partial(attention_kernel, first),
        grid_spec=pltpu.PrefetchScalarGridSpec(
            num_scalar_prefetch=2,
            grid=(1,),
            in_specs=[
                anywhere,
                anywhere,
                anywhere,
                anywhere,
                anywhere,
            ],
            out_specs=[whole_block(*shape)] * count,
            scratch_shapes=[
                pltpu.VMEM((length, WIDTH), bf16),
                pltpu.VMEM((blocks, slots * BLOCK), f32),
                pltpu.VMEM((height, WIDTH), bf16),
                pltpu.VMEM(hot.shape, bf16),
                pltpu.SemaphoreType.DMA((5,)),
            ],
        ),
        out_shape=[jax.ShapeDtypeStruct(shape, bf16)] * count,
        compiler_params=pltpu.CompilerParams(vmem_limit_bytes=VMEM_LIMIT),
        cost_estimate=pl.CostEstimate(
            flops=8 * length * WIDTH * slots * BLOCK, bytes_accessed=10 << 20, transcendentals=0
        ),
        name="attend",
    )(at, where, queries, mask, pairs, near, hot)
    return list(outs) if split else outs[0]


def out_kernel(order, slot, *refs):
    count = order.shape[0]
    n = pl.program_id(0)
    if len(refs) > 2 * count + 4:
        pieces, refs = refs[:count], refs[count:]
    else:
        pieces, refs = [refs[0].at[order[k]] for k in range(count)], refs[1:]
    weights, gain, refs = refs[:count], refs[count], refs[count + 1 :]
    outs, (mixed, squares) = refs[:-2], refs[-2:]
    rows = jnp.concatenate([piece[...] for piece in pieces], axis=1)
    weight = jnp.concatenate([w[...] for w in weights], axis=0)
    sums = jnp.dot(rows, weight, preferred_element_type=f32)
    tile = sums.shape[1]
    for i in range(tile // WIDTH):
        mixed[(tile // WIDTH) * n + i] = sums[:, i * WIDTH : (i + 1) * WIDTH]
    part = sum(sums[:, i : i + 128] * sums[:, i : i + 128] for i in range(0, tile, 128))

    @pl.when(n == 0)
    def _():
        squares[...] = part

    @pl.when(n > 0)
    def _():
        squares[...] += part

    @pl.when(n == pl.num_programs(0) - 1)
    def _():
        total = jnp.sum(squares[...], axis=-1, keepdims=True)
        factor = lax.rsqrt(total * (1.0 / (count * WIDTH)) + norm_eps)
        for k in range(count):
            value = (mixed[slot[k]] * factor * gain[slot[k]]).astype(bf16)
            if len(outs) == 1:
                outs[0][k] = value
            else:
                outs[k][...] = value


def project_out(split, order, slot, pieces, weights, gain):
    count = len(weights)
    pieces = list(pieces) if split else [pieces]
    rows = pieces[0].shape[-2]
    depth, width = weights[0].shape
    tile = 4 * WIDTH
    shape = (rows, WIDTH) if split else (count, rows, WIDTH)
    outs = pl.pallas_call(
        out_kernel,
        grid_spec=pltpu.PrefetchScalarGridSpec(
            num_scalar_prefetch=2,
            grid=(width // tile,),
            in_specs=[whole_block(*shape)] * len(pieces)
            + [pl.BlockSpec((depth, tile), lambda n, *_: (0, n))] * count
            + [whole_block(*gain.shape)],
            out_specs=[whole_block(*shape)] * len(pieces),
            scratch_shapes=[
                pltpu.VMEM((count, rows, WIDTH), f32),
                pltpu.VMEM((rows, 128), f32),
            ],
        ),
        out_shape=[jax.ShapeDtypeStruct(shape, bf16)] * len(pieces),
        compiler_params=pltpu.CompilerParams(vmem_limit_bytes=VMEM_LIMIT),
        cost_estimate=pl.CostEstimate(
            flops=2 * rows * width * width, bytes_accessed=12 << 20, transcendentals=0
        ),
        name="project_out",
    )(order, slot, *pieces, *weights, gain)
    return list(outs) if split else outs[0]


def place_kernel(order, whole, *rest):
    count = len(rest) - 2
    parts, out, sems = rest[:count], rest[count], rest[count + 1]
    rows = parts[0].shape[0]
    base = whole.shape[0]
    copies = [pltpu.make_async_copy(whole, out.at[pl.ds(0, base)], sems.at[count])]
    for k in range(count):
        to = pl.multiple_of(base + order[k] * rows, BLOCK)
        copies.append(pltpu.make_async_copy(parts[k], out.at[pl.ds(to, rows)], sems.at[k]))
    for copy in copies:
        copy.start()
    for copy in copies:
        copy.wait()


def place(order, whole, parts):
    count = len(parts)
    length = whole.shape[0] + count * parts[0].shape[0]
    anywhere = pl.BlockSpec(memory_space=pl.ANY)
    return pl.pallas_call(
        place_kernel,
        grid_spec=pltpu.PrefetchScalarGridSpec(
            num_scalar_prefetch=1,
            grid=(1,),
            in_specs=[anywhere] * (count + 1),
            out_specs=anywhere,
            scratch_shapes=[pltpu.SemaphoreType.DMA((count + 1,))],
        ),
        out_shape=jax.ShapeDtypeStruct((length, WIDTH), bf16),
        compiler_params=pltpu.CompilerParams(vmem_limit_bytes=8 << 20),
        cost_estimate=pl.CostEstimate(flops=1 << 20, bytes_accessed=4 << 20, transcendentals=0),
        name="place",
    )(order, whole, *parts)


def exchange(pieces, axes):
    return lax.all_to_all(pieces, axes, split_axis=0, concat_axis=0, tiled=True)


def tied(*arrays):
    return lax.optimization_barrier(arrays)


def along_y(piece, shift):
    ring = lax.axis_size(TP[0])
    return lax.ppermute(piece, TP[0], [(i, (i + shift) % ring) for i in range(ring)])


def across(piece):
    return lax.ppermute(piece, TP[1], [(0, 1), (1, 0)])


def turned(blocks, here, step, axis):
    size = lax.axis_size(axis)
    mine = lax.dynamic_index_in_dim(blocks, (here + step) % size, 0, keepdims=False)
    if step == 0:
        return mine
    return lax.ppermute(mine, axis, [(i, (i + step) % size) for i in range(size)])


def both_cores(parts):
    same = jnp.stack(parts)
    return same, across(same)


OFFSETS = (0, -1, 1, 2)


def piece_order(sign):
    ring = lax.axis_size(TP[0])
    y = lax.axis_index(TP[0])
    c = lax.axis_index(TP[1])
    rows = jnp.stack([(y + ring + sign * d) % ring for d in OFFSETS])
    return jnp.concatenate([2 * rows + c, 2 * rows + 1 - c]).astype(jnp.int32)


def send_pieces(pieces):
    ring = lax.axis_size(TP[0])
    got = []
    for k in range(2 * ring):
        step, swap = OFFSETS[k % ring], k // ring
        pairs = [
            (2 * y + c, 2 * ((y - step) % ring) + (c + swap) % 2)
            for y in range(ring)
            for c in range(2)
        ]
        got.append(lax.ppermute(pieces[k], TP, pairs) if k else pieces[0])
    return got


def local(tokens, w_query, w_key, w_value, w_out, query_gain, key_gain, out_gain, chosen):
    length, _ = tokens.shape
    blocks_here = length // BLOCK
    devices = lax.axis_size(KV)
    position = lax.axis_index(KV)
    ranks = lax.axis_size(TP)
    key_row = key_gain[None, :]
    query_row = (query_gain * (HEAD_DIM ** (-0.5) * LOG2E))[None, :]

    rank = lax.axis_index(TP).astype(jnp.int32).reshape(1)
    shares = token_shares(rank, tokens, devices)
    chosen, shares = tied(chosen, shares)
    shares = exchange(shares, KV)[0]

    usable = chosen >= 0
    pick = jnp.where(usable, chosen, 0)
    owner_of = pick // blocks_here
    all_blocks = jnp.arange(devices * blocks_here, dtype=jnp.int32)
    marked = jnp.where(usable & (owner_of != position), chosen, -1)
    wanted = jnp.any(marked[:, :, None] == all_blocks[None, None, :], axis=(0, 1)).reshape(
        devices, blocks_here
    )
    rank_of = jnp.cumsum(wanted.astype(jnp.int32), axis=1) - 1
    local_ids = jnp.arange(blocks_here, dtype=jnp.int32)
    places = wanted[:, :, None] & (
        rank_of[:, :, None] == jnp.arange(HOT, dtype=jnp.int32)[None, None, :]
    )
    named = jnp.sum(jnp.where(places, local_ids[None, :, None], 0), axis=1).astype(jnp.int32)
    requests = jnp.concatenate([named, jnp.broadcast_to(named[:1], named.shape)], axis=1)
    order = piece_order(1)
    toward = piece_order(-1)
    same_order = jnp.arange(ranks, dtype=jnp.int32)

    long, side = lax.axis_size(KV[0]), lax.axis_size(KV[1])
    z, x = lax.axis_index(KV[0]), lax.axis_index(KV[1])
    by_row = requests.reshape(long, side, -1)
    rows_in = [turned(by_row, z, step, KV[0]) for step in range(long)]
    by_side = jnp.stack(rows_in, axis=1)
    sides_in = [turned(by_side, x, step, KV[1]) for step in range(side)]
    pairs = project_kv(tokens, w_key, w_value, key_row).reshape(-1, WIDTH)
    pairs, *sides_in = tied(pairs, *sides_in)
    asked = jnp.stack(sides_in, axis=1).reshape(devices, -1)
    sources = jnp.stack(
        [((z + long - s) % long) * side + (x + side - t) % side for s in range(long) for t in range(side)]
    )
    wheres = sources[None, :] == jnp.arange(devices, dtype=jnp.int32)[:, None]
    asked = jnp.sum(jnp.where(wheres[:, :, None], asked[None], 0), axis=1).astype(jnp.int32)
    asked_near = asked[:, :REACH].reshape(-1)
    asked_hot = asked[:, HOT:].reshape(-1)

    sent = gather_near(asked_near, pairs)
    sent, shares = tied(sent, shares)
    near = exchange(sent.reshape(devices, -1, WIDTH), KV).reshape(-1, WIDTH)
    parts = [shares] + [along_y(shares, shift) for shift in (1, -1, 2)]
    w_after = along_y(w_out, 1)
    w_before = along_y(w_out, -1)
    w_own = across(w_out)
    again, sent = tied(tokens, sent)
    queries = project_q(again, w_query, query_row)
    queries, *parts = tied(queries, *parts)
    rows_same, rows_other = both_cores(parts)
    sent_hot = project_sent(
        asked_hot, order, rows_same, rows_other, w_key, w_value, key_row, devices
    )
    pick, owner_of, rank_of, usable, sent_hot = tied(pick, owner_of, rank_of, usable, sent_hot)
    flat_rank = rank_of.reshape(-1)
    slot_rank = jnp.sum(
        jnp.where(pick[:, :, None] == all_blocks[None, None, :], flat_rank[None, None, :], 0), axis=-1
    )
    near_at = blocks_here + owner_of * REACH + slot_rank
    hot_at = blocks_here + devices * REACH + slot_rank
    at = jnp.where(
        owner_of == position, pick % blocks_here, jnp.where(owner_of == 0, hot_at, near_at)
    )
    at = jnp.where(usable, at, 0).astype(jnp.int32).reshape(-1)
    mask = jnp.repeat(usable.astype(f32), BLOCK, axis=1)

    at, mask, order, toward, same_order, sent_hot = tied(
        at, mask, order, toward, same_order, sent_hot
    )
    near, sent_hot = tied(near, sent_hot)
    hot = exchange(sent_hot, KV)
    w_far = along_y(w_after, 1)
    w_swapped = [across(w_after), across(w_before)]
    w_swapped.append(across(w_far))
    weights = [w_out, w_after, w_before, w_far, w_own] + w_swapped

    gains = out_gain.reshape(ranks, 1, WIDTH)
    early = (FIRST_BLOCKS * blocks_here) // 8
    first = attend(0, early, False, at, same_order, queries, mask, pairs, near, hot)
    first = exchange(first, TP)
    second = attend(early, blocks_here - early, True, at, toward, queries, mask, pairs, near, hot)
    second = send_pieces(second)
    first = project_out(False, order, same_order, first, weights, gains)
    moved = exchange(first, TP)
    second = tied(first, *second)[1:]
    second = project_out(True, order, toward, second, weights, gains)
    second = send_pieces(second)
    return place(order, moved.reshape(-1, WIDTH), second)


def solution(mesh):
    split = Mesh(mesh.devices.reshape(4, 4, 4, 2), KV + TP)
    return jax.shard_map(
        local,
        mesh=split,
        in_specs=(
            P(KV, None),
            P(None, TP),
            P(None, TP),
            P(None, TP),
            P(TP, None),
            P(),
            P(),
            P(),
            P(KV, None),
        ),
        out_specs=P(KV, TP),
        check_vma=False,
    )
```

```python
import functools

import jax
import jax.numpy as jnp
from jax import lax
from jax.experimental import pallas as pl
from jax.experimental.pallas import tpu as pltpu
from jax.sharding import Mesh
from jax.sharding import PartitionSpec as P

HEAD_DIM = 128
BLOCK = 64
HOT = 8
REACH = 2
FIRST_BLOCKS = 4
KV = ("kv_0", "kv_1")
TP = ("tp_0", "tp_1")
WIDTH = 256
PAIR = 2
norm_eps = 1e-06
LOG2E = 1.4426950408889634
bf16 = jnp.bfloat16
f32 = jnp.float32
VMEM_LIMIT = 60 * 1024 * 1024


def head_norm(values, gain_row):
    factor = lax.rsqrt(jnp.mean(values * values, axis=-1, keepdims=True) + norm_eps)
    return (values * factor * gain_row).astype(bf16)


def share_kernel(rank, tok, *outs):
    rows = tok[...].astype(f32)
    side, small, _ = outs[0].shape
    devices = len(outs) * side
    part = BLOCK // devices
    for k in range(small // 16):
        parts = []
        for b in range(16 // part):
            first = (k * (16 // part) + b) * BLOCK
            parts.append(rows[first : first + BLOCK].reshape(devices, part, WIDTH))
        joined = jnp.concatenate(parts, axis=1).astype(bf16)
        for n, out in enumerate(outs):
            out[:, k * 16 : (k + 1) * 16, :] = joined[n * side : (n + 1) * side]


def token_shares(rank, tokens, long, side):
    length = tokens.shape[0]
    devices = long * side
    tile = 1024
    return pl.pallas_call(
        share_kernel,
        grid_spec=pltpu.PrefetchScalarGridSpec(
            num_scalar_prefetch=1,
            grid=(length // tile,),
            in_specs=[pl.BlockSpec((tile, WIDTH), lambda i, rank: (i, rank[0]))],
            out_specs=[pl.BlockSpec((side, tile // devices, WIDTH), lambda i, rank: (0, i, 0))] * long,
        ),
        out_shape=[jax.ShapeDtypeStruct((side, length // devices, WIDTH), bf16)] * long,
        compiler_params=pltpu.CompilerParams(vmem_limit_bytes=VMEM_LIMIT),
        cost_estimate=pl.CostEstimate(flops=1 << 20, bytes_accessed=4 << 20, transcendentals=0),
        name="token_shares",
    )(rank, tokens)


def kv_kernel(tok, wk, wv, gain, out):
    rows = tok[...]
    keys = jnp.dot(rows, wk[...], preferred_element_type=f32)
    blocks = out.shape[0]
    for h in range(2):
        lanes = slice(h * HEAD_DIM, (h + 1) * HEAD_DIM)
        normed = head_norm(keys[:, lanes], gain[...])
        out[:, 0, :, lanes] = normed.reshape(blocks, BLOCK, HEAD_DIM)
    vals = jnp.dot(rows, wv[...], preferred_element_type=f32).astype(bf16)
    out[:, 1, :, :] = vals.reshape(blocks, BLOCK, WIDTH)


def project_kv(tokens, w_key, w_value, gain):
    length, depth = tokens.shape
    tile = 1024
    blocks = tile // BLOCK
    return pl.pallas_call(
        kv_kernel,
        grid=(length // tile,),
        in_specs=[
            pl.BlockSpec((tile, depth), lambda i: (i, 0)),
            pl.BlockSpec((depth, WIDTH), lambda i: (0, 0)),
            pl.BlockSpec((depth, WIDTH), lambda i: (0, 0)),
            pl.BlockSpec((1, HEAD_DIM), lambda i: (0, 0)),
        ],
        out_specs=pl.BlockSpec((blocks, PAIR, BLOCK, WIDTH), lambda i: (i, 0, 0, 0)),
        out_shape=jax.ShapeDtypeStruct((length // BLOCK, PAIR, BLOCK, WIDTH), bf16),
        compiler_params=pltpu.CompilerParams(vmem_limit_bytes=VMEM_LIMIT),
        cost_estimate=pl.CostEstimate(
            flops=4 * length * depth * WIDTH, bytes_accessed=2 * length * depth, transcendentals=0
        ),
        name="project_kv",
    )(tokens, w_key, w_value, gain)


def q_kernel(tok, wq, gain, out):
    values = jnp.dot(tok[...], wq[...], preferred_element_type=f32)
    for h in range(2):
        lanes = slice(h * HEAD_DIM, (h + 1) * HEAD_DIM)
        out[:, lanes] = head_norm(values[:, lanes], gain[...])


def project_q(tokens, w_query, gain):
    length, depth = tokens.shape
    tile = 1024
    return pl.pallas_call(
        q_kernel,
        grid=(length // tile,),
        in_specs=[
            pl.BlockSpec((tile, depth), lambda i: (i, 0)),
            pl.BlockSpec((depth, WIDTH), lambda i: (0, 0)),
            pl.BlockSpec((1, HEAD_DIM), lambda i: (0, 0)),
        ],
        out_specs=pl.BlockSpec((tile, WIDTH), lambda i: (i, 0)),
        out_shape=jax.ShapeDtypeStruct((length, WIDTH), bf16),
        compiler_params=pltpu.CompilerParams(vmem_limit_bytes=VMEM_LIMIT),
        cost_estimate=pl.CostEstimate(
            flops=2 * length * depth * WIDTH, bytes_accessed=2 * length * depth, transcendentals=0
        ),
        name="project_q",
    )(tokens, w_query, gain)


def near_kernel(near, pairs, out, room, in_sems, out_sems):
    unit = PAIR * BLOCK
    coming, going = [], []
    for m in range(near.shape[0]):
        first = pl.multiple_of(near[m] * unit, unit)
        coming.append(
            pltpu.make_async_copy(pairs.at[pl.ds(first, unit)], room.at[m], in_sems.at[m])
        )
        going.append(pltpu.make_async_copy(room.at[m], out.at[m], out_sems.at[m]))
    for copy in coming:
        copy.start()
    for n, copy in enumerate(coming):
        copy.wait()
        going[n].start()
    for copy in going:
        copy.wait()


def gather_near(near, pairs):
    anywhere = pl.BlockSpec(memory_space=pl.ANY)
    sends = near.shape[0]
    return pl.pallas_call(
        near_kernel,
        grid_spec=pltpu.PrefetchScalarGridSpec(
            num_scalar_prefetch=1,
            grid=(1,),
            in_specs=[anywhere],
            out_specs=anywhere,
            scratch_shapes=[
                pltpu.VMEM((sends, PAIR * BLOCK, WIDTH), bf16),
                pltpu.SemaphoreType.DMA((sends,)),
                pltpu.SemaphoreType.DMA((sends,)),
            ],
        ),
        out_shape=jax.ShapeDtypeStruct((sends, PAIR * BLOCK, WIDTH), bf16),
        compiler_params=pltpu.CompilerParams(vmem_limit_bytes=VMEM_LIMIT),
        cost_estimate=pl.CostEstimate(flops=1 << 20, bytes_accessed=4 << 20, transcendentals=0),
        name="gather_near",
    )(near, pairs)


def send_kernel(asked, order, same, other, wk, wv, gain, out, keep):
    devices, rows, _ = out.shape
    keys = jnp.zeros((same.shape[1], WIDTH), f32)
    vals = jnp.zeros((same.shape[1], WIDTH), f32)
    count = same.shape[0]
    for k in range(2 * count):
        tokens = same[k] if k < count else other[k - count]
        span = pl.ds(pl.multiple_of(order[k] * WIDTH, WIDTH), WIDTH)
        keys += jnp.dot(tokens, wk[span, :], preferred_element_type=f32)
        vals += jnp.dot(tokens, wv[span, :], preferred_element_type=f32)
    groups, unit, _ = keep.shape
    part = unit // 2
    for h in range(2):
        lanes = slice(h * HEAD_DIM, (h + 1) * HEAD_DIM)
        x = keys[:, lanes]
        factor = lax.rsqrt(jnp.mean(x * x, axis=-1, keepdims=True) + norm_eps)
        keep[:, :part, lanes] = (x * factor * gain[...]).reshape(groups, part, HEAD_DIM)
    keep[:, part:, :] = vals.reshape(groups, part, WIDTH)

    twos = rows // (2 * unit)

    def one(m, carry):
        both = jnp.concatenate([keep[asked[2 * m]], keep[asked[2 * m + 1]]], axis=0)
        at = pl.multiple_of((m % twos) * 2 * unit, 2 * unit)
        out[m // twos, pl.ds(at, 2 * unit), :] = both.astype(bf16)
        return carry

    lax.fori_loop(0, devices * twos, one, 0, unroll=4)


def whole_block(*shape):
    return pl.BlockSpec(shape, lambda i, *_: (0,) * len(shape))


def project_sent(asked, order, same, other, w_key, w_value, gain, devices):
    count, rows, _ = same.shape
    groups = 64
    unit = 2 * rows // groups
    depth = w_key.shape[0]
    shape = (devices, (asked.shape[0] // devices) * unit, WIDTH)
    return pl.pallas_call(
        send_kernel,
        grid_spec=pltpu.PrefetchScalarGridSpec(
            num_scalar_prefetch=2,
            grid=(1,),
            in_specs=[
                whole_block(count, rows, WIDTH),
                whole_block(count, rows, WIDTH),
                whole_block(depth, WIDTH),
                whole_block(depth, WIDTH),
                whole_block(1, HEAD_DIM),
            ],
            out_specs=whole_block(*shape),
            scratch_shapes=[pltpu.VMEM((groups, unit, WIDTH), f32)],
        ),
        out_shape=jax.ShapeDtypeStruct(shape, bf16),
        compiler_params=pltpu.CompilerParams(vmem_limit_bytes=VMEM_LIMIT),
        cost_estimate=pl.CostEstimate(
            flops=4 * rows * depth * WIDTH, bytes_accessed=8 << 20, transcendentals=0
        ),
        name="project_sent",
    )(asked, order, same, other, w_key, w_value, gain)


def attention_kernel(first, at, where, queries, masks, pairs, near, hot, *rest):
    outs, (q, mask, table, raw, sems) = rest[:-5], rest[-5:]
    devices, hot_rows, _ = hot.shape
    here = pairs.shape[0]
    plain = near.shape[0]
    copies = [
        pltpu.make_async_copy(hot, raw, sems.at[0]),
        pltpu.make_async_copy(pairs, table.at[pl.ds(0, here)], sems.at[1]),
        pltpu.make_async_copy(near, table.at[pl.ds(here, plain)], sems.at[2]),
        pltpu.make_async_copy(queries.at[pl.ds(first * BLOCK, q.shape[0])], q, sems.at[3]),
        pltpu.make_async_copy(masks.at[pl.ds(first, mask.shape[0])], mask, sems.at[4]),
    ]
    for copy in copies:
        copy.start()
    copies[0].wait()
    part = BLOCK // devices
    for n in range(hot_rows // 16):
        both = raw[:, n * 16 : (n + 1) * 16, :].astype(f32)
        for m in range(2):
            start = here + plain + (2 * n + m) * PAIR * BLOCK
            for kind in range(PAIR):
                low = m * 2 * part + kind * part
                piece = both[:, low : low + part, :].reshape(BLOCK, WIDTH).astype(bf16)
                table[start + kind * BLOCK : start + (kind + 1) * BLOCK, :] = piece
    for copy in copies[1:]:
        copy.wait()
    slots = mask.shape[1] // BLOCK
    count = where.shape[0]
    whole = len(outs) == 1
    per_piece = mask.shape[0] // count
    blank = jnp.zeros((BLOCK, HEAD_DIM), bf16)

    def load(block):
        row = pl.multiple_of(block * BLOCK, BLOCK)
        rows = q[pl.ds(row, BLOCK), :]
        both = jnp.concatenate(
            [
                jnp.concatenate([rows[:, :HEAD_DIM], blank], axis=1),
                jnp.concatenate([blank, rows[:, HEAD_DIM:]], axis=1),
            ],
            axis=0,
        )
        base = (first + block) * slots
        return both, [
            pl.multiple_of(at[base + j] * PAIR * BLOCK, PAIR * BLOCK) for j in range(slots)
        ]

    def piece_of(n, put):
        items = [load(where[n] * per_piece + i) for i in range(per_piece)]
        logits = []
        for both, picks in items:
            keys = jnp.concatenate([table[pl.ds(p, BLOCK), :] for p in picks], axis=0)
            logits.append(
                lax.dot_general(both, keys, (((1,), (1,)), ((), ())), preferred_element_type=f32)
            )
        weights = []
        for i in range(per_piece):
            block = where[n] * per_piece + i
            weights.append(jnp.exp2(logits[i]) * mask[pl.ds(block, 1), :])
        for i, (both, picks) in enumerate(items):
            values = jnp.concatenate(
                [table[pl.ds(p + BLOCK, BLOCK), :] for p in picks], axis=0
            )
            sums = jnp.dot(weights[i].astype(bf16), values, preferred_element_type=f32)
            scale = 1.0 / jnp.sum(weights[i], axis=-1, keepdims=True)
            to = slice(i * BLOCK, (i + 1) * BLOCK)
            put(to, slice(0, HEAD_DIM), sums[:BLOCK, :HEAD_DIM] * scale[:BLOCK])
            put(to, slice(HEAD_DIM, WIDTH), sums[BLOCK:, HEAD_DIM:] * scale[BLOCK:])

    if whole:

        def one(n, carry):
            def put(rows, lanes, value):
                outs[0][n, rows, lanes] = value.astype(bf16)

            piece_of(n, put)
            return carry

        lax.fori_loop(0, count, one, 0)
    else:
        for n in range(count):

            def put(rows, lanes, value, n=n):
                outs[n][rows, lanes] = value.astype(bf16)

            piece_of(n, put)


def attend(first, blocks, split, at, where, queries, mask, pairs, near, hot):
    ranks = where.shape[0]
    length = blocks * BLOCK
    slots = mask.shape[1] // BLOCK
    rows = length // ranks
    anywhere = pl.BlockSpec(memory_space=pl.ANY)
    shape = (rows, WIDTH) if split else (ranks, rows, WIDTH)
    count = ranks if split else 1
    height = pairs.shape[0] + near.shape[0] + HOT * PAIR * BLOCK
    outs = pl.pallas_call(
        functools.partial(attention_kernel, first),
        grid_spec=pltpu.PrefetchScalarGridSpec(
            num_scalar_prefetch=2,
            grid=(1,),
            in_specs=[
                anywhere,
                anywhere,
                anywhere,
                anywhere,
                anywhere,
            ],
            out_specs=[whole_block(*shape)] * count,
            scratch_shapes=[
                pltpu.VMEM((length, WIDTH), bf16),
                pltpu.VMEM((blocks, slots * BLOCK), f32),
                pltpu.VMEM((height, WIDTH), bf16),
                pltpu.VMEM(hot.shape, bf16),
                pltpu.SemaphoreType.DMA((5,)),
            ],
        ),
        out_shape=[jax.ShapeDtypeStruct(shape, bf16)] * count,
        compiler_params=pltpu.CompilerParams(vmem_limit_bytes=VMEM_LIMIT),
        cost_estimate=pl.CostEstimate(
            flops=8 * length * WIDTH * slots * BLOCK, bytes_accessed=10 << 20, transcendentals=0
        ),
        name="attend",
    )(at, where, queries, mask, pairs, near, hot)
    return list(outs) if split else outs[0]


def out_kernel(order, slot, *refs):
    count = order.shape[0]
    n = pl.program_id(0)
    if len(refs) > 2 * count + 4:
        pieces, refs = refs[:count], refs[count:]
    else:
        pieces, refs = [refs[0].at[order[k]] for k in range(count)], refs[1:]
    weights, gain, refs = refs[:count], refs[count], refs[count + 1 :]
    outs, (mixed, squares) = refs[:-2], refs[-2:]
    rows = jnp.concatenate([piece[...] for piece in pieces], axis=1)
    weight = jnp.concatenate([w[...] for w in weights], axis=0)
    sums = jnp.dot(rows, weight, preferred_element_type=f32)
    tile = sums.shape[1]
    for i in range(tile // WIDTH):
        mixed[(tile // WIDTH) * n + i] = sums[:, i * WIDTH : (i + 1) * WIDTH]
    part = sum(sums[:, i : i + 128] * sums[:, i : i + 128] for i in range(0, tile, 128))

    @pl.when(n == 0)
    def _():
        squares[...] = part

    @pl.when(n > 0)
    def _():
        squares[...] += part

    @pl.when(n == pl.num_programs(0) - 1)
    def _():
        total = jnp.sum(squares[...], axis=-1, keepdims=True)
        factor = lax.rsqrt(total * (1.0 / (count * WIDTH)) + norm_eps)
        for k in range(count):
            value = (mixed[slot[k]] * factor * gain[slot[k]]).astype(bf16)
            if len(outs) == 1:
                outs[0][k] = value
            else:
                outs[k][...] = value


def project_out(split, order, slot, pieces, weights, gain):
    count = len(weights)
    pieces = list(pieces) if split else [pieces]
    rows = pieces[0].shape[-2]
    depth, width = weights[0].shape
    tile = 4 * WIDTH
    shape = (rows, WIDTH) if split else (count, rows, WIDTH)
    outs = pl.pallas_call(
        out_kernel,
        grid_spec=pltpu.PrefetchScalarGridSpec(
            num_scalar_prefetch=2,
            grid=(width // tile,),
            in_specs=[whole_block(*shape)] * len(pieces)
            + [pl.BlockSpec((depth, tile), lambda n, *_: (0, n))] * count
            + [whole_block(*gain.shape)],
            out_specs=[whole_block(*shape)] * len(pieces),
            scratch_shapes=[
                pltpu.VMEM((count, rows, WIDTH), f32),
                pltpu.VMEM((rows, 128), f32),
            ],
        ),
        out_shape=[jax.ShapeDtypeStruct(shape, bf16)] * len(pieces),
        compiler_params=pltpu.CompilerParams(vmem_limit_bytes=VMEM_LIMIT),
        cost_estimate=pl.CostEstimate(
            flops=2 * rows * width * width, bytes_accessed=12 << 20, transcendentals=0
        ),
        name="project_out",
    )(order, slot, *pieces, *weights, gain)
    return list(outs) if split else outs[0]


def place_kernel(order, whole, *rest):
    count = len(rest) - 2
    parts, out, sems = rest[:count], rest[count], rest[count + 1]
    rows = parts[0].shape[0]
    base = whole.shape[0]
    copies = [pltpu.make_async_copy(whole, out.at[pl.ds(0, base)], sems.at[count])]
    for k in range(count):
        to = pl.multiple_of(base + order[k] * rows, BLOCK)
        copies.append(pltpu.make_async_copy(parts[k], out.at[pl.ds(to, rows)], sems.at[k]))
    for copy in copies:
        copy.start()
    for copy in copies:
        copy.wait()


def place(order, whole, parts):
    count = len(parts)
    length = whole.shape[0] + count * parts[0].shape[0]
    anywhere = pl.BlockSpec(memory_space=pl.ANY)
    return pl.pallas_call(
        place_kernel,
        grid_spec=pltpu.PrefetchScalarGridSpec(
            num_scalar_prefetch=1,
            grid=(1,),
            in_specs=[anywhere] * (count + 1),
            out_specs=anywhere,
            scratch_shapes=[pltpu.SemaphoreType.DMA((count + 1,))],
        ),
        out_shape=jax.ShapeDtypeStruct((length, WIDTH), bf16),
        compiler_params=pltpu.CompilerParams(vmem_limit_bytes=8 << 20),
        cost_estimate=pl.CostEstimate(flops=1 << 20, bytes_accessed=4 << 20, transcendentals=0),
        name="place",
    )(order, whole, *parts)


def exchange(pieces, axes):
    return lax.all_to_all(pieces, axes, split_axis=0, concat_axis=0, tiled=True)


def tied(*arrays):
    return lax.optimization_barrier(arrays)


def along_y(piece, shift):
    ring = lax.axis_size(TP[0])
    return lax.ppermute(piece, TP[0], [(i, (i + shift) % ring) for i in range(ring)])


def across(piece):
    return lax.ppermute(piece, TP[1], [(0, 1), (1, 0)])


def chosen_of(options, index):
    result = options[0]
    for n, option in enumerate(options[1:], 1):
        result = jnp.where(index == n, option, result)
    return result


def both_cores(parts):
    same = jnp.stack(parts)
    return same, across(same)


OFFSETS = (0, -1, 1, 2)


def piece_order(sign):
    ring = lax.axis_size(TP[0])
    y = lax.axis_index(TP[0])
    c = lax.axis_index(TP[1])
    rows = jnp.stack([(y + ring + sign * d) % ring for d in OFFSETS])
    return jnp.concatenate([2 * rows + c, 2 * rows + 1 - c]).astype(jnp.int32)


def send_pieces(pieces):
    ring = lax.axis_size(TP[0])
    got = []
    for k in range(2 * ring):
        step, swap = OFFSETS[k % ring], k // ring
        pairs = [
            (2 * y + c, 2 * ((y - step) % ring) + (c + swap) % 2)
            for y in range(ring)
            for c in range(2)
        ]
        got.append(lax.ppermute(pieces[k], TP, pairs) if k else pieces[0])
    return got


def local(tokens, w_query, w_key, w_value, w_out, query_gain, key_gain, out_gain, chosen):
    length, _ = tokens.shape
    blocks_here = length // BLOCK
    devices = lax.axis_size(KV)
    position = lax.axis_index(KV)
    ranks = lax.axis_size(TP)
    key_row = key_gain[None, :]
    query_row = (query_gain * (HEAD_DIM ** (-0.5) * LOG2E))[None, :]

    rank = lax.axis_index(TP).astype(jnp.int32).reshape(1)
    long, side = lax.axis_size(KV[0]), lax.axis_size(KV[1])
    z, x = lax.axis_index(KV[0]), lax.axis_index(KV[1])
    columns = token_shares(rank, tokens, long, side)
    chosen, *columns = tied(chosen, *columns)
    columns = columns[:1] + [lax.ppermute(columns[n], KV, [(0, n * side)]) for n in range(1, long)]

    usable = chosen >= 0
    pick = jnp.where(usable, chosen, 0)
    owner_of = pick // blocks_here
    all_blocks = jnp.arange(devices * blocks_here, dtype=jnp.int32)
    marked = jnp.where(usable & (owner_of != position), chosen, -1)
    wanted = jnp.any(marked[:, :, None] == all_blocks[None, None, :], axis=(0, 1)).reshape(
        devices, blocks_here
    )
    rank_of = jnp.cumsum(wanted.astype(jnp.int32), axis=1) - 1
    local_ids = jnp.arange(blocks_here, dtype=jnp.int32)
    places = wanted[:, :, None] & (
        rank_of[:, :, None] == jnp.arange(HOT, dtype=jnp.int32)[None, None, :]
    )
    named = jnp.sum(jnp.where(places, local_ids[None, :, None], 0), axis=1).astype(jnp.int32)
    requests = jnp.concatenate([named, jnp.broadcast_to(named[:1], named.shape)], axis=1)
    order = piece_order(1)
    toward = piece_order(-1)
    same_order = jnp.arange(ranks, dtype=jnp.int32)

    asked = exchange(requests, KV)
    pairs = project_kv(tokens, w_key, w_value, key_row).reshape(-1, WIDTH)
    asked_near = asked[:, :REACH].reshape(-1)
    asked_hot = asked[:, HOT:].reshape(-1)

    sent = gather_near(asked_near, pairs)
    sent, *columns = tied(sent, *columns)
    held = [chosen_of([c[n] for c in columns], z) for n in range(side)]
    starts = range(0, devices, side)
    held = held[:1] + [
        lax.ppermute(held[n], KV, [(i, i + n) for i in starts]) for n in range(1, side)
    ]
    near = exchange(sent.reshape(devices, -1, WIDTH), KV).reshape(-1, WIDTH)
    again, sent = tied(tokens, sent)
    queries = project_q(again, w_query, query_row)
    queries, *held = tied(queries, *held)
    shares = chosen_of(held, x)
    parts = [shares] + [along_y(shares, shift) for shift in (1, -1, 2)]
    w_after = along_y(w_out, 1)
    w_before = along_y(w_out, -1)
    w_own = across(w_out)
    rows_same, rows_other = both_cores(parts)
    sent_hot = project_sent(
        asked_hot, order, rows_same, rows_other, w_key, w_value, key_row, devices
    )
    pick, owner_of, rank_of, usable, sent_hot = tied(pick, owner_of, rank_of, usable, sent_hot)
    flat_rank = rank_of.reshape(-1)
    slot_rank = jnp.sum(
        jnp.where(pick[:, :, None] == all_blocks[None, None, :], flat_rank[None, None, :], 0), axis=-1
    )
    near_at = blocks_here + owner_of * REACH + slot_rank
    hot_at = blocks_here + devices * REACH + slot_rank
    at = jnp.where(
        owner_of == position, pick % blocks_here, jnp.where(owner_of == 0, hot_at, near_at)
    )
    at = jnp.where(usable, at, 0).astype(jnp.int32).reshape(-1)
    mask = jnp.repeat(usable.astype(f32), BLOCK, axis=1)

    at, mask, order, toward, same_order, sent_hot = tied(
        at, mask, order, toward, same_order, sent_hot
    )
    near, sent_hot = tied(near, sent_hot)
    hot = exchange(sent_hot, KV)
    w_far = along_y(w_after, 1)
    w_swapped = [across(w_after), across(w_before)]
    w_swapped.append(across(w_far))
    weights = [w_out, w_after, w_before, w_far, w_own] + w_swapped

    gains = out_gain.reshape(ranks, 1, WIDTH)
    early = (FIRST_BLOCKS * blocks_here) // 8
    first = attend(0, early, False, at, same_order, queries, mask, pairs, near, hot)
    first = exchange(first, TP)
    second = attend(early, blocks_here - early, True, at, toward, queries, mask, pairs, near, hot)
    second = send_pieces(second)
    first = project_out(False, order, same_order, first, weights, gains)
    moved = exchange(first, TP)
    second = tied(first, *second)[1:]
    second = project_out(True, order, toward, second, weights, gains)
    second = send_pieces(second)
    return place(order, moved.reshape(-1, WIDTH), second)


def solution(mesh):
    split = Mesh(mesh.devices.reshape(4, 4, 4, 2), KV + TP)
    return jax.shard_map(
        local,
        mesh=split,
        in_specs=(
            P(KV, None),
            P(None, TP),
            P(None, TP),
            P(None, TP),
            P(TP, None),
            P(),
            P(),
            P(),
            P(KV, None),
        ),
        out_specs=P(KV, TP),
        check_vma=False,
    )
```

```python
import functools

import jax
import jax.numpy as jnp
from jax import lax
from jax.experimental import pallas as pl
from jax.experimental.pallas import tpu as pltpu
from jax.sharding import Mesh
from jax.sharding import PartitionSpec as P

HEAD_DIM = 128
BLOCK = 64
HOT = 8
REACH = 2
FIRST_BLOCKS = 4
KV = ("kv_0", "kv_1")
TP = ("tp_0", "tp_1")
WIDTH = 256
PAIR = 2
norm_eps = 1e-06
LOG2E = 1.4426950408889634
bf16 = jnp.bfloat16
f32 = jnp.float32
VMEM_LIMIT = 60 * 1024 * 1024


def head_norm(values, gain_row):
    factor = lax.rsqrt(jnp.mean(values * values, axis=-1, keepdims=True) + norm_eps)
    return (values * factor * gain_row).astype(bf16)


def share_kernel(rank, tok, *outs):
    rows = tok[...].astype(f32)
    side, small, _ = outs[0].shape
    devices = len(outs) * side
    part = BLOCK // devices
    for k in range(small // 16):
        parts = []
        for b in range(16 // part):
            first = (k * (16 // part) + b) * BLOCK
            parts.append(rows[first : first + BLOCK].reshape(devices, part, WIDTH))
        joined = jnp.concatenate(parts, axis=1).astype(bf16)
        for n, out in enumerate(outs):
            out[:, k * 16 : (k + 1) * 16, :] = joined[n * side : (n + 1) * side]


def token_shares(rank, tokens, long, side):
    length = tokens.shape[0]
    devices = long * side
    tile = 1024
    return pl.pallas_call(
        share_kernel,
        grid_spec=pltpu.PrefetchScalarGridSpec(
            num_scalar_prefetch=1,
            grid=(length // tile,),
            in_specs=[pl.BlockSpec((tile, WIDTH), lambda i, rank: (i, rank[0]))],
            out_specs=[pl.BlockSpec((side, tile // devices, WIDTH), lambda i, rank: (0, i, 0))] * long,
        ),
        out_shape=[jax.ShapeDtypeStruct((side, length // devices, WIDTH), bf16)] * long,
        compiler_params=pltpu.CompilerParams(vmem_limit_bytes=VMEM_LIMIT),
        cost_estimate=pl.CostEstimate(flops=1 << 20, bytes_accessed=4 << 20, transcendentals=0),
        name="token_shares",
    )(rank, tokens)


def kv_kernel(tok, wk, wv, gain, out):
    rows = tok[...]
    keys = jnp.dot(rows, wk[...], preferred_element_type=f32)
    blocks = out.shape[0]
    for h in range(2):
        lanes = slice(h * HEAD_DIM, (h + 1) * HEAD_DIM)
        normed = head_norm(keys[:, lanes], gain[...])
        out[:, 0, :, lanes] = normed.reshape(blocks, BLOCK, HEAD_DIM)
    vals = jnp.dot(rows, wv[...], preferred_element_type=f32).astype(bf16)
    out[:, 1, :, :] = vals.reshape(blocks, BLOCK, WIDTH)


def project_kv(tokens, w_key, w_value, gain):
    length, depth = tokens.shape
    tile = 1024
    blocks = tile // BLOCK
    return pl.pallas_call(
        kv_kernel,
        grid=(length // tile,),
        in_specs=[
            pl.BlockSpec((tile, depth), lambda i: (i, 0)),
            pl.BlockSpec((depth, WIDTH), lambda i: (0, 0)),
            pl.BlockSpec((depth, WIDTH), lambda i: (0, 0)),
            pl.BlockSpec((1, HEAD_DIM), lambda i: (0, 0)),
        ],
        out_specs=pl.BlockSpec((blocks, PAIR, BLOCK, WIDTH), lambda i: (i, 0, 0, 0)),
        out_shape=jax.ShapeDtypeStruct((length // BLOCK, PAIR, BLOCK, WIDTH), bf16),
        compiler_params=pltpu.CompilerParams(vmem_limit_bytes=VMEM_LIMIT),
        cost_estimate=pl.CostEstimate(
            flops=4 * length * depth * WIDTH, bytes_accessed=2 * length * depth, transcendentals=0
        ),
        name="project_kv",
    )(tokens, w_key, w_value, gain)


def q_kernel(tok, wq, gain, out):
    values = jnp.dot(tok[...], wq[...], preferred_element_type=f32)
    for h in range(2):
        lanes = slice(h * HEAD_DIM, (h + 1) * HEAD_DIM)
        out[:, lanes] = head_norm(values[:, lanes], gain[...])


def project_q(tokens, w_query, gain):
    length, depth = tokens.shape
    tile = 1024
    return pl.pallas_call(
        q_kernel,
        grid=(length // tile,),
        in_specs=[
            pl.BlockSpec((tile, depth), lambda i: (i, 0)),
            pl.BlockSpec((depth, WIDTH), lambda i: (0, 0)),
            pl.BlockSpec((1, HEAD_DIM), lambda i: (0, 0)),
        ],
        out_specs=pl.BlockSpec((tile, WIDTH), lambda i: (i, 0)),
        out_shape=jax.ShapeDtypeStruct((length, WIDTH), bf16),
        compiler_params=pltpu.CompilerParams(vmem_limit_bytes=VMEM_LIMIT),
        cost_estimate=pl.CostEstimate(
            flops=2 * length * depth * WIDTH, bytes_accessed=2 * length * depth, transcendentals=0
        ),
        name="project_q",
    )(tokens, w_query, gain)


def near_kernel(near, pairs, out, room, in_sems, out_sems):
    unit = PAIR * BLOCK
    coming, going = [], []
    for m in range(near.shape[0]):
        first = pl.multiple_of(near[m] * unit, unit)
        coming.append(
            pltpu.make_async_copy(pairs.at[pl.ds(first, unit)], room.at[m], in_sems.at[m])
        )
        going.append(pltpu.make_async_copy(room.at[m], out.at[m], out_sems.at[m]))
    for copy in coming:
        copy.start()
    for n, copy in enumerate(coming):
        copy.wait()
        going[n].start()
    for copy in going:
        copy.wait()


def gather_near(near, pairs):
    anywhere = pl.BlockSpec(memory_space=pl.ANY)
    sends = near.shape[0]
    return pl.pallas_call(
        near_kernel,
        grid_spec=pltpu.PrefetchScalarGridSpec(
            num_scalar_prefetch=1,
            grid=(1,),
            in_specs=[anywhere],
            out_specs=anywhere,
            scratch_shapes=[
                pltpu.VMEM((sends, PAIR * BLOCK, WIDTH), bf16),
                pltpu.SemaphoreType.DMA((sends,)),
                pltpu.SemaphoreType.DMA((sends,)),
            ],
        ),
        out_shape=jax.ShapeDtypeStruct((sends, PAIR * BLOCK, WIDTH), bf16),
        compiler_params=pltpu.CompilerParams(vmem_limit_bytes=VMEM_LIMIT),
        cost_estimate=pl.CostEstimate(flops=1 << 20, bytes_accessed=4 << 20, transcendentals=0),
        name="gather_near",
    )(near, pairs)


def send_kernel(asked, order, same, other, wk, wv, gain, out, keep):
    devices, rows, _ = out.shape
    keys = jnp.zeros((same.shape[1], WIDTH), f32)
    vals = jnp.zeros((same.shape[1], WIDTH), f32)
    count = same.shape[0]
    for k in range(2 * count):
        tokens = same[k] if k < count else other[k - count]
        span = pl.ds(pl.multiple_of(order[k] * WIDTH, WIDTH), WIDTH)
        keys += jnp.dot(tokens, wk[span, :], preferred_element_type=f32)
        vals += jnp.dot(tokens, wv[span, :], preferred_element_type=f32)
    groups, unit, _ = keep.shape
    part = unit // 2
    for h in range(2):
        lanes = slice(h * HEAD_DIM, (h + 1) * HEAD_DIM)
        x = keys[:, lanes]
        factor = lax.rsqrt(jnp.mean(x * x, axis=-1, keepdims=True) + norm_eps)
        keep[:, :part, lanes] = (x * factor * gain[...]).reshape(groups, part, HEAD_DIM)
    keep[:, part:, :] = vals.reshape(groups, part, WIDTH)

    twos = rows // (2 * unit)

    def one(m, carry):
        both = jnp.concatenate([keep[asked[2 * m]], keep[asked[2 * m + 1]]], axis=0)
        at = pl.multiple_of((m % twos) * 2 * unit, 2 * unit)
        out[m // twos, pl.ds(at, 2 * unit), :] = both.astype(bf16)
        return carry

    lax.fori_loop(0, devices * twos, one, 0, unroll=4)


def whole_block(*shape):
    return pl.BlockSpec(shape, lambda i, *_: (0,) * len(shape))


def project_sent(asked, order, same, other, w_key, w_value, gain, devices):
    count, rows, _ = same.shape
    groups = 64
    unit = 2 * rows // groups
    depth = w_key.shape[0]
    shape = (devices, (asked.shape[0] // devices) * unit, WIDTH)
    return pl.pallas_call(
        send_kernel,
        grid_spec=pltpu.PrefetchScalarGridSpec(
            num_scalar_prefetch=2,
            grid=(1,),
            in_specs=[
                whole_block(count, rows, WIDTH),
                whole_block(count, rows, WIDTH),
                whole_block(depth, WIDTH),
                whole_block(depth, WIDTH),
                whole_block(1, HEAD_DIM),
            ],
            out_specs=whole_block(*shape),
            scratch_shapes=[pltpu.VMEM((groups, unit, WIDTH), f32)],
        ),
        out_shape=jax.ShapeDtypeStruct(shape, bf16),
        compiler_params=pltpu.CompilerParams(vmem_limit_bytes=VMEM_LIMIT),
        cost_estimate=pl.CostEstimate(
            flops=4 * rows * depth * WIDTH, bytes_accessed=8 << 20, transcendentals=0
        ),
        name="project_sent",
    )(asked, order, same, other, w_key, w_value, gain)


def attention_kernel(first, at, where, queries, masks, pairs, near, hot, *rest):
    outs, (q, mask, table, raw, sems) = rest[:-5], rest[-5:]
    devices, hot_rows, _ = hot.shape
    here = pairs.shape[0]
    plain = near.shape[0]
    copies = [
        pltpu.make_async_copy(hot, raw, sems.at[0]),
        pltpu.make_async_copy(pairs, table.at[pl.ds(0, here)], sems.at[1]),
        pltpu.make_async_copy(near, table.at[pl.ds(here, plain)], sems.at[2]),
        pltpu.make_async_copy(queries.at[pl.ds(first * BLOCK, q.shape[0])], q, sems.at[3]),
        pltpu.make_async_copy(masks.at[pl.ds(first, mask.shape[0])], mask, sems.at[4]),
    ]
    for copy in copies:
        copy.start()
    copies[0].wait()
    part = BLOCK // devices
    for n in range(hot_rows // 16):
        both = raw[:, n * 16 : (n + 1) * 16, :].astype(f32)
        for m in range(2):
            start = here + plain + (2 * n + m) * PAIR * BLOCK
            for kind in range(PAIR):
                low = m * 2 * part + kind * part
                piece = both[:, low : low + part, :].reshape(BLOCK, WIDTH).astype(bf16)
                table[start + kind * BLOCK : start + (kind + 1) * BLOCK, :] = piece
    for copy in copies[1:]:
        copy.wait()
    slots = mask.shape[1] // BLOCK
    count = where.shape[0]
    whole = len(outs) == 1
    per_piece = mask.shape[0] // count
    blank = jnp.zeros((BLOCK, HEAD_DIM), bf16)

    def load(block):
        row = pl.multiple_of(block * BLOCK, BLOCK)
        rows = q[pl.ds(row, BLOCK), :]
        both = jnp.concatenate(
            [
                jnp.concatenate([rows[:, :HEAD_DIM], blank], axis=1),
                jnp.concatenate([blank, rows[:, HEAD_DIM:]], axis=1),
            ],
            axis=0,
        )
        base = (first + block) * slots
        return both, [
            pl.multiple_of(at[base + j] * PAIR * BLOCK, PAIR * BLOCK) for j in range(slots)
        ]

    def piece_of(n, put):
        items = [load(where[n] * per_piece + i) for i in range(per_piece)]
        logits = []
        for both, picks in items:
            keys = jnp.concatenate([table[pl.ds(p, BLOCK), :] for p in picks], axis=0)
            logits.append(
                lax.dot_general(both, keys, (((1,), (1,)), ((), ())), preferred_element_type=f32)
            )
        weights = []
        for i in range(per_piece):
            block = where[n] * per_piece + i
            weights.append(jnp.exp2(logits[i]) * mask[pl.ds(block, 1), :])
        for i, (both, picks) in enumerate(items):
            values = jnp.concatenate(
                [table[pl.ds(p + BLOCK, BLOCK), :] for p in picks], axis=0
            )
            sums = jnp.dot(weights[i].astype(bf16), values, preferred_element_type=f32)
            scale = 1.0 / jnp.sum(weights[i], axis=-1, keepdims=True)
            to = slice(i * BLOCK, (i + 1) * BLOCK)
            put(to, slice(0, HEAD_DIM), sums[:BLOCK, :HEAD_DIM] * scale[:BLOCK])
            put(to, slice(HEAD_DIM, WIDTH), sums[BLOCK:, HEAD_DIM:] * scale[BLOCK:])

    if whole:

        def one(n, carry):
            def put(rows, lanes, value):
                outs[0][n, rows, lanes] = value.astype(bf16)

            piece_of(n, put)
            return carry

        lax.fori_loop(0, count, one, 0)
    else:
        for n in range(count):

            def put(rows, lanes, value, n=n):
                outs[n][rows, lanes] = value.astype(bf16)

            piece_of(n, put)


def attend(first, blocks, split, at, where, queries, mask, pairs, near, hot):
    ranks = where.shape[0]
    length = blocks * BLOCK
    slots = mask.shape[1] // BLOCK
    rows = length // ranks
    anywhere = pl.BlockSpec(memory_space=pl.ANY)
    shape = (rows, WIDTH) if split else (ranks, rows, WIDTH)
    count = ranks if split else 1
    height = pairs.shape[0] + near.shape[0] + HOT * PAIR * BLOCK
    outs = pl.pallas_call(
        functools.partial(attention_kernel, first),
        grid_spec=pltpu.PrefetchScalarGridSpec(
            num_scalar_prefetch=2,
            grid=(1,),
            in_specs=[
                anywhere,
                anywhere,
                anywhere,
                anywhere,
                anywhere,
            ],
            out_specs=[whole_block(*shape)] * count,
            scratch_shapes=[
                pltpu.VMEM((length, WIDTH), bf16),
                pltpu.VMEM((blocks, slots * BLOCK), f32),
                pltpu.VMEM((height, WIDTH), bf16),
                pltpu.VMEM(hot.shape, bf16),
                pltpu.SemaphoreType.DMA((5,)),
            ],
        ),
        out_shape=[jax.ShapeDtypeStruct(shape, bf16)] * count,
        compiler_params=pltpu.CompilerParams(vmem_limit_bytes=VMEM_LIMIT),
        cost_estimate=pl.CostEstimate(
            flops=8 * length * WIDTH * slots * BLOCK, bytes_accessed=10 << 20, transcendentals=0
        ),
        name="attend",
    )(at, where, queries, mask, pairs, near, hot)
    return list(outs) if split else outs[0]


def out_kernel(order, slot, *refs):
    count = order.shape[0]
    n = pl.program_id(0)
    if len(refs) > 2 * count + 4:
        pieces, refs = refs[:count], refs[count:]
    else:
        pieces, refs = [refs[0].at[order[k]] for k in range(count)], refs[1:]
    weights, gain, refs = refs[:count], refs[count], refs[count + 1 :]
    outs, (mixed, squares) = refs[:-2], refs[-2:]
    rows = jnp.concatenate([piece[...] for piece in pieces], axis=1)
    weight = jnp.concatenate([w[...] for w in weights], axis=0)
    sums = jnp.dot(rows, weight, preferred_element_type=f32)
    tile = sums.shape[1]
    for i in range(tile // WIDTH):
        mixed[(tile // WIDTH) * n + i] = sums[:, i * WIDTH : (i + 1) * WIDTH]
    part = sum(sums[:, i : i + 128] * sums[:, i : i + 128] for i in range(0, tile, 128))

    @pl.when(n == 0)
    def _():
        squares[...] = part

    @pl.when(n > 0)
    def _():
        squares[...] += part

    @pl.when(n == pl.num_programs(0) - 1)
    def _():
        total = jnp.sum(squares[...], axis=-1, keepdims=True)
        factor = lax.rsqrt(total * (1.0 / (count * WIDTH)) + norm_eps)
        for k in range(count):
            value = (mixed[slot[k]] * factor * gain[slot[k]]).astype(bf16)
            if len(outs) == 1:
                outs[0][k] = value
            else:
                outs[k][...] = value


def project_out(split, order, slot, pieces, weights, gain):
    count = len(weights)
    pieces = list(pieces) if split else [pieces]
    rows = pieces[0].shape[-2]
    depth, width = weights[0].shape
    tile = 4 * WIDTH
    shape = (rows, WIDTH) if split else (count, rows, WIDTH)
    outs = pl.pallas_call(
        out_kernel,
        grid_spec=pltpu.PrefetchScalarGridSpec(
            num_scalar_prefetch=2,
            grid=(width // tile,),
            in_specs=[whole_block(*shape)] * len(pieces)
            + [pl.BlockSpec((depth, tile), lambda n, *_: (0, n))] * count
            + [whole_block(*gain.shape)],
            out_specs=[whole_block(*shape)] * len(pieces),
            scratch_shapes=[
                pltpu.VMEM((count, rows, WIDTH), f32),
                pltpu.VMEM((rows, 128), f32),
            ],
        ),
        out_shape=[jax.ShapeDtypeStruct(shape, bf16)] * len(pieces),
        compiler_params=pltpu.CompilerParams(vmem_limit_bytes=VMEM_LIMIT),
        cost_estimate=pl.CostEstimate(
            flops=2 * rows * width * width, bytes_accessed=12 << 20, transcendentals=0
        ),
        name="project_out",
    )(order, slot, *pieces, *weights, gain)
    return list(outs) if split else outs[0]


def place_kernel(order, whole, *rest):
    count = len(rest) - 2
    parts, out, sems = rest[:count], rest[count], rest[count + 1]
    rows = parts[0].shape[0]
    base = whole.shape[0]
    copies = [pltpu.make_async_copy(whole, out.at[pl.ds(0, base)], sems.at[count])]
    for k in range(count):
        to = pl.multiple_of(base + order[k] * rows, BLOCK)
        copies.append(pltpu.make_async_copy(parts[k], out.at[pl.ds(to, rows)], sems.at[k]))
    for copy in copies:
        copy.start()
    for copy in copies:
        copy.wait()


def place(order, whole, parts):
    count = len(parts)
    length = whole.shape[0] + count * parts[0].shape[0]
    anywhere = pl.BlockSpec(memory_space=pl.ANY)
    return pl.pallas_call(
        place_kernel,
        grid_spec=pltpu.PrefetchScalarGridSpec(
            num_scalar_prefetch=1,
            grid=(1,),
            in_specs=[anywhere] * (count + 1),
            out_specs=anywhere,
            scratch_shapes=[pltpu.SemaphoreType.DMA((count + 1,))],
        ),
        out_shape=jax.ShapeDtypeStruct((length, WIDTH), bf16),
        compiler_params=pltpu.CompilerParams(vmem_limit_bytes=8 << 20),
        cost_estimate=pl.CostEstimate(flops=1 << 20, bytes_accessed=4 << 20, transcendentals=0),
        name="place",
    )(order, whole, *parts)


def exchange(pieces, axes):
    return lax.all_to_all(pieces, axes, split_axis=0, concat_axis=0, tiled=True)


def tied(*arrays):
    return lax.optimization_barrier(arrays)


def along_y(piece, shift):
    ring = lax.axis_size(TP[0])
    return lax.ppermute(piece, TP[0], [(i, (i + shift) % ring) for i in range(ring)])


def across(piece):
    return lax.ppermute(piece, TP[1], [(0, 1), (1, 0)])


def chosen_of(options, index):
    result = options[0]
    for n, option in enumerate(options[1:], 1):
        result = jnp.where(index == n, option, result)
    return result


def both_cores(parts):
    same = jnp.stack(parts)
    return same, across(same)


OFFSETS = (0, -1, 1, 2)


def piece_order(sign):
    ring = lax.axis_size(TP[0])
    y = lax.axis_index(TP[0])
    c = lax.axis_index(TP[1])
    rows = jnp.stack([(y + ring + sign * d) % ring for d in OFFSETS])
    return jnp.concatenate([2 * rows + c, 2 * rows + 1 - c]).astype(jnp.int32)


def send_pieces(pieces):
    ring = lax.axis_size(TP[0])
    got = []
    for k in range(2 * ring):
        step, swap = OFFSETS[k % ring], k // ring
        pairs = [
            (2 * y + c, 2 * ((y - step) % ring) + (c + swap) % 2)
            for y in range(ring)
            for c in range(2)
        ]
        got.append(lax.ppermute(pieces[k], TP, pairs) if k else pieces[0])
    return got


def local(tokens, w_query, w_key, w_value, w_out, query_gain, key_gain, out_gain, chosen):
    length, _ = tokens.shape
    blocks_here = length // BLOCK
    devices = lax.axis_size(KV)
    position = lax.axis_index(KV)
    ranks = lax.axis_size(TP)
    key_row = key_gain[None, :]
    query_row = (query_gain * (HEAD_DIM ** (-0.5) * LOG2E))[None, :]

    rank = lax.axis_index(TP).astype(jnp.int32).reshape(1)
    long, side = lax.axis_size(KV[0]), lax.axis_size(KV[1])
    z, x = lax.axis_index(KV[0]), lax.axis_index(KV[1])
    columns = token_shares(rank, tokens, long, side)
    chosen, *columns = tied(chosen, *columns)
    columns = columns[:1] + [lax.ppermute(columns[n], KV, [(0, n * side)]) for n in range(1, long)]

    usable = chosen >= 0
    pick = jnp.where(usable, chosen, 0)
    owner_of = pick // blocks_here
    all_blocks = jnp.arange(devices * blocks_here, dtype=jnp.int32)
    marked = jnp.where(usable & (owner_of != position), chosen, -1)
    wanted = jnp.any(marked[:, :, None] == all_blocks[None, None, :], axis=(0, 1)).reshape(
        devices, blocks_here
    )
    rank_of = jnp.cumsum(wanted.astype(jnp.int32), axis=1) - 1
    local_ids = jnp.arange(blocks_here, dtype=jnp.int32)
    places = wanted[:, :, None] & (
        rank_of[:, :, None] == jnp.arange(HOT, dtype=jnp.int32)[None, None, :]
    )
    named = jnp.sum(jnp.where(places, local_ids[None, :, None], 0), axis=1).astype(jnp.int32)
    requests = jnp.concatenate([named, jnp.broadcast_to(named[:1], named.shape)], axis=1)
    order = piece_order(1)
    toward = piece_order(-1)
    same_order = jnp.arange(ranks, dtype=jnp.int32)

    asked = exchange(requests, KV)
    pairs = project_kv(tokens, w_key, w_value, key_row).reshape(-1, WIDTH)
    asked_near = asked[:, :REACH].reshape(-1)
    asked_hot = asked[:, HOT:].reshape(-1)

    sent = gather_near(asked_near, pairs)
    sent, *columns = tied(sent, *columns)
    held = [chosen_of([c[n] for c in columns], z) for n in range(side)]
    starts = range(0, devices, side)
    held = held[:1] + [
        lax.ppermute(held[n], KV, [(i, i + n) for i in starts]) for n in range(1, side)
    ]
    near = exchange(sent.reshape(devices, -1, WIDTH), KV).reshape(-1, WIDTH)
    again, sent = tied(tokens, sent)
    queries = project_q(again, w_query, query_row)
    queries, *held = tied(queries, *held)
    shares = chosen_of(held, x)
    parts = [shares] + [along_y(shares, shift) for shift in (1, -1, 2)]
    w_after = along_y(w_out, 1)
    w_own = across(w_out)
    rows_same, rows_other = both_cores(parts)
    sent_hot = project_sent(
        asked_hot, order, rows_same, rows_other, w_key, w_value, key_row, devices
    )
    pick, owner_of, rank_of, usable, sent_hot = tied(pick, owner_of, rank_of, usable, sent_hot)
    flat_rank = rank_of.reshape(-1)
    slot_rank = jnp.sum(
        jnp.where(pick[:, :, None] == all_blocks[None, None, :], flat_rank[None, None, :], 0), axis=-1
    )
    near_at = blocks_here + owner_of * REACH + slot_rank
    hot_at = blocks_here + devices * REACH + slot_rank
    at = jnp.where(
        owner_of == position, pick % blocks_here, jnp.where(owner_of == 0, hot_at, near_at)
    )
    at = jnp.where(usable, at, 0).astype(jnp.int32).reshape(-1)
    mask = jnp.repeat(usable.astype(f32), BLOCK, axis=1)

    order, toward, same_order, sent_hot = tied(order, toward, same_order, sent_hot)
    near, sent_hot = tied(near, sent_hot)
    hot = exchange(sent_hot, KV)
    w_before = along_y(w_out, -1)
    w_far = along_y(w_after, 1)

    gains = out_gain.reshape(ranks, 1, WIDTH)
    early = (FIRST_BLOCKS * blocks_here) // 8
    first = attend(0, early, False, at, same_order, queries, mask, pairs, near, hot)
    first = exchange(first, TP)
    second = attend(early, blocks_here - early, True, at, toward, queries, mask, pairs, near, hot)
    *second, w_after, w_before, w_far = tied(*second, w_after, w_before, w_far)
    w_swapped = [across(w_after), across(w_before), across(w_far)]
    weights = [w_out, w_after, w_before, w_far, w_own] + w_swapped
    second = send_pieces(second)
    first = project_out(False, order, same_order, first, weights, gains)
    moved = exchange(first, TP)
    second = tied(first, *second)[1:]
    second = project_out(True, order, toward, second, weights, gains)
    second = send_pieces(second)
    return place(order, moved.reshape(-1, WIDTH), second)


def solution(mesh):
    split = Mesh(mesh.devices.reshape(4, 4, 4, 2), KV + TP)
    return jax.shard_map(
        local,
        mesh=split,
        in_specs=(
            P(KV, None),
            P(None, TP),
            P(None, TP),
            P(None, TP),
            P(TP, None),
            P(),
            P(),
            P(),
            P(KV, None),
        ),
        out_specs=P(KV, TP),
        check_vma=False,
    )
```

```python
import functools

import jax
import jax.numpy as jnp
from jax import lax
from jax.experimental import pallas as pl
from jax.experimental.pallas import tpu as pltpu
from jax.sharding import Mesh
from jax.sharding import PartitionSpec as P

HEAD_DIM = 128
BLOCK = 64
HOT = 8
REACH = 2
FIRST_BLOCKS = 4
KV = ("kv_0", "kv_1")
TP = ("tp_0", "tp_1")
WIDTH = 256
PAIR = 2
norm_eps = 1e-06
LOG2E = 1.4426950408889634
bf16 = jnp.bfloat16
f32 = jnp.float32
VMEM_LIMIT = 60 * 1024 * 1024


def head_norm(values, gain_row):
    factor = lax.rsqrt(jnp.mean(values * values, axis=-1, keepdims=True) + norm_eps)
    return (values * factor * gain_row).astype(bf16)


def share_kernel(rank, tok, *outs):
    rows = tok[...].astype(f32)
    side, small, _ = outs[0].shape
    devices = len(outs) * side
    part = BLOCK // devices
    for k in range(small // 16):
        parts = []
        for b in range(16 // part):
            first = (k * (16 // part) + b) * BLOCK
            parts.append(rows[first : first + BLOCK].reshape(devices, part, WIDTH))
        joined = jnp.concatenate(parts, axis=1).astype(bf16)
        for n, out in enumerate(outs):
            out[:, k * 16 : (k + 1) * 16, :] = joined[n * side : (n + 1) * side]


def token_shares(rank, tokens, long, side):
    length = tokens.shape[0]
    devices = long * side
    tile = 1024
    return pl.pallas_call(
        share_kernel,
        grid_spec=pltpu.PrefetchScalarGridSpec(
            num_scalar_prefetch=1,
            grid=(length // tile,),
            in_specs=[pl.BlockSpec((tile, WIDTH), lambda i, rank: (i, rank[0]))],
            out_specs=[pl.BlockSpec((side, tile // devices, WIDTH), lambda i, rank: (0, i, 0))] * long,
        ),
        out_shape=[jax.ShapeDtypeStruct((side, length // devices, WIDTH), bf16)] * long,
        compiler_params=pltpu.CompilerParams(vmem_limit_bytes=VMEM_LIMIT),
        cost_estimate=pl.CostEstimate(flops=1 << 20, bytes_accessed=4 << 20, transcendentals=0),
        name="token_shares",
    )(rank, tokens)


def kv_kernel(tok, wk, wv, gain, out):
    rows = tok[...]
    keys = jnp.dot(rows, wk[...], preferred_element_type=f32)
    blocks = out.shape[0]
    for h in range(2):
        lanes = slice(h * HEAD_DIM, (h + 1) * HEAD_DIM)
        normed = head_norm(keys[:, lanes], gain[...])
        out[:, 0, :, lanes] = normed.reshape(blocks, BLOCK, HEAD_DIM)
    vals = jnp.dot(rows, wv[...], preferred_element_type=f32).astype(bf16)
    out[:, 1, :, :] = vals.reshape(blocks, BLOCK, WIDTH)


def project_kv(tokens, w_key, w_value, gain):
    length, depth = tokens.shape
    tile = 1024
    blocks = tile // BLOCK
    return pl.pallas_call(
        kv_kernel,
        grid=(length // tile,),
        in_specs=[
            pl.BlockSpec((tile, depth), lambda i: (i, 0)),
            pl.BlockSpec((depth, WIDTH), lambda i: (0, 0)),
            pl.BlockSpec((depth, WIDTH), lambda i: (0, 0)),
            pl.BlockSpec((1, HEAD_DIM), lambda i: (0, 0)),
        ],
        out_specs=pl.BlockSpec((blocks, PAIR, BLOCK, WIDTH), lambda i: (i, 0, 0, 0)),
        out_shape=jax.ShapeDtypeStruct((length // BLOCK, PAIR, BLOCK, WIDTH), bf16),
        compiler_params=pltpu.CompilerParams(vmem_limit_bytes=VMEM_LIMIT),
        cost_estimate=pl.CostEstimate(
            flops=4 * length * depth * WIDTH, bytes_accessed=2 * length * depth, transcendentals=0
        ),
        name="project_kv",
    )(tokens, w_key, w_value, gain)


def q_kernel(tok, wq, gain, out):
    values = jnp.dot(tok[...], wq[...], preferred_element_type=f32)
    for h in range(2):
        lanes = slice(h * HEAD_DIM, (h + 1) * HEAD_DIM)
        out[:, lanes] = head_norm(values[:, lanes], gain[...])


def project_q(tokens, w_query, gain):
    length, depth = tokens.shape
    tile = 1024
    return pl.pallas_call(
        q_kernel,
        grid=(length // tile,),
        in_specs=[
            pl.BlockSpec((tile, depth), lambda i: (i, 0)),
            pl.BlockSpec((depth, WIDTH), lambda i: (0, 0)),
            pl.BlockSpec((1, HEAD_DIM), lambda i: (0, 0)),
        ],
        out_specs=pl.BlockSpec((tile, WIDTH), lambda i: (i, 0)),
        out_shape=jax.ShapeDtypeStruct((length, WIDTH), bf16),
        compiler_params=pltpu.CompilerParams(vmem_limit_bytes=VMEM_LIMIT),
        cost_estimate=pl.CostEstimate(
            flops=2 * length * depth * WIDTH, bytes_accessed=2 * length * depth, transcendentals=0
        ),
        name="project_q",
    )(tokens, w_query, gain)


def near_kernel(near, pairs, out, room, in_sems, out_sems):
    unit = PAIR * BLOCK
    coming, going = [], []
    for m in range(near.shape[0]):
        first = pl.multiple_of(near[m] * unit, unit)
        coming.append(
            pltpu.make_async_copy(pairs.at[pl.ds(first, unit)], room.at[m], in_sems.at[m])
        )
        going.append(pltpu.make_async_copy(room.at[m], out.at[m], out_sems.at[m]))
    for copy in coming:
        copy.start()
    for n, copy in enumerate(coming):
        copy.wait()
        going[n].start()
    for copy in going:
        copy.wait()


def gather_near(near, pairs):
    anywhere = pl.BlockSpec(memory_space=pl.ANY)
    sends = near.shape[0]
    return pl.pallas_call(
        near_kernel,
        grid_spec=pltpu.PrefetchScalarGridSpec(
            num_scalar_prefetch=1,
            grid=(1,),
            in_specs=[anywhere],
            out_specs=anywhere,
            scratch_shapes=[
                pltpu.VMEM((sends, PAIR * BLOCK, WIDTH), bf16),
                pltpu.SemaphoreType.DMA((sends,)),
                pltpu.SemaphoreType.DMA((sends,)),
            ],
        ),
        out_shape=jax.ShapeDtypeStruct((sends, PAIR * BLOCK, WIDTH), bf16),
        compiler_params=pltpu.CompilerParams(vmem_limit_bytes=VMEM_LIMIT),
        cost_estimate=pl.CostEstimate(flops=1 << 20, bytes_accessed=4 << 20, transcendentals=0),
        name="gather_near",
    )(near, pairs)


def send_kernel(asked, order, same, other, wk, wv, gain, out, keep):
    devices, rows, _ = out.shape
    keys = jnp.zeros((same.shape[1], WIDTH), f32)
    vals = jnp.zeros((same.shape[1], WIDTH), f32)
    count = same.shape[0]
    for k in range(2 * count):
        tokens = same[k] if k < count else other[k - count]
        span = pl.ds(pl.multiple_of(order[k] * WIDTH, WIDTH), WIDTH)
        keys += jnp.dot(tokens, wk[span, :], preferred_element_type=f32)
        vals += jnp.dot(tokens, wv[span, :], preferred_element_type=f32)
    groups, unit, _ = keep.shape
    part = unit // 2
    for h in range(2):
        lanes = slice(h * HEAD_DIM, (h + 1) * HEAD_DIM)
        x = keys[:, lanes]
        factor = lax.rsqrt(jnp.mean(x * x, axis=-1, keepdims=True) + norm_eps)
        keep[:, :part, lanes] = (x * factor * gain[...]).reshape(groups, part, HEAD_DIM)
    keep[:, part:, :] = vals.reshape(groups, part, WIDTH)

    twos = rows // (2 * unit)

    def one(m, carry):
        both = jnp.concatenate([keep[asked[2 * m]], keep[asked[2 * m + 1]]], axis=0)
        at = pl.multiple_of((m % twos) * 2 * unit, 2 * unit)
        out[m // twos, pl.ds(at, 2 * unit), :] = both.astype(bf16)
        return carry

    lax.fori_loop(0, devices * twos, one, 0, unroll=4)


def whole_block(*shape):
    return pl.BlockSpec(shape, lambda i, *_: (0,) * len(shape))


def project_sent(asked, order, same, other, w_key, w_value, gain, devices):
    count, rows, _ = same.shape
    groups = 64
    unit = 2 * rows // groups
    depth = w_key.shape[0]
    shape = (devices, (asked.shape[0] // devices) * unit, WIDTH)
    return pl.pallas_call(
        send_kernel,
        grid_spec=pltpu.PrefetchScalarGridSpec(
            num_scalar_prefetch=2,
            grid=(1,),
            in_specs=[
                whole_block(count, rows, WIDTH),
                whole_block(count, rows, WIDTH),
                whole_block(depth, WIDTH),
                whole_block(depth, WIDTH),
                whole_block(1, HEAD_DIM),
            ],
            out_specs=whole_block(*shape),
            scratch_shapes=[pltpu.VMEM((groups, unit, WIDTH), f32)],
        ),
        out_shape=jax.ShapeDtypeStruct(shape, bf16),
        compiler_params=pltpu.CompilerParams(vmem_limit_bytes=VMEM_LIMIT),
        cost_estimate=pl.CostEstimate(
            flops=4 * rows * depth * WIDTH, bytes_accessed=8 << 20, transcendentals=0
        ),
        name="project_sent",
    )(asked, order, same, other, w_key, w_value, gain)


def attention_kernel(first, at, where, queries, masks, pairs, near, hot, *rest):
    outs, (q, mask, table, raw, sems) = rest[:-5], rest[-5:]
    devices, hot_rows, _ = hot.shape
    here = pairs.shape[0]
    plain = near.shape[0]
    used = pl.ds(0, (first + mask.shape[0]) * PAIR * BLOCK)
    copies = [
        pltpu.make_async_copy(hot, raw, sems.at[0]),
        pltpu.make_async_copy(pairs.at[used], table.at[used], sems.at[1]),
        pltpu.make_async_copy(near, table.at[pl.ds(here, plain)], sems.at[2]),
        pltpu.make_async_copy(queries.at[pl.ds(first * BLOCK, q.shape[0])], q, sems.at[3]),
        pltpu.make_async_copy(masks.at[pl.ds(first, mask.shape[0])], mask, sems.at[4]),
    ]
    for copy in copies:
        copy.start()
    copies[0].wait()
    part = BLOCK // devices
    for n in range(hot_rows // 16):
        both = raw[:, n * 16 : (n + 1) * 16, :].astype(f32)
        for m in range(2):
            start = here + plain + (2 * n + m) * PAIR * BLOCK
            for kind in range(PAIR):
                low = m * 2 * part + kind * part
                piece = both[:, low : low + part, :].reshape(BLOCK, WIDTH).astype(bf16)
                table[start + kind * BLOCK : start + (kind + 1) * BLOCK, :] = piece
    for copy in copies[1:]:
        copy.wait()
    slots = mask.shape[1] // BLOCK
    count = where.shape[0]
    whole = len(outs) == 1
    per_piece = mask.shape[0] // count
    blank = jnp.zeros((BLOCK, HEAD_DIM), bf16)

    def load(block):
        row = pl.multiple_of(block * BLOCK, BLOCK)
        rows = q[pl.ds(row, BLOCK), :]
        both = jnp.concatenate(
            [
                jnp.concatenate([rows[:, :HEAD_DIM], blank], axis=1),
                jnp.concatenate([blank, rows[:, HEAD_DIM:]], axis=1),
            ],
            axis=0,
        )
        base = (first + block) * slots
        return both, [
            pl.multiple_of(at[base + j] * PAIR * BLOCK, PAIR * BLOCK) for j in range(slots)
        ]

    def piece_of(n, put):
        items = [load(where[n] * per_piece + i) for i in range(per_piece)]
        logits = []
        for both, picks in items:
            keys = jnp.concatenate([table[pl.ds(p, BLOCK), :] for p in picks], axis=0)
            logits.append(
                lax.dot_general(both, keys, (((1,), (1,)), ((), ())), preferred_element_type=f32)
            )
        weights = []
        for i in range(per_piece):
            block = where[n] * per_piece + i
            weights.append(jnp.exp2(logits[i]) * mask[pl.ds(block, 1), :])
        for i, (both, picks) in enumerate(items):
            values = jnp.concatenate(
                [table[pl.ds(p + BLOCK, BLOCK), :] for p in picks], axis=0
            )
            sums = jnp.dot(weights[i].astype(bf16), values, preferred_element_type=f32)
            scale = 1.0 / jnp.sum(weights[i], axis=-1, keepdims=True)
            to = slice(i * BLOCK, (i + 1) * BLOCK)
            put(to, slice(0, HEAD_DIM), sums[:BLOCK, :HEAD_DIM] * scale[:BLOCK])
            put(to, slice(HEAD_DIM, WIDTH), sums[BLOCK:, HEAD_DIM:] * scale[BLOCK:])

    if whole:

        def one(n, carry):
            def put(rows, lanes, value):
                outs[0][n, rows, lanes] = value.astype(bf16)

            piece_of(n, put)
            return carry

        lax.fori_loop(0, count, one, 0)
    else:
        for n in range(count):

            def put(rows, lanes, value, n=n):
                outs[n][rows, lanes] = value.astype(bf16)

            piece_of(n, put)


def attend(first, blocks, split, at, where, queries, mask, pairs, near, hot):
    ranks = where.shape[0]
    length = blocks * BLOCK
    slots = mask.shape[1] // BLOCK
    rows = length // ranks
    anywhere = pl.BlockSpec(memory_space=pl.ANY)
    shape = (rows, WIDTH) if split else (ranks, rows, WIDTH)
    count = ranks if split else 1
    height = pairs.shape[0] + near.shape[0] + HOT * PAIR * BLOCK
    outs = pl.pallas_call(
        functools.partial(attention_kernel, first),
        grid_spec=pltpu.PrefetchScalarGridSpec(
            num_scalar_prefetch=2,
            grid=(1,),
            in_specs=[
                anywhere,
                anywhere,
                anywhere,
                anywhere,
                anywhere,
            ],
            out_specs=[whole_block(*shape)] * count,
            scratch_shapes=[
                pltpu.VMEM((length, WIDTH), bf16),
                pltpu.VMEM((blocks, slots * BLOCK), f32),
                pltpu.VMEM((height, WIDTH), bf16),
                pltpu.VMEM(hot.shape, bf16),
                pltpu.SemaphoreType.DMA((5,)),
            ],
        ),
        out_shape=[jax.ShapeDtypeStruct(shape, bf16)] * count,
        compiler_params=pltpu.CompilerParams(vmem_limit_bytes=VMEM_LIMIT),
        cost_estimate=pl.CostEstimate(
            flops=8 * length * WIDTH * slots * BLOCK, bytes_accessed=10 << 20, transcendentals=0
        ),
        name="attend",
    )(at, where, queries, mask, pairs, near, hot)
    return list(outs) if split else outs[0]


def out_kernel(order, slot, *refs):
    count = order.shape[0]
    n = pl.program_id(0)
    if len(refs) > 2 * count + 4:
        pieces, refs = refs[:count], refs[count:]
    else:
        pieces, refs = [refs[0].at[order[k]] for k in range(count)], refs[1:]
    weights, gain, refs = refs[:count], refs[count], refs[count + 1 :]
    outs, (mixed, squares) = refs[:-2], refs[-2:]
    rows = jnp.concatenate([piece[...] for piece in pieces], axis=1)
    weight = jnp.concatenate([w[...] for w in weights], axis=0)
    sums = jnp.dot(rows, weight, preferred_element_type=f32)
    tile = sums.shape[1]
    for i in range(tile // WIDTH):
        mixed[(tile // WIDTH) * n + i] = sums[:, i * WIDTH : (i + 1) * WIDTH]
    part = sum(sums[:, i : i + 128] * sums[:, i : i + 128] for i in range(0, tile, 128))

    @pl.when(n == 0)
    def _():
        squares[...] = part

    @pl.when(n > 0)
    def _():
        squares[...] += part

    @pl.when(n == pl.num_programs(0) - 1)
    def _():
        total = jnp.sum(squares[...], axis=-1, keepdims=True)
        factor = lax.rsqrt(total * (1.0 / (count * WIDTH)) + norm_eps)
        for k in range(count):
            value = (mixed[slot[k]] * factor * gain[slot[k]]).astype(bf16)
            if len(outs) == 1:
                outs[0][k] = value
            else:
                outs[k][...] = value


def project_out(split, order, slot, pieces, weights, gain):
    count = len(weights)
    pieces = list(pieces) if split else [pieces]
    rows = pieces[0].shape[-2]
    depth, width = weights[0].shape
    tile = 4 * WIDTH
    shape = (rows, WIDTH) if split else (count, rows, WIDTH)
    outs = pl.pallas_call(
        out_kernel,
        grid_spec=pltpu.PrefetchScalarGridSpec(
            num_scalar_prefetch=2,
            grid=(width // tile,),
            in_specs=[whole_block(*shape)] * len(pieces)
            + [pl.BlockSpec((depth, tile), lambda n, *_: (0, n))] * count
            + [whole_block(*gain.shape)],
            out_specs=[whole_block(*shape)] * len(pieces),
            scratch_shapes=[
                pltpu.VMEM((count, rows, WIDTH), f32),
                pltpu.VMEM((rows, 128), f32),
            ],
        ),
        out_shape=[jax.ShapeDtypeStruct(shape, bf16)] * len(pieces),
        compiler_params=pltpu.CompilerParams(vmem_limit_bytes=VMEM_LIMIT),
        cost_estimate=pl.CostEstimate(
            flops=2 * rows * width * width, bytes_accessed=12 << 20, transcendentals=0
        ),
        name="project_out",
    )(order, slot, *pieces, *weights, gain)
    return list(outs) if split else outs[0]


def place_whole_kernel(order, whole, own, out, sems):
    base, rows = whole.shape[0], own.shape[0]
    to = pl.multiple_of(base + order[0] * rows, BLOCK)
    copies = [
        pltpu.make_async_copy(whole, out.at[pl.ds(0, base)], sems.at[0]),
        pltpu.make_async_copy(own, out.at[pl.ds(to, rows)], sems.at[1]),
    ]
    for copy in copies:
        copy.start()
    for copy in copies:
        copy.wait()


def place_parts_kernel(order, filled, *rest):
    parts, out, sems = rest[:-2], rest[-2], rest[-1]
    rows = parts[0].shape[0]
    base = out.shape[0] - (len(parts) + 1) * rows
    copies = []
    for k, part in enumerate(parts):
        to = pl.multiple_of(base + order[k + 1] * rows, BLOCK)
        copies.append(pltpu.make_async_copy(part, out.at[pl.ds(to, rows)], sems.at[k]))
    for copy in copies:
        copy.start()
    for copy in copies:
        copy.wait()


def place(kernel, length, order, *arrays, aliases=()):
    anywhere = pl.BlockSpec(memory_space=pl.ANY)
    return pl.pallas_call(
        kernel,
        grid_spec=pltpu.PrefetchScalarGridSpec(
            num_scalar_prefetch=1,
            grid=(1,),
            in_specs=[anywhere] * len(arrays),
            out_specs=anywhere,
            scratch_shapes=[pltpu.SemaphoreType.DMA((len(arrays),))],
        ),
        out_shape=jax.ShapeDtypeStruct((length, WIDTH), bf16),
        input_output_aliases=dict(aliases),
        compiler_params=pltpu.CompilerParams(vmem_limit_bytes=8 << 20),
        cost_estimate=pl.CostEstimate(flops=1 << 20, bytes_accessed=4 << 20, transcendentals=0),
        name="place",
    )(order, *arrays)


def exchange(pieces, axes):
    return lax.all_to_all(pieces, axes, split_axis=0, concat_axis=0, tiled=True)


def tied(*arrays):
    return lax.optimization_barrier(arrays)


def along_y(piece, shift):
    ring = lax.axis_size(TP[0])
    return lax.ppermute(piece, TP[0], [(i, (i + shift) % ring) for i in range(ring)])


def across(piece):
    return lax.ppermute(piece, TP[1], [(0, 1), (1, 0)])


def chosen_of(options, index):
    result = options[0]
    for n, option in enumerate(options[1:], 1):
        result = jnp.where(index == n, option, result)
    return result


def both_cores(parts):
    same = jnp.stack(parts)
    return same, across(same)


OFFSETS = (0, -1, 1, 2)


def piece_order(sign):
    ring = lax.axis_size(TP[0])
    y = lax.axis_index(TP[0])
    c = lax.axis_index(TP[1])
    rows = jnp.stack([(y + ring + sign * d) % ring for d in OFFSETS])
    return jnp.concatenate([2 * rows + c, 2 * rows + 1 - c]).astype(jnp.int32)


def send_pieces(pieces):
    ring = lax.axis_size(TP[0])
    got = []
    for k in range(2 * ring):
        step, swap = OFFSETS[k % ring], k // ring
        pairs = [
            (2 * y + c, 2 * ((y - step) % ring) + (c + swap) % 2)
            for y in range(ring)
            for c in range(2)
        ]
        got.append(lax.ppermute(pieces[k], TP, pairs) if k else pieces[0])
    return got


def local(tokens, w_query, w_key, w_value, w_out, query_gain, key_gain, out_gain, chosen):
    length, _ = tokens.shape
    blocks_here = length // BLOCK
    devices = lax.axis_size(KV)
    position = lax.axis_index(KV)
    ranks = lax.axis_size(TP)
    key_row = key_gain[None, :]
    query_row = (query_gain * (HEAD_DIM ** (-0.5) * LOG2E))[None, :]

    rank = lax.axis_index(TP).astype(jnp.int32).reshape(1)
    long, side = lax.axis_size(KV[0]), lax.axis_size(KV[1])
    z, x = lax.axis_index(KV[0]), lax.axis_index(KV[1])
    columns = token_shares(rank, tokens, long, side)
    chosen, *columns = tied(chosen, *columns)
    columns = columns[:1] + [lax.ppermute(columns[n], KV, [(0, n * side)]) for n in range(1, long)]

    usable = chosen >= 0
    pick = jnp.where(usable, chosen, 0)
    owner_of = pick // blocks_here
    all_blocks = jnp.arange(devices * blocks_here, dtype=jnp.int32)
    marked = jnp.where(usable & (owner_of != position), chosen, -1)
    wanted = jnp.any(marked[:, :, None] == all_blocks[None, None, :], axis=(0, 1)).reshape(
        devices, blocks_here
    )
    rank_of = jnp.cumsum(wanted.astype(jnp.int32), axis=1) - 1
    local_ids = jnp.arange(blocks_here, dtype=jnp.int32)
    places = wanted[:, :, None] & (
        rank_of[:, :, None] == jnp.arange(HOT, dtype=jnp.int32)[None, None, :]
    )
    named = jnp.sum(jnp.where(places, local_ids[None, :, None], 0), axis=1).astype(jnp.int32)
    requests = jnp.concatenate([named, jnp.broadcast_to(named[:1], named.shape)], axis=1)
    order = piece_order(1)
    toward = piece_order(-1)
    same_order = jnp.arange(ranks, dtype=jnp.int32)

    asked = exchange(requests, KV)
    pairs = project_kv(tokens, w_key, w_value, key_row).reshape(-1, WIDTH)
    asked_near = asked[:, :REACH].reshape(-1)
    asked_hot = asked[:, HOT:].reshape(-1)

    sent = gather_near(asked_near, pairs)
    sent, *columns = tied(sent, *columns)
    held = [chosen_of([c[n] for c in columns], z) for n in range(side)]
    starts = range(0, devices, side)
    held = held[:1] + [
        lax.ppermute(held[n], KV, [(i, i + n) for i in starts]) for n in range(1, side)
    ]
    near = exchange(sent.reshape(devices, -1, WIDTH), KV).reshape(-1, WIDTH)
    shares = chosen_of(held, x)
    parts = [shares] + [along_y(shares, shift) for shift in (1, -1, 2)]
    w_after = along_y(w_out, 1)
    w_own = across(w_out)
    again, sent = tied(tokens, sent)
    queries = project_q(again, w_query, query_row)
    queries, *parts = tied(queries, *parts)
    rows_same, rows_other = both_cores(parts)
    sent_hot = project_sent(
        asked_hot, order, rows_same, rows_other, w_key, w_value, key_row, devices
    )
    pick, owner_of, rank_of, usable, sent_hot = tied(pick, owner_of, rank_of, usable, sent_hot)
    flat_rank = rank_of.reshape(-1)
    slot_rank = jnp.sum(
        jnp.where(pick[:, :, None] == all_blocks[None, None, :], flat_rank[None, None, :], 0), axis=-1
    )
    near_at = blocks_here + owner_of * REACH + slot_rank
    hot_at = blocks_here + devices * REACH + slot_rank
    at = jnp.where(
        owner_of == position, pick % blocks_here, jnp.where(owner_of == 0, hot_at, near_at)
    )
    at = jnp.where(usable, at, 0).astype(jnp.int32).reshape(-1)
    mask = jnp.repeat(usable.astype(f32), BLOCK, axis=1)

    order, toward, same_order, sent_hot = tied(order, toward, same_order, sent_hot)
    near, sent_hot = tied(near, sent_hot)
    hot = exchange(sent_hot, KV)
    w_before = along_y(w_out, -1)
    w_far = along_y(w_after, 1)

    gains = out_gain.reshape(ranks, 1, WIDTH)
    early = (FIRST_BLOCKS * blocks_here) // 8
    first = attend(0, early, False, at, same_order, queries, mask, pairs, near, hot)
    first = exchange(first, TP)
    second = attend(early, blocks_here - early, True, at, toward, queries, mask, pairs, near, hot)
    *second, w_after, w_before, w_far = tied(*second, w_after, w_before, w_far)
    w_swapped = [across(w_after), across(w_before), across(w_far)]
    weights = [w_out, w_after, w_before, w_far, w_own] + w_swapped
    second = send_pieces(second)
    first = project_out(False, order, same_order, first, weights, gains)
    moved = exchange(first, TP)
    second = tied(first, *second)[1:]
    second = project_out(True, order, toward, second, weights, gains)
    second = send_pieces(second)
    filled = place(place_whole_kernel, length, order, moved.reshape(-1, WIDTH), second[0])
    return place(place_parts_kernel, length, order, filled, *second[1:], aliases={1: 0})


def solution(mesh):
    split = Mesh(mesh.devices.reshape(4, 4, 4, 2), KV + TP)
    return jax.shard_map(
        local,
        mesh=split,
        in_specs=(
            P(KV, None),
            P(None, TP),
            P(None, TP),
            P(None, TP),
            P(TP, None),
            P(),
            P(),
            P(),
            P(KV, None),
        ),
        out_specs=P(KV, TP),
        check_vma=False,
    )
```

```python
import functools

import jax
import jax.numpy as jnp
from jax import lax
from jax.experimental import pallas as pl
from jax.experimental.pallas import tpu as pltpu
from jax.sharding import Mesh
from jax.sharding import PartitionSpec as P

HEAD_DIM = 128
BLOCK = 64
HOT = 8
REACH = 2
FIRST_BLOCKS = 4
KV = ("kv_0", "kv_1")
TP = ("tp_0", "tp_1")
WIDTH = 256
PAIR = 2
norm_eps = 1e-06
LOG2E = 1.4426950408889634
bf16 = jnp.bfloat16
f32 = jnp.float32
VMEM_LIMIT = 60 * 1024 * 1024
KERNEL_LIMIT = 48 * 1024 * 1024


def head_norm(values, gain_row):
    factor = lax.rsqrt(jnp.mean(values * values, axis=-1, keepdims=True) + norm_eps)
    return (values * factor * gain_row).astype(bf16)


def share_kernel(rank, tok, *outs):
    rows = tok[...].astype(f32)
    side, small, _ = outs[0].shape
    devices = len(outs) * side
    part = BLOCK // devices
    for k in range(small // 16):
        parts = []
        for b in range(16 // part):
            first = (k * (16 // part) + b) * BLOCK
            parts.append(rows[first : first + BLOCK].reshape(devices, part, WIDTH))
        joined = jnp.concatenate(parts, axis=1).astype(bf16)
        for n, out in enumerate(outs):
            out[:, k * 16 : (k + 1) * 16, :] = joined[n * side : (n + 1) * side]


def token_shares(rank, tokens, long, side):
    length = tokens.shape[0]
    devices = long * side
    tile = 1024
    return pl.pallas_call(
        share_kernel,
        grid_spec=pltpu.PrefetchScalarGridSpec(
            num_scalar_prefetch=1,
            grid=(length // tile,),
            in_specs=[pl.BlockSpec((tile, WIDTH), lambda i, rank: (i, rank[0]))],
            out_specs=[pl.BlockSpec((side, tile // devices, WIDTH), lambda i, rank: (0, i, 0))] * long,
        ),
        out_shape=[jax.ShapeDtypeStruct((side, length // devices, WIDTH), bf16)] * long,
        compiler_params=pltpu.CompilerParams(vmem_limit_bytes=VMEM_LIMIT),
        cost_estimate=pl.CostEstimate(flops=1 << 20, bytes_accessed=4 << 20, transcendentals=0),
        name="token_shares",
    )(rank, tokens)


def kv_kernel(tok, wk, wv, gain, out):
    rows = tok[...]
    keys = jnp.dot(rows, wk[...], preferred_element_type=f32)
    blocks = out.shape[0]
    for h in range(2):
        lanes = slice(h * HEAD_DIM, (h + 1) * HEAD_DIM)
        normed = head_norm(keys[:, lanes], gain[...])
        out[:, 0, :, lanes] = normed.reshape(blocks, BLOCK, HEAD_DIM)
    vals = jnp.dot(rows, wv[...], preferred_element_type=f32).astype(bf16)
    out[:, 1, :, :] = vals.reshape(blocks, BLOCK, WIDTH)


def project_kv(tokens, w_key, w_value, gain):
    length, depth = tokens.shape
    tile = 1024
    blocks = tile // BLOCK
    return pl.pallas_call(
        kv_kernel,
        grid=(length // tile,),
        in_specs=[
            pl.BlockSpec((tile, depth), lambda i: (i, 0)),
            pl.BlockSpec((depth, WIDTH), lambda i: (0, 0)),
            pl.BlockSpec((depth, WIDTH), lambda i: (0, 0)),
            pl.BlockSpec((1, HEAD_DIM), lambda i: (0, 0)),
        ],
        out_specs=pl.BlockSpec((blocks, PAIR, BLOCK, WIDTH), lambda i: (i, 0, 0, 0)),
        out_shape=jax.ShapeDtypeStruct((length // BLOCK, PAIR, BLOCK, WIDTH), bf16),
        compiler_params=pltpu.CompilerParams(vmem_limit_bytes=VMEM_LIMIT),
        cost_estimate=pl.CostEstimate(
            flops=4 * length * depth * WIDTH, bytes_accessed=2 * length * depth, transcendentals=0
        ),
        name="project_kv",
    )(tokens, w_key, w_value, gain)


def q_kernel(tok, wq, gain, out):
    values = jnp.dot(tok[...], wq[...], preferred_element_type=f32)
    for h in range(2):
        lanes = slice(h * HEAD_DIM, (h + 1) * HEAD_DIM)
        out[:, lanes] = head_norm(values[:, lanes], gain[...])


def project_q(tokens, w_query, gain):
    length, depth = tokens.shape
    tile = 1024
    return pl.pallas_call(
        q_kernel,
        grid=(length // tile,),
        in_specs=[
            pl.BlockSpec((tile, depth), lambda i: (i, 0)),
            pl.BlockSpec((depth, WIDTH), lambda i: (0, 0)),
            pl.BlockSpec((1, HEAD_DIM), lambda i: (0, 0)),
        ],
        out_specs=pl.BlockSpec((tile, WIDTH), lambda i: (i, 0)),
        out_shape=jax.ShapeDtypeStruct((length, WIDTH), bf16),
        compiler_params=pltpu.CompilerParams(vmem_limit_bytes=VMEM_LIMIT),
        cost_estimate=pl.CostEstimate(
            flops=2 * length * depth * WIDTH, bytes_accessed=2 * length * depth, transcendentals=0
        ),
        name="project_q",
    )(tokens, w_query, gain)


def near_kernel(near, pairs, out, room, in_sems, out_sems):
    unit = PAIR * BLOCK
    coming, going = [], []
    for m in range(near.shape[0]):
        first = pl.multiple_of(near[m] * unit, unit)
        coming.append(
            pltpu.make_async_copy(pairs.at[pl.ds(first, unit)], room.at[m], in_sems.at[m])
        )
        going.append(pltpu.make_async_copy(room.at[m], out.at[m], out_sems.at[m]))
    for copy in coming:
        copy.start()
    for n, copy in enumerate(coming):
        copy.wait()
        going[n].start()
    for copy in going:
        copy.wait()


def gather_near(near, pairs):
    anywhere = pl.BlockSpec(memory_space=pl.ANY)
    sends = near.shape[0]
    return pl.pallas_call(
        near_kernel,
        grid_spec=pltpu.PrefetchScalarGridSpec(
            num_scalar_prefetch=1,
            grid=(1,),
            in_specs=[anywhere],
            out_specs=anywhere,
            scratch_shapes=[
                pltpu.VMEM((sends, PAIR * BLOCK, WIDTH), bf16),
                pltpu.SemaphoreType.DMA((sends,)),
                pltpu.SemaphoreType.DMA((sends,)),
            ],
        ),
        out_shape=jax.ShapeDtypeStruct((sends, PAIR * BLOCK, WIDTH), bf16),
        compiler_params=pltpu.CompilerParams(vmem_limit_bytes=VMEM_LIMIT),
        cost_estimate=pl.CostEstimate(flops=1 << 20, bytes_accessed=4 << 20, transcendentals=0),
        name="gather_near",
    )(near, pairs)


def send_kernel(asked, order, same, other, wk, wv, gain, out, keep):
    devices, rows, _ = out.shape
    keys = jnp.zeros((same.shape[1], WIDTH), f32)
    vals = jnp.zeros((same.shape[1], WIDTH), f32)
    count = same.shape[0]
    for k in range(2 * count):
        tokens = same[k] if k < count else other[k - count]
        span = pl.ds(pl.multiple_of(order[k] * WIDTH, WIDTH), WIDTH)
        keys += jnp.dot(tokens, wk[span, :], preferred_element_type=f32)
        vals += jnp.dot(tokens, wv[span, :], preferred_element_type=f32)
    groups, unit, _ = keep.shape
    part = unit // 2
    for h in range(2):
        lanes = slice(h * HEAD_DIM, (h + 1) * HEAD_DIM)
        x = keys[:, lanes]
        factor = lax.rsqrt(jnp.mean(x * x, axis=-1, keepdims=True) + norm_eps)
        keep[:, :part, lanes] = (x * factor * gain[...]).reshape(groups, part, HEAD_DIM)
    keep[:, part:, :] = vals.reshape(groups, part, WIDTH)

    twos = rows // (2 * unit)

    def one(m, carry):
        both = jnp.concatenate([keep[asked[2 * m]], keep[asked[2 * m + 1]]], axis=0)
        at = pl.multiple_of((m % twos) * 2 * unit, 2 * unit)
        out[m // twos, pl.ds(at, 2 * unit), :] = both.astype(bf16)
        return carry

    lax.fori_loop(0, devices * twos, one, 0, unroll=4)


def whole_block(*shape):
    return pl.BlockSpec(shape, lambda i, *_: (0,) * len(shape))


def project_sent(asked, order, same, other, w_key, w_value, gain, devices):
    count, rows, _ = same.shape
    groups = 64
    unit = 2 * rows // groups
    depth = w_key.shape[0]
    shape = (devices, (asked.shape[0] // devices) * unit, WIDTH)
    return pl.pallas_call(
        send_kernel,
        grid_spec=pltpu.PrefetchScalarGridSpec(
            num_scalar_prefetch=2,
            grid=(1,),
            in_specs=[
                whole_block(count, rows, WIDTH),
                whole_block(count, rows, WIDTH),
                whole_block(depth, WIDTH),
                whole_block(depth, WIDTH),
                whole_block(1, HEAD_DIM),
            ],
            out_specs=whole_block(*shape),
            scratch_shapes=[pltpu.VMEM((groups, unit, WIDTH), f32)],
        ),
        out_shape=jax.ShapeDtypeStruct(shape, bf16),
        compiler_params=pltpu.CompilerParams(vmem_limit_bytes=VMEM_LIMIT),
        cost_estimate=pl.CostEstimate(
            flops=4 * rows * depth * WIDTH, bytes_accessed=8 << 20, transcendentals=0
        ),
        name="project_sent",
    )(asked, order, same, other, w_key, w_value, gain)


def attention_kernel(first, at, where, queries, masks, pairs, near, hot, *rest):
    outs, (q, mask, table, raw, sems) = rest[:-5], rest[-5:]
    devices, hot_rows, _ = hot.shape
    here = pairs.shape[0]
    plain = near.shape[0]
    used = pl.ds(0, (first + mask.shape[0]) * PAIR * BLOCK)
    copies = [
        pltpu.make_async_copy(hot, raw, sems.at[0]),
        pltpu.make_async_copy(pairs.at[used], table.at[used], sems.at[1]),
        pltpu.make_async_copy(near, table.at[pl.ds(here, plain)], sems.at[2]),
        pltpu.make_async_copy(queries.at[pl.ds(first * BLOCK, q.shape[0])], q, sems.at[3]),
        pltpu.make_async_copy(masks.at[pl.ds(first, mask.shape[0])], mask, sems.at[4]),
    ]
    for copy in copies:
        copy.start()
    copies[0].wait()
    part = BLOCK // devices
    for n in range(hot_rows // 16):
        both = raw[:, n * 16 : (n + 1) * 16, :].astype(f32)
        for m in range(2):
            start = here + plain + (2 * n + m) * PAIR * BLOCK
            for kind in range(PAIR):
                low = m * 2 * part + kind * part
                piece = both[:, low : low + part, :].reshape(BLOCK, WIDTH).astype(bf16)
                table[start + kind * BLOCK : start + (kind + 1) * BLOCK, :] = piece
    for copy in copies[1:]:
        copy.wait()
    slots = mask.shape[1] // BLOCK
    count = where.shape[0]
    whole = len(outs) == 1
    per_piece = mask.shape[0] // count
    blank = jnp.zeros((BLOCK, HEAD_DIM), bf16)

    def load(block):
        row = pl.multiple_of(block * BLOCK, BLOCK)
        rows = q[pl.ds(row, BLOCK), :]
        both = jnp.concatenate(
            [
                jnp.concatenate([rows[:, :HEAD_DIM], blank], axis=1),
                jnp.concatenate([blank, rows[:, HEAD_DIM:]], axis=1),
            ],
            axis=0,
        )
        base = (first + block) * slots
        return both, [
            pl.multiple_of(at[base + j] * PAIR * BLOCK, PAIR * BLOCK) for j in range(slots)
        ]

    def piece_of(n, put):
        items = [load(where[n] * per_piece + i) for i in range(per_piece)]
        logits = []
        for both, picks in items:
            keys = jnp.concatenate([table[pl.ds(p, BLOCK), :] for p in picks], axis=0)
            logits.append(
                lax.dot_general(both, keys, (((1,), (1,)), ((), ())), preferred_element_type=f32)
            )
        weights = []
        for i in range(per_piece):
            block = where[n] * per_piece + i
            weights.append(jnp.exp2(logits[i]) * mask[pl.ds(block, 1), :])
        for i, (both, picks) in enumerate(items):
            values = jnp.concatenate(
                [table[pl.ds(p + BLOCK, BLOCK), :] for p in picks], axis=0
            )
            sums = jnp.dot(weights[i].astype(bf16), values, preferred_element_type=f32)
            scale = 1.0 / jnp.sum(weights[i], axis=-1, keepdims=True)
            to = slice(i * BLOCK, (i + 1) * BLOCK)
            put(to, slice(0, HEAD_DIM), sums[:BLOCK, :HEAD_DIM] * scale[:BLOCK])
            put(to, slice(HEAD_DIM, WIDTH), sums[BLOCK:, HEAD_DIM:] * scale[BLOCK:])

    if whole:

        def one(n, carry):
            def put(rows, lanes, value):
                outs[0][n, rows, lanes] = value.astype(bf16)

            piece_of(n, put)
            return carry

        lax.fori_loop(0, count, one, 0)
    else:
        for n in range(count):

            def put(rows, lanes, value, n=n):
                outs[n % len(outs)][n // len(outs), rows, lanes] = value.astype(bf16)

            piece_of(n, put)


def attend(first, blocks, split, at, where, queries, mask, pairs, near, hot):
    ranks = where.shape[0]
    length = blocks * BLOCK
    slots = mask.shape[1] // BLOCK
    rows = length // ranks
    anywhere = pl.BlockSpec(memory_space=pl.ANY)
    shape = (2, rows, WIDTH) if split else (ranks, rows, WIDTH)
    count = ranks // 2 if split else 1
    height = pairs.shape[0] + near.shape[0] + HOT * PAIR * BLOCK
    outs = pl.pallas_call(
        functools.partial(attention_kernel, first),
        grid_spec=pltpu.PrefetchScalarGridSpec(
            num_scalar_prefetch=2,
            grid=(1,),
            in_specs=[
                anywhere,
                anywhere,
                anywhere,
                anywhere,
                anywhere,
            ],
            out_specs=[whole_block(*shape)] * count,
            scratch_shapes=[
                pltpu.VMEM((length, WIDTH), bf16),
                pltpu.VMEM((blocks, slots * BLOCK), f32),
                pltpu.VMEM((height, WIDTH), bf16),
                pltpu.VMEM(hot.shape, bf16),
                pltpu.SemaphoreType.DMA((5,)),
            ],
        ),
        out_shape=[jax.ShapeDtypeStruct(shape, bf16)] * count,
        compiler_params=pltpu.CompilerParams(vmem_limit_bytes=VMEM_LIMIT),
        cost_estimate=pl.CostEstimate(
            flops=8 * length * WIDTH * slots * BLOCK, bytes_accessed=10 << 20, transcendentals=0
        ),
        name="attend",
    )(at, where, queries, mask, pairs, near, hot)
    return list(outs) if split else outs[0]


def out_kernel(order, slot, *refs):
    count = order.shape[0]
    n = pl.program_id(0)
    if len(refs) > 2 * count + 4:
        pieces = [ref.at[0] for ref in refs[: count // 2]] + list(refs[count // 2 : count])
        refs = refs[count:]
    else:
        pieces, refs = [refs[0].at[order[k]] for k in range(count)], refs[1:]
    weights, gain, refs = refs[:count], refs[count], refs[count + 1 :]
    outs, (mixed, squares) = refs[:-2], refs[-2:]
    rows = jnp.concatenate([piece[...] for piece in pieces], axis=1)
    weight = jnp.concatenate([w[...] for w in weights], axis=0)
    sums = jnp.dot(rows, weight, preferred_element_type=f32)
    tile = sums.shape[1]
    for i in range(tile // WIDTH):
        mixed[(tile // WIDTH) * n + i] = sums[:, i * WIDTH : (i + 1) * WIDTH]
    part = sum(sums[:, i : i + 128] * sums[:, i : i + 128] for i in range(0, tile, 128))

    @pl.when(n == 0)
    def _():
        squares[...] = part

    @pl.when(n > 0)
    def _():
        squares[...] += part

    @pl.when(n == pl.num_programs(0) - 1)
    def _():
        total = jnp.sum(squares[...], axis=-1, keepdims=True)
        factor = lax.rsqrt(total * (1.0 / (count * WIDTH)) + norm_eps)
        for k in range(count):
            value = (mixed[slot[k]] * factor * gain[slot[k]]).astype(bf16)
            if len(outs) == 1:
                outs[0][k] = value
            else:
                outs[k][...] = value


def project_out(split, order, slot, pieces, weights, gain):
    count = len(weights)
    pieces = list(pieces) if split else [pieces]
    rows = pieces[0].shape[-2]
    depth, width = weights[0].shape
    tile = 4 * WIDTH
    shape = (rows, WIDTH) if split else (count, rows, WIDTH)
    outs = pl.pallas_call(
        out_kernel,
        grid_spec=pltpu.PrefetchScalarGridSpec(
            num_scalar_prefetch=2,
            grid=(width // tile,),
            in_specs=[whole_block(*piece.shape) for piece in pieces]
            + [pl.BlockSpec((depth, tile), lambda n, *_: (0, n))] * count
            + [whole_block(*gain.shape)],
            out_specs=[whole_block(*shape)] * len(pieces),
            scratch_shapes=[
                pltpu.VMEM((count, rows, WIDTH), f32),
                pltpu.VMEM((rows, 128), f32),
            ],
        ),
        out_shape=[jax.ShapeDtypeStruct(shape, bf16)] * len(pieces),
        compiler_params=pltpu.CompilerParams(vmem_limit_bytes=KERNEL_LIMIT),
        cost_estimate=pl.CostEstimate(
            flops=2 * rows * width * width, bytes_accessed=12 << 20, transcendentals=0
        ),
        name="project_out",
    )(order, slot, *pieces, *weights, gain)
    return list(outs) if split else outs[0]


def place_whole_kernel(order, whole, own, out, sems):
    base, rows = whole.shape[0], own.shape[0]
    to = pl.multiple_of(base + order[0] * rows, BLOCK)
    copies = [
        pltpu.make_async_copy(whole, out.at[pl.ds(0, base)], sems.at[0]),
        pltpu.make_async_copy(own, out.at[pl.ds(to, rows)], sems.at[1]),
    ]
    for copy in copies:
        copy.start()
    for copy in copies:
        copy.wait()


def place_parts_kernel(order, filled, *rest):
    parts, out, sems = rest[:-2], rest[-2], rest[-1]
    rows = parts[0].shape[0]
    base = out.shape[0] - (len(parts) + 1) * rows
    copies = []
    for k, part in enumerate(parts):
        to = pl.multiple_of(base + order[k + 1] * rows, BLOCK)
        copies.append(pltpu.make_async_copy(part, out.at[pl.ds(to, rows)], sems.at[k]))
    for copy in copies:
        copy.start()
    for copy in copies:
        copy.wait()


def place(kernel, length, order, *arrays, aliases=()):
    anywhere = pl.BlockSpec(memory_space=pl.ANY)
    return pl.pallas_call(
        kernel,
        grid_spec=pltpu.PrefetchScalarGridSpec(
            num_scalar_prefetch=1,
            grid=(1,),
            in_specs=[anywhere] * len(arrays),
            out_specs=anywhere,
            scratch_shapes=[pltpu.SemaphoreType.DMA((len(arrays),))],
        ),
        out_shape=jax.ShapeDtypeStruct((length, WIDTH), bf16),
        input_output_aliases=dict(aliases),
        compiler_params=pltpu.CompilerParams(vmem_limit_bytes=8 << 20),
        cost_estimate=pl.CostEstimate(flops=1 << 20, bytes_accessed=4 << 20, transcendentals=0),
        name="place",
    )(order, *arrays)


def exchange(pieces, axes):
    return lax.all_to_all(pieces, axes, split_axis=0, concat_axis=0, tiled=True)


def tied(*arrays):
    return lax.optimization_barrier(arrays)


def along_y(piece, shift):
    ring = lax.axis_size(TP[0])
    return lax.ppermute(piece, TP[0], [(i, (i + shift) % ring) for i in range(ring)])


def across(piece):
    return lax.ppermute(piece, TP[1], [(0, 1), (1, 0)])


def chosen_of(options, index):
    result = options[0]
    for n, option in enumerate(options[1:], 1):
        result = jnp.where(index == n, option, result)
    return result


def both_cores(parts):
    same = jnp.stack(parts)
    return same, across(same)


OFFSETS = (0, -1, 1, 2)


def piece_order(sign):
    ring = lax.axis_size(TP[0])
    y = lax.axis_index(TP[0])
    c = lax.axis_index(TP[1])
    rows = jnp.stack([(y + ring + sign * d) % ring for d in OFFSETS])
    return jnp.concatenate([2 * rows + c, 2 * rows + 1 - c]).astype(jnp.int32)


def along_ring(pieces):
    ring = lax.axis_size(TP[0])
    got = [pieces[0]]
    for k in range(1, ring):
        pairs = [(y, (y - OFFSETS[k]) % ring) for y in range(ring)]
        got.append(lax.ppermute(pieces[k], TP[0], pairs))
    return got


def send_pieces(pieces):
    ring = lax.axis_size(TP[0])
    got = []
    for k in range(2 * ring):
        step, swap = OFFSETS[k % ring], k // ring
        pairs = [
            (2 * y + c, 2 * ((y - step) % ring) + (c + swap) % 2)
            for y in range(ring)
            for c in range(2)
        ]
        got.append(lax.ppermute(pieces[k], TP, pairs) if k else pieces[0])
    return got


def local(tokens, w_query, w_key, w_value, w_out, query_gain, key_gain, out_gain, chosen):
    length, _ = tokens.shape
    blocks_here = length // BLOCK
    devices = lax.axis_size(KV)
    position = lax.axis_index(KV)
    ranks = lax.axis_size(TP)
    key_row = key_gain[None, :]
    query_row = (query_gain * (HEAD_DIM ** (-0.5) * LOG2E))[None, :]

    rank = lax.axis_index(TP).astype(jnp.int32).reshape(1)
    long, side = lax.axis_size(KV[0]), lax.axis_size(KV[1])
    z, x = lax.axis_index(KV[0]), lax.axis_index(KV[1])
    columns = token_shares(rank, tokens, long, side)
    chosen, *columns = tied(chosen, *columns)
    columns = columns[:1] + [lax.ppermute(columns[n], KV, [(0, n * side)]) for n in range(1, long)]

    usable = chosen >= 0
    pick = jnp.where(usable, chosen, 0)
    owner_of = pick // blocks_here
    all_blocks = jnp.arange(devices * blocks_here, dtype=jnp.int32)
    marked = jnp.where(usable & (owner_of != position), chosen, -1)
    wanted = jnp.any(marked[:, :, None] == all_blocks[None, None, :], axis=(0, 1)).reshape(
        devices, blocks_here
    )
    rank_of = jnp.cumsum(wanted.astype(jnp.int32), axis=1) - 1
    local_ids = jnp.arange(blocks_here, dtype=jnp.int32)
    places = wanted[:, :, None] & (
        rank_of[:, :, None] == jnp.arange(HOT, dtype=jnp.int32)[None, None, :]
    )
    named = jnp.sum(jnp.where(places, local_ids[None, :, None], 0), axis=1).astype(jnp.int32)
    requests = jnp.concatenate([named, jnp.broadcast_to(named[:1], named.shape)], axis=1)
    order = piece_order(1)
    toward = piece_order(-1)
    same_order = jnp.arange(ranks, dtype=jnp.int32)

    asked = exchange(requests, KV)
    pairs = project_kv(tokens, w_key, w_value, key_row).reshape(-1, WIDTH)
    asked_near = asked[:, :REACH].reshape(-1)
    asked_hot = asked[:, HOT:].reshape(-1)

    sent = gather_near(asked_near, pairs)
    sent, *columns = tied(sent, *columns)
    held = [chosen_of([c[n] for c in columns], z) for n in range(side)]
    starts = range(0, devices, side)
    held = held[:1] + [
        lax.ppermute(held[n], KV, [(i, i + n) for i in starts]) for n in range(1, side)
    ]
    near = exchange(sent.reshape(devices, -1, WIDTH), KV).reshape(-1, WIDTH)
    shares = chosen_of(held, x)
    parts = [shares] + [along_y(shares, shift) for shift in (1, -1, 2)]
    w_after = along_y(w_out, 1)
    w_own = across(w_out)
    again, sent = tied(tokens, sent)
    queries = project_q(again, w_query, query_row)
    queries, *parts = tied(queries, *parts)
    rows_same, rows_other = both_cores(parts)
    sent_hot = project_sent(
        asked_hot, order, rows_same, rows_other, w_key, w_value, key_row, devices
    )
    pick, owner_of, rank_of, usable, sent_hot = tied(pick, owner_of, rank_of, usable, sent_hot)
    flat_rank = rank_of.reshape(-1)
    slot_rank = jnp.sum(
        jnp.where(pick[:, :, None] == all_blocks[None, None, :], flat_rank[None, None, :], 0), axis=-1
    )
    near_at = blocks_here + owner_of * REACH + slot_rank
    hot_at = blocks_here + devices * REACH + slot_rank
    at = jnp.where(
        owner_of == position, pick % blocks_here, jnp.where(owner_of == 0, hot_at, near_at)
    )
    at = jnp.where(usable, at, 0).astype(jnp.int32).reshape(-1)
    mask = jnp.repeat(usable.astype(f32), BLOCK, axis=1)

    order, toward, same_order, sent_hot = tied(order, toward, same_order, sent_hot)
    near, sent_hot = tied(near, sent_hot)
    hot = exchange(sent_hot, KV)
    w_before = along_y(w_out, -1)
    w_far = along_y(w_after, 1)

    gains = out_gain.reshape(ranks, 1, WIDTH)
    early = (FIRST_BLOCKS * blocks_here) // 8
    first = attend(0, early, False, at, same_order, queries, mask, pairs, near, hot)
    first = exchange(first, TP)
    second = attend(early, blocks_here - early, True, at, toward, queries, mask, pairs, near, hot)
    *second, w_after, w_before, w_far = tied(*second, w_after, w_before, w_far)
    w_swapped = [across(w_after), across(w_before), across(w_far)]
    weights = [w_out, w_after, w_before, w_far, w_own] + w_swapped
    second = along_ring(second)
    first = project_out(False, order, same_order, first, weights, gains)
    moved = exchange(first, TP)
    second = list(tied(first, *second)[1:])
    second += [across(pair[1]) for pair in second]
    second = project_out(True, order, toward, second, weights, gains)
    second = send_pieces(second)
    filled = place(place_whole_kernel, length, order, moved.reshape(-1, WIDTH), second[0])
    return place(place_parts_kernel, length, order, filled, *second[1:], aliases={1: 0})


def solution(mesh):
    split = Mesh(mesh.devices.reshape(4, 4, 4, 2), KV + TP)
    return jax.shard_map(
        local,
        mesh=split,
        in_specs=(
            P(KV, None),
            P(None, TP),
            P(None, TP),
            P(None, TP),
            P(TP, None),
            P(),
            P(),
            P(),
            P(KV, None),
        ),
        out_specs=P(KV, TP),
        check_vma=False,
    )
```

```python
import functools

import jax
import jax.numpy as jnp
from jax import lax
from jax.experimental import pallas as pl
from jax.experimental.pallas import tpu as pltpu
from jax.sharding import Mesh
from jax.sharding import PartitionSpec as P

HEAD_DIM = 128
BLOCK = 64
HOT = 8
REACH = 2
FIRST_BLOCKS = 3
KV = ("kv_0", "kv_1")
TP = ("tp_0", "tp_1")
WIDTH = 256
PAIR = 2
norm_eps = 1e-06
LOG2E = 1.4426950408889634
bf16 = jnp.bfloat16
f32 = jnp.float32
VMEM_LIMIT = 60 * 1024 * 1024
KERNEL_LIMIT = 48 * 1024 * 1024


def head_norm(values, gain_row):
    factor = lax.rsqrt(jnp.mean(values * values, axis=-1, keepdims=True) + norm_eps)
    return (values * factor * gain_row).astype(bf16)


def share_kernel(rank, tok, *outs):
    rows = tok[...].astype(f32)
    side, small, _ = outs[0].shape
    devices = len(outs) * side
    part = BLOCK // devices
    for k in range(small // 16):
        parts = []
        for b in range(16 // part):
            first = (k * (16 // part) + b) * BLOCK
            parts.append(rows[first : first + BLOCK].reshape(devices, part, WIDTH))
        joined = jnp.concatenate(parts, axis=1).astype(bf16)
        for n, out in enumerate(outs):
            out[:, k * 16 : (k + 1) * 16, :] = joined[n * side : (n + 1) * side]


def token_shares(rank, tokens, long, side):
    length = tokens.shape[0]
    devices = long * side
    tile = 1024
    return pl.pallas_call(
        share_kernel,
        grid_spec=pltpu.PrefetchScalarGridSpec(
            num_scalar_prefetch=1,
            grid=(length // tile,),
            in_specs=[pl.BlockSpec((tile, WIDTH), lambda i, rank: (i, rank[0]))],
            out_specs=[pl.BlockSpec((side, tile // devices, WIDTH), lambda i, rank: (0, i, 0))] * long,
        ),
        out_shape=[jax.ShapeDtypeStruct((side, length // devices, WIDTH), bf16)] * long,
        compiler_params=pltpu.CompilerParams(vmem_limit_bytes=VMEM_LIMIT),
        cost_estimate=pl.CostEstimate(flops=1 << 20, bytes_accessed=4 << 20, transcendentals=0),
        name="token_shares",
    )(rank, tokens)


def kv_kernel(tok, wk, wv, gain, out):
    rows = tok[...]
    keys = jnp.dot(rows, wk[...], preferred_element_type=f32)
    blocks = out.shape[0]
    for h in range(2):
        lanes = slice(h * HEAD_DIM, (h + 1) * HEAD_DIM)
        normed = head_norm(keys[:, lanes], gain[...])
        out[:, 0, :, lanes] = normed.reshape(blocks, BLOCK, HEAD_DIM)
    vals = jnp.dot(rows, wv[...], preferred_element_type=f32).astype(bf16)
    out[:, 1, :, :] = vals.reshape(blocks, BLOCK, WIDTH)


def project_kv(tokens, w_key, w_value, gain):
    length, depth = tokens.shape
    tile = 1024
    blocks = tile // BLOCK
    return pl.pallas_call(
        kv_kernel,
        grid=(length // tile,),
        in_specs=[
            pl.BlockSpec((tile, depth), lambda i: (i, 0)),
            pl.BlockSpec((depth, WIDTH), lambda i: (0, 0)),
            pl.BlockSpec((depth, WIDTH), lambda i: (0, 0)),
            pl.BlockSpec((1, HEAD_DIM), lambda i: (0, 0)),
        ],
        out_specs=pl.BlockSpec((blocks, PAIR, BLOCK, WIDTH), lambda i: (i, 0, 0, 0)),
        out_shape=jax.ShapeDtypeStruct((length // BLOCK, PAIR, BLOCK, WIDTH), bf16),
        compiler_params=pltpu.CompilerParams(vmem_limit_bytes=VMEM_LIMIT),
        cost_estimate=pl.CostEstimate(
            flops=4 * length * depth * WIDTH, bytes_accessed=2 * length * depth, transcendentals=0
        ),
        name="project_kv",
    )(tokens, w_key, w_value, gain)


def q_kernel(tok, wq, gain, out):
    values = jnp.dot(tok[...], wq[...], preferred_element_type=f32)
    for h in range(2):
        lanes = slice(h * HEAD_DIM, (h + 1) * HEAD_DIM)
        out[:, lanes] = head_norm(values[:, lanes], gain[...])


def project_q(tokens, w_query, gain):
    length, depth = tokens.shape
    tile = 1024
    return pl.pallas_call(
        q_kernel,
        grid=(length // tile,),
        in_specs=[
            pl.BlockSpec((tile, depth), lambda i: (i, 0)),
            pl.BlockSpec((depth, WIDTH), lambda i: (0, 0)),
            pl.BlockSpec((1, HEAD_DIM), lambda i: (0, 0)),
        ],
        out_specs=pl.BlockSpec((tile, WIDTH), lambda i: (i, 0)),
        out_shape=jax.ShapeDtypeStruct((length, WIDTH), bf16),
        compiler_params=pltpu.CompilerParams(vmem_limit_bytes=VMEM_LIMIT),
        cost_estimate=pl.CostEstimate(
            flops=2 * length * depth * WIDTH, bytes_accessed=2 * length * depth, transcendentals=0
        ),
        name="project_q",
    )(tokens, w_query, gain)


def near_kernel(near, pairs, out, room, in_sems, out_sems):
    unit = PAIR * BLOCK
    coming, going = [], []
    for m in range(near.shape[0]):
        first = pl.multiple_of(near[m] * unit, unit)
        coming.append(
            pltpu.make_async_copy(pairs.at[pl.ds(first, unit)], room.at[m], in_sems.at[m])
        )
        going.append(pltpu.make_async_copy(room.at[m], out.at[m], out_sems.at[m]))
    for copy in coming:
        copy.start()
    for n, copy in enumerate(coming):
        copy.wait()
        going[n].start()
    for copy in going:
        copy.wait()


def gather_near(near, pairs):
    anywhere = pl.BlockSpec(memory_space=pl.ANY)
    sends = near.shape[0]
    return pl.pallas_call(
        near_kernel,
        grid_spec=pltpu.PrefetchScalarGridSpec(
            num_scalar_prefetch=1,
            grid=(1,),
            in_specs=[anywhere],
            out_specs=anywhere,
            scratch_shapes=[
                pltpu.VMEM((sends, PAIR * BLOCK, WIDTH), bf16),
                pltpu.SemaphoreType.DMA((sends,)),
                pltpu.SemaphoreType.DMA((sends,)),
            ],
        ),
        out_shape=jax.ShapeDtypeStruct((sends, PAIR * BLOCK, WIDTH), bf16),
        compiler_params=pltpu.CompilerParams(vmem_limit_bytes=VMEM_LIMIT),
        cost_estimate=pl.CostEstimate(flops=1 << 20, bytes_accessed=4 << 20, transcendentals=0),
        name="gather_near",
    )(near, pairs)


def send_kernel(asked, order, same, other, wk, wv, gain, out, keep):
    devices, rows, _ = out.shape
    keys = jnp.zeros((same.shape[1], WIDTH), f32)
    vals = jnp.zeros((same.shape[1], WIDTH), f32)
    count = same.shape[0]
    for k in range(2 * count):
        tokens = same[k] if k < count else other[k - count]
        span = pl.ds(pl.multiple_of(order[k] * WIDTH, WIDTH), WIDTH)
        keys += jnp.dot(tokens, wk[span, :], preferred_element_type=f32)
        vals += jnp.dot(tokens, wv[span, :], preferred_element_type=f32)
    groups, unit, _ = keep.shape
    part = unit // 2
    for h in range(2):
        lanes = slice(h * HEAD_DIM, (h + 1) * HEAD_DIM)
        x = keys[:, lanes]
        factor = lax.rsqrt(jnp.mean(x * x, axis=-1, keepdims=True) + norm_eps)
        keep[:, :part, lanes] = (x * factor * gain[...]).reshape(groups, part, HEAD_DIM)
    keep[:, part:, :] = vals.reshape(groups, part, WIDTH)

    twos = rows // (2 * unit)

    def one(m, carry):
        both = jnp.concatenate([keep[asked[2 * m]], keep[asked[2 * m + 1]]], axis=0)
        at = pl.multiple_of((m % twos) * 2 * unit, 2 * unit)
        out[m // twos, pl.ds(at, 2 * unit), :] = both.astype(bf16)
        return carry

    lax.fori_loop(0, devices * twos, one, 0, unroll=4)


def whole_block(*shape):
    return pl.BlockSpec(shape, lambda i, *_: (0,) * len(shape))


def project_sent(asked, order, same, other, w_key, w_value, gain, devices):
    count, rows, _ = same.shape
    groups = 64
    unit = 2 * rows // groups
    depth = w_key.shape[0]
    shape = (devices, (asked.shape[0] // devices) * unit, WIDTH)
    return pl.pallas_call(
        send_kernel,
        grid_spec=pltpu.PrefetchScalarGridSpec(
            num_scalar_prefetch=2,
            grid=(1,),
            in_specs=[
                whole_block(count, rows, WIDTH),
                whole_block(count, rows, WIDTH),
                whole_block(depth, WIDTH),
                whole_block(depth, WIDTH),
                whole_block(1, HEAD_DIM),
            ],
            out_specs=whole_block(*shape),
            scratch_shapes=[pltpu.VMEM((groups, unit, WIDTH), f32)],
        ),
        out_shape=jax.ShapeDtypeStruct(shape, bf16),
        compiler_params=pltpu.CompilerParams(vmem_limit_bytes=VMEM_LIMIT),
        cost_estimate=pl.CostEstimate(
            flops=4 * rows * depth * WIDTH, bytes_accessed=8 << 20, transcendentals=0
        ),
        name="project_sent",
    )(asked, order, same, other, w_key, w_value, gain)


def attention_kernel(first, at, where, queries, masks, pairs, near, hot, *rest):
    outs, (q, mask, table, raw, sems) = rest[:-5], rest[-5:]
    devices, hot_rows, _ = hot.shape
    here = pairs.shape[0]
    plain = near.shape[0]
    used = pl.ds(0, (first + mask.shape[0]) * PAIR * BLOCK)
    copies = [
        pltpu.make_async_copy(hot, raw, sems.at[0]),
        pltpu.make_async_copy(pairs.at[used], table.at[used], sems.at[1]),
        pltpu.make_async_copy(near, table.at[pl.ds(here, plain)], sems.at[2]),
        pltpu.make_async_copy(queries.at[pl.ds(first * BLOCK, q.shape[0])], q, sems.at[3]),
        pltpu.make_async_copy(masks.at[pl.ds(first, mask.shape[0])], mask, sems.at[4]),
    ]
    for copy in copies:
        copy.start()
    copies[0].wait()
    part = BLOCK // devices
    for n in range(hot_rows // 16):
        both = raw[:, n * 16 : (n + 1) * 16, :].astype(f32)
        for m in range(2):
            start = here + plain + (2 * n + m) * PAIR * BLOCK
            for kind in range(PAIR):
                low = m * 2 * part + kind * part
                piece = both[:, low : low + part, :].reshape(BLOCK, WIDTH).astype(bf16)
                table[start + kind * BLOCK : start + (kind + 1) * BLOCK, :] = piece
    for copy in copies[1:]:
        copy.wait()
    slots = mask.shape[1] // BLOCK
    count = where.shape[0]
    whole = len(outs) == 1
    per_piece = mask.shape[0] // count
    blank = jnp.zeros((BLOCK, HEAD_DIM), bf16)

    def load(block):
        row = pl.multiple_of(block * BLOCK, BLOCK)
        rows = q[pl.ds(row, BLOCK), :]
        both = jnp.concatenate(
            [
                jnp.concatenate([rows[:, :HEAD_DIM], blank], axis=1),
                jnp.concatenate([blank, rows[:, HEAD_DIM:]], axis=1),
            ],
            axis=0,
        )
        base = (first + block) * slots
        return both, [
            pl.multiple_of(at[base + j] * PAIR * BLOCK, PAIR * BLOCK) for j in range(slots)
        ]

    def piece_of(n, put):
        items = [load(where[n] * per_piece + i) for i in range(per_piece)]
        logits = []
        for both, picks in items:
            keys = jnp.concatenate([table[pl.ds(p, BLOCK), :] for p in picks], axis=0)
            logits.append(
                lax.dot_general(both, keys, (((1,), (1,)), ((), ())), preferred_element_type=f32)
            )
        weights = []
        for i in range(per_piece):
            block = where[n] * per_piece + i
            weights.append(jnp.exp2(logits[i]) * mask[pl.ds(block, 1), :])
        for i, (both, picks) in enumerate(items):
            values = jnp.concatenate(
                [table[pl.ds(p + BLOCK, BLOCK), :] for p in picks], axis=0
            )
            sums = jnp.dot(weights[i].astype(bf16), values, preferred_element_type=f32)
            scale = 1.0 / jnp.sum(weights[i], axis=-1, keepdims=True)
            to = slice(i * BLOCK, (i + 1) * BLOCK)
            put(to, slice(0, HEAD_DIM), sums[:BLOCK, :HEAD_DIM] * scale[:BLOCK])
            put(to, slice(HEAD_DIM, WIDTH), sums[BLOCK:, HEAD_DIM:] * scale[BLOCK:])

    if whole:

        def one(n, carry):
            def put(rows, lanes, value):
                outs[0][n, rows, lanes] = value.astype(bf16)

            piece_of(n, put)
            return carry

        lax.fori_loop(0, count, one, 0)
    else:
        for n in range(count):

            def put(rows, lanes, value, n=n):
                outs[n][rows, lanes] = value.astype(bf16)

            piece_of(n, put)


def attend(first, blocks, split, at, where, queries, mask, pairs, near, hot):
    ranks = where.shape[0]
    length = blocks * BLOCK
    slots = mask.shape[1] // BLOCK
    rows = length // ranks
    anywhere = pl.BlockSpec(memory_space=pl.ANY)
    shape = (rows, WIDTH) if split else (ranks, rows, WIDTH)
    count = ranks if split else 1
    height = pairs.shape[0] + near.shape[0] + HOT * PAIR * BLOCK
    outs = pl.pallas_call(
        functools.partial(attention_kernel, first),
        grid_spec=pltpu.PrefetchScalarGridSpec(
            num_scalar_prefetch=2,
            grid=(1,),
            in_specs=[
                anywhere,
                anywhere,
                anywhere,
                anywhere,
                anywhere,
            ],
            out_specs=[whole_block(*shape)] * count,
            scratch_shapes=[
                pltpu.VMEM((length, WIDTH), bf16),
                pltpu.VMEM((blocks, slots * BLOCK), f32),
                pltpu.VMEM((height, WIDTH), bf16),
                pltpu.VMEM(hot.shape, bf16),
                pltpu.SemaphoreType.DMA((5,)),
            ],
        ),
        out_shape=[jax.ShapeDtypeStruct(shape, bf16)] * count,
        compiler_params=pltpu.CompilerParams(vmem_limit_bytes=VMEM_LIMIT),
        cost_estimate=pl.CostEstimate(
            flops=8 * length * WIDTH * slots * BLOCK, bytes_accessed=10 << 20, transcendentals=0
        ),
        name="attend",
    )(at, where, queries, mask, pairs, near, hot)
    return list(outs) if split else outs[0]


def out_kernel(order, slot, *refs):
    count = order.shape[0]
    n = pl.program_id(0)
    if len(refs) > 2 * count + 4:
        pieces, refs = refs[:count], refs[count:]
    else:
        pieces, refs = [refs[0].at[order[k]] for k in range(count)], refs[1:]
    weights, gain, refs = refs[:count], refs[count], refs[count + 1 :]
    outs, (mixed, squares) = refs[:-2], refs[-2:]
    rows = jnp.concatenate([piece[...] for piece in pieces], axis=1)
    weight = jnp.concatenate([w[...] for w in weights], axis=0)
    sums = jnp.dot(rows, weight, preferred_element_type=f32)
    tile = sums.shape[1]
    for i in range(tile // WIDTH):
        mixed[(tile // WIDTH) * n + i] = sums[:, i * WIDTH : (i + 1) * WIDTH]
    part = sum(sums[:, i : i + 128] * sums[:, i : i + 128] for i in range(0, tile, 128))

    @pl.when(n == 0)
    def _():
        squares[...] = part

    @pl.when(n > 0)
    def _():
        squares[...] += part

    @pl.when(n == pl.num_programs(0) - 1)
    def _():
        total = jnp.sum(squares[...], axis=-1, keepdims=True)
        factor = lax.rsqrt(total * (1.0 / (count * WIDTH)) + norm_eps)
        for k in range(count):
            value = (mixed[slot[k]] * factor * gain[slot[k]]).astype(bf16)
            if len(outs) == 1:
                outs[0][k] = value
            else:
                outs[k][...] = value


def project_out(split, order, slot, pieces, weights, gain):
    count = len(weights)
    pieces = list(pieces) if split else [pieces]
    rows = pieces[0].shape[-2]
    depth, width = weights[0].shape
    tile = 4 * WIDTH
    shape = (rows, WIDTH) if split else (count, rows, WIDTH)
    outs = pl.pallas_call(
        out_kernel,
        grid_spec=pltpu.PrefetchScalarGridSpec(
            num_scalar_prefetch=2,
            grid=(width // tile,),
            in_specs=[whole_block(*shape)] * len(pieces)
            + [pl.BlockSpec((depth, tile), lambda n, *_: (0, n))] * count
            + [whole_block(*gain.shape)],
            out_specs=[whole_block(*shape)] * len(pieces),
            scratch_shapes=[
                pltpu.VMEM((count, rows, WIDTH), f32),
                pltpu.VMEM((rows, 128), f32),
            ],
        ),
        out_shape=[jax.ShapeDtypeStruct(shape, bf16)] * len(pieces),
        compiler_params=pltpu.CompilerParams(vmem_limit_bytes=KERNEL_LIMIT),
        cost_estimate=pl.CostEstimate(
            flops=2 * rows * width * width, bytes_accessed=12 << 20, transcendentals=0
        ),
        name="project_out",
    )(order, slot, *pieces, *weights, gain)
    return list(outs) if split else outs[0]


def place_whole_kernel(order, whole, own, out, sems):
    base, rows = whole.shape[0], own.shape[0]
    to = pl.multiple_of(base + order[0] * rows, BLOCK)
    copies = [
        pltpu.make_async_copy(whole, out.at[pl.ds(0, base)], sems.at[0]),
        pltpu.make_async_copy(own, out.at[pl.ds(to, rows)], sems.at[1]),
    ]
    for copy in copies:
        copy.start()
    for copy in copies:
        copy.wait()


def place_parts_kernel(order, filled, *rest):
    parts, out, sems = rest[:-2], rest[-2], rest[-1]
    rows = parts[0].shape[0]
    base = out.shape[0] - (len(parts) + 1) * rows
    copies = []
    for k, part in enumerate(parts):
        to = pl.multiple_of(base + order[k + 1] * rows, BLOCK)
        copies.append(pltpu.make_async_copy(part, out.at[pl.ds(to, rows)], sems.at[k]))
    for copy in copies:
        copy.start()
    for copy in copies:
        copy.wait()


def place(kernel, length, order, *arrays, aliases=()):
    anywhere = pl.BlockSpec(memory_space=pl.ANY)
    return pl.pallas_call(
        kernel,
        grid_spec=pltpu.PrefetchScalarGridSpec(
            num_scalar_prefetch=1,
            grid=(1,),
            in_specs=[anywhere] * len(arrays),
            out_specs=anywhere,
            scratch_shapes=[pltpu.SemaphoreType.DMA((len(arrays),))],
        ),
        out_shape=jax.ShapeDtypeStruct((length, WIDTH), bf16),
        input_output_aliases=dict(aliases),
        compiler_params=pltpu.CompilerParams(vmem_limit_bytes=8 << 20),
        cost_estimate=pl.CostEstimate(flops=1 << 20, bytes_accessed=4 << 20, transcendentals=0),
        name="place",
    )(order, *arrays)


def exchange(pieces, axes):
    return lax.all_to_all(pieces, axes, split_axis=0, concat_axis=0, tiled=True)


def tied(*arrays):
    return lax.optimization_barrier(arrays)


def along_y(piece, shift):
    ring = lax.axis_size(TP[0])
    return lax.ppermute(piece, TP[0], [(i, (i + shift) % ring) for i in range(ring)])


def across(piece):
    return lax.ppermute(piece, TP[1], [(0, 1), (1, 0)])


def chosen_of(options, index):
    result = options[0]
    for n, option in enumerate(options[1:], 1):
        result = jnp.where(index == n, option, result)
    return result


def both_cores(parts):
    same = jnp.stack(parts)
    return same, across(same)


OFFSETS = (0, -1, 1, 2)


def piece_order(sign):
    ring = lax.axis_size(TP[0])
    y = lax.axis_index(TP[0])
    c = lax.axis_index(TP[1])
    rows = jnp.stack([(y + ring + sign * d) % ring for d in OFFSETS])
    return jnp.concatenate([2 * rows + c, 2 * rows + 1 - c]).astype(jnp.int32)


def send_pieces(pieces):
    ring = lax.axis_size(TP[0])
    got = []
    for k in range(2 * ring):
        step, swap = OFFSETS[k % ring], k // ring
        pairs = [
            (2 * y + c, 2 * ((y - step) % ring) + (c + swap) % 2)
            for y in range(ring)
            for c in range(2)
        ]
        got.append(lax.ppermute(pieces[k], TP, pairs) if k else pieces[0])
    return got


def local(tokens, w_query, w_key, w_value, w_out, query_gain, key_gain, out_gain, chosen):
    length, _ = tokens.shape
    blocks_here = length // BLOCK
    devices = lax.axis_size(KV)
    position = lax.axis_index(KV)
    ranks = lax.axis_size(TP)
    key_row = key_gain[None, :]
    query_row = (query_gain * (HEAD_DIM ** (-0.5) * LOG2E))[None, :]

    rank = lax.axis_index(TP).astype(jnp.int32).reshape(1)
    long, side = lax.axis_size(KV[0]), lax.axis_size(KV[1])
    z, x = lax.axis_index(KV[0]), lax.axis_index(KV[1])
    columns = token_shares(rank, tokens, long, side)
    chosen, *columns = tied(chosen, *columns)
    columns = columns[:1] + [lax.ppermute(columns[n], KV, [(0, n * side)]) for n in range(1, long)]

    usable = chosen >= 0
    pick = jnp.where(usable, chosen, 0)
    owner_of = pick // blocks_here
    all_blocks = jnp.arange(devices * blocks_here, dtype=jnp.int32)
    marked = jnp.where(usable & (owner_of != position), chosen, -1)
    wanted = jnp.any(marked[:, :, None] == all_blocks[None, None, :], axis=(0, 1)).reshape(
        devices, blocks_here
    )
    rank_of = jnp.cumsum(wanted.astype(jnp.int32), axis=1) - 1
    local_ids = jnp.arange(blocks_here, dtype=jnp.int32)
    places = wanted[:, :, None] & (
        rank_of[:, :, None] == jnp.arange(HOT, dtype=jnp.int32)[None, None, :]
    )
    named = jnp.sum(jnp.where(places, local_ids[None, :, None], 0), axis=1).astype(jnp.int32)
    requests = jnp.concatenate([named, jnp.broadcast_to(named[:1], named.shape)], axis=1)
    order = piece_order(1)
    toward = piece_order(-1)
    same_order = jnp.arange(ranks, dtype=jnp.int32)

    asked = exchange(requests, KV)
    pairs = project_kv(tokens, w_key, w_value, key_row).reshape(-1, WIDTH)
    asked_near = asked[:, :REACH].reshape(-1)
    asked_hot = asked[:, HOT:].reshape(-1)

    sent = gather_near(asked_near, pairs)
    sent, *columns = tied(sent, *columns)
    held = [chosen_of([c[n] for c in columns], z) for n in range(side)]
    starts = range(0, devices, side)
    held = held[:1] + [
        lax.ppermute(held[n], KV, [(i, i + n) for i in starts]) for n in range(1, side)
    ]
    near = exchange(sent.reshape(devices, -1, WIDTH), KV).reshape(-1, WIDTH)
    shares = chosen_of(held, x)
    parts = [shares] + [along_y(shares, shift) for shift in (1, -1, 2)]
    w_after = along_y(w_out, 1)
    w_own = across(w_out)
    again, sent = tied(tokens, sent)
    queries = project_q(again, w_query, query_row)
    queries, *parts = tied(queries, *parts)
    rows_same, rows_other = both_cores(parts)
    sent_hot = project_sent(
        asked_hot, order, rows_same, rows_other, w_key, w_value, key_row, devices
    )
    pick, owner_of, rank_of, usable, sent_hot = tied(pick, owner_of, rank_of, usable, sent_hot)
    flat_rank = rank_of.reshape(-1)
    slot_rank = jnp.sum(
        jnp.where(pick[:, :, None] == all_blocks[None, None, :], flat_rank[None, None, :], 0), axis=-1
    )
    near_at = blocks_here + owner_of * REACH + slot_rank
    hot_at = blocks_here + devices * REACH + slot_rank
    at = jnp.where(
        owner_of == position, pick % blocks_here, jnp.where(owner_of == 0, hot_at, near_at)
    )
    at = jnp.where(usable, at, 0).astype(jnp.int32).reshape(-1)
    mask = jnp.repeat(usable.astype(f32), BLOCK, axis=1)

    order, toward, same_order, sent_hot = tied(order, toward, same_order, sent_hot)
    near, sent_hot = tied(near, sent_hot)
    hot = exchange(sent_hot, KV)
    w_before = along_y(w_out, -1)
    w_far = along_y(w_after, 1)

    gains = out_gain.reshape(ranks, 1, WIDTH)
    early = (FIRST_BLOCKS * blocks_here) // 8
    first = attend(0, early, False, at, same_order, queries, mask, pairs, near, hot)
    first = exchange(first, TP)
    second = attend(early, blocks_here - early, True, at, toward, queries, mask, pairs, near, hot)
    *second, w_after, w_before, w_far = tied(*second, w_after, w_before, w_far)
    w_swapped = [across(w_after), across(w_before), across(w_far)]
    weights = [w_out, w_after, w_before, w_far, w_own] + w_swapped
    second = send_pieces(second)
    first = project_out(False, order, same_order, first, weights, gains)
    moved = exchange(first, TP)
    second = tied(first, *second)[1:]
    second = project_out(True, order, toward, second, weights, gains)
    second = send_pieces(second)
    filled = place(place_whole_kernel, length, order, moved.reshape(-1, WIDTH), second[0])
    return place(place_parts_kernel, length, order, filled, *second[1:], aliases={1: 0})


def solution(mesh):
    split = Mesh(mesh.devices.reshape(4, 4, 4, 2), KV + TP)
    return jax.shard_map(
        local,
        mesh=split,
        in_specs=(
            P(KV, None),
            P(None, TP),
            P(None, TP),
            P(None, TP),
            P(TP, None),
            P(),
            P(),
            P(),
            P(KV, None),
        ),
        out_specs=P(KV, TP),
        check_vma=False,
    )
```

```python
import functools

import jax
import jax.numpy as jnp
from jax import lax
from jax.experimental import pallas as pl
from jax.experimental.pallas import tpu as pltpu
from jax.sharding import Mesh
from jax.sharding import PartitionSpec as P

HEAD_DIM = 128
BLOCK = 64
HOT = 8
REACH = 2
FIRST_BLOCKS = 4
KV = ("kv_0", "kv_1")
TP = ("tp_0", "tp_1")
WIDTH = 256
PAIR = 2
norm_eps = 1e-06
LOG2E = 1.4426950408889634
bf16 = jnp.bfloat16
f32 = jnp.float32
VMEM_LIMIT = 60 * 1024 * 1024
KERNEL_LIMIT = 48 * 1024 * 1024


def head_norm(values, gain_row):
    factor = lax.rsqrt(jnp.mean(values * values, axis=-1, keepdims=True) + norm_eps)
    return (values * factor * gain_row).astype(bf16)


def share_kernel(rank, tok, *outs):
    rows = tok[...].astype(f32)
    side, small, _ = outs[0].shape
    devices = len(outs) * side
    part = BLOCK // devices
    for k in range(small // 16):
        parts = []
        for b in range(16 // part):
            first = (k * (16 // part) + b) * BLOCK
            parts.append(rows[first : first + BLOCK].reshape(devices, part, WIDTH))
        joined = jnp.concatenate(parts, axis=1).astype(bf16)
        for n, out in enumerate(outs):
            out[:, k * 16 : (k + 1) * 16, :] = joined[n * side : (n + 1) * side]


def token_shares(rank, tokens, long, side):
    length = tokens.shape[0]
    devices = long * side
    tile = 4096
    return pl.pallas_call(
        share_kernel,
        grid_spec=pltpu.PrefetchScalarGridSpec(
            num_scalar_prefetch=1,
            grid=(length // tile,),
            in_specs=[pl.BlockSpec((tile, WIDTH), lambda i, rank: (i, rank[0]))],
            out_specs=[pl.BlockSpec((side, tile // devices, WIDTH), lambda i, rank: (0, i, 0))] * long,
        ),
        out_shape=[jax.ShapeDtypeStruct((side, length // devices, WIDTH), bf16)] * long,
        compiler_params=pltpu.CompilerParams(vmem_limit_bytes=VMEM_LIMIT),
        cost_estimate=pl.CostEstimate(flops=1 << 20, bytes_accessed=4 << 20, transcendentals=0),
        name="token_shares",
    )(rank, tokens)


def kv_kernel(tok, wk, wv, gain, out):
    rows = tok[...]
    keys = jnp.dot(rows, wk[...], preferred_element_type=f32)
    blocks = out.shape[0]
    for h in range(2):
        lanes = slice(h * HEAD_DIM, (h + 1) * HEAD_DIM)
        normed = head_norm(keys[:, lanes], gain[...])
        out[:, 0, :, lanes] = normed.reshape(blocks, BLOCK, HEAD_DIM)
    vals = jnp.dot(rows, wv[...], preferred_element_type=f32).astype(bf16)
    out[:, 1, :, :] = vals.reshape(blocks, BLOCK, WIDTH)


def project_kv(tokens, w_key, w_value, gain):
    length, depth = tokens.shape
    tile = 1024
    blocks = tile // BLOCK
    return pl.pallas_call(
        kv_kernel,
        grid=(length // tile,),
        in_specs=[
            pl.BlockSpec((tile, depth), lambda i: (i, 0)),
            pl.BlockSpec((depth, WIDTH), lambda i: (0, 0)),
            pl.BlockSpec((depth, WIDTH), lambda i: (0, 0)),
            pl.BlockSpec((1, HEAD_DIM), lambda i: (0, 0)),
        ],
        out_specs=pl.BlockSpec((blocks, PAIR, BLOCK, WIDTH), lambda i: (i, 0, 0, 0)),
        out_shape=jax.ShapeDtypeStruct((length // BLOCK, PAIR, BLOCK, WIDTH), bf16),
        compiler_params=pltpu.CompilerParams(vmem_limit_bytes=VMEM_LIMIT),
        cost_estimate=pl.CostEstimate(
            flops=4 * length * depth * WIDTH, bytes_accessed=2 * length * depth, transcendentals=0
        ),
        name="project_kv",
    )(tokens, w_key, w_value, gain)


def q_kernel(tok, wq, gain, out):
    values = jnp.dot(tok[...], wq[...], preferred_element_type=f32)
    for h in range(2):
        lanes = slice(h * HEAD_DIM, (h + 1) * HEAD_DIM)
        out[:, lanes] = head_norm(values[:, lanes], gain[...])


def project_q(tokens, w_query, gain):
    length, depth = tokens.shape
    tile = 1024
    return pl.pallas_call(
        q_kernel,
        grid=(length // tile,),
        in_specs=[
            pl.BlockSpec((tile, depth), lambda i: (i, 0)),
            pl.BlockSpec((depth, WIDTH), lambda i: (0, 0)),
            pl.BlockSpec((1, HEAD_DIM), lambda i: (0, 0)),
        ],
        out_specs=pl.BlockSpec((tile, WIDTH), lambda i: (i, 0)),
        out_shape=jax.ShapeDtypeStruct((length, WIDTH), bf16),
        compiler_params=pltpu.CompilerParams(vmem_limit_bytes=VMEM_LIMIT),
        cost_estimate=pl.CostEstimate(
            flops=2 * length * depth * WIDTH, bytes_accessed=2 * length * depth, transcendentals=0
        ),
        name="project_q",
    )(tokens, w_query, gain)


def near_kernel(near, pairs, out, room, in_sems, out_sems):
    unit = PAIR * BLOCK
    coming, going = [], []
    for m in range(near.shape[0]):
        first = pl.multiple_of(near[m] * unit, unit)
        coming.append(
            pltpu.make_async_copy(pairs.at[pl.ds(first, unit)], room.at[m], in_sems.at[m])
        )
        going.append(pltpu.make_async_copy(room.at[m], out.at[m], out_sems.at[m]))
    for copy in coming:
        copy.start()
    for n, copy in enumerate(coming):
        copy.wait()
        going[n].start()
    for copy in going:
        copy.wait()


def gather_near(near, pairs):
    anywhere = pl.BlockSpec(memory_space=pl.ANY)
    sends = near.shape[0]
    return pl.pallas_call(
        near_kernel,
        grid_spec=pltpu.PrefetchScalarGridSpec(
            num_scalar_prefetch=1,
            grid=(1,),
            in_specs=[anywhere],
            out_specs=anywhere,
            scratch_shapes=[
                pltpu.VMEM((sends, PAIR * BLOCK, WIDTH), bf16),
                pltpu.SemaphoreType.DMA((sends,)),
                pltpu.SemaphoreType.DMA((sends,)),
            ],
        ),
        out_shape=jax.ShapeDtypeStruct((sends, PAIR * BLOCK, WIDTH), bf16),
        compiler_params=pltpu.CompilerParams(vmem_limit_bytes=VMEM_LIMIT),
        cost_estimate=pl.CostEstimate(flops=1 << 20, bytes_accessed=4 << 20, transcendentals=0),
        name="gather_near",
    )(near, pairs)


def send_kernel(asked, order, same, other, wk, wv, gain, out, keep):
    devices, rows, _ = out.shape
    keys = jnp.zeros((same.shape[1], WIDTH), f32)
    vals = jnp.zeros((same.shape[1], WIDTH), f32)
    count = same.shape[0]
    for k in range(2 * count):
        tokens = same[k] if k < count else other[k - count]
        span = pl.ds(pl.multiple_of(order[k] * WIDTH, WIDTH), WIDTH)
        keys += jnp.dot(tokens, wk[span, :], preferred_element_type=f32)
        vals += jnp.dot(tokens, wv[span, :], preferred_element_type=f32)
    groups, unit, _ = keep.shape
    part = unit // 2
    for h in range(2):
        lanes = slice(h * HEAD_DIM, (h + 1) * HEAD_DIM)
        x = keys[:, lanes]
        factor = lax.rsqrt(jnp.mean(x * x, axis=-1, keepdims=True) + norm_eps)
        keep[:, :part, lanes] = (x * factor * gain[...]).reshape(groups, part, HEAD_DIM)
    keep[:, part:, :] = vals.reshape(groups, part, WIDTH)

    twos = rows // (2 * unit)

    def one(m, carry):
        both = jnp.concatenate([keep[asked[2 * m]], keep[asked[2 * m + 1]]], axis=0)
        at = pl.multiple_of((m % twos) * 2 * unit, 2 * unit)
        out[m // twos, pl.ds(at, 2 * unit), :] = both.astype(bf16)
        return carry

    lax.fori_loop(0, devices * twos, one, 0, unroll=4)


def whole_block(*shape):
    return pl.BlockSpec(shape, lambda i, *_: (0,) * len(shape))


def project_sent(asked, order, same, other, w_key, w_value, gain, devices):
    count, rows, _ = same.shape
    groups = 64
    unit = 2 * rows // groups
    depth = w_key.shape[0]
    shape = (devices, (asked.shape[0] // devices) * unit, WIDTH)
    return pl.pallas_call(
        send_kernel,
        grid_spec=pltpu.PrefetchScalarGridSpec(
            num_scalar_prefetch=2,
            grid=(1,),
            in_specs=[
                whole_block(count, rows, WIDTH),
                whole_block(count, rows, WIDTH),
                whole_block(depth, WIDTH),
                whole_block(depth, WIDTH),
                whole_block(1, HEAD_DIM),
            ],
            out_specs=whole_block(*shape),
            scratch_shapes=[pltpu.VMEM((groups, unit, WIDTH), f32)],
        ),
        out_shape=jax.ShapeDtypeStruct(shape, bf16),
        compiler_params=pltpu.CompilerParams(vmem_limit_bytes=VMEM_LIMIT),
        cost_estimate=pl.CostEstimate(
            flops=4 * rows * depth * WIDTH, bytes_accessed=8 << 20, transcendentals=0
        ),
        name="project_sent",
    )(asked, order, same, other, w_key, w_value, gain)


def attention_kernel(first, at, where, queries, masks, pairs, near, hot, *rest):
    outs, (q, mask, table, raw, sems) = rest[:-5], rest[-5:]
    devices, hot_rows, _ = hot.shape
    here = pairs.shape[0]
    plain = near.shape[0]
    count = where.shape[0]
    whole = len(outs) == 1
    steps = 2 if whole else 1
    used = (first + mask.shape[0]) * PAIR * BLOCK // steps
    owns = []
    for n in range(steps):
        span = pl.ds(n * used, used)
        owns.append(pltpu.make_async_copy(pairs.at[span], table.at[span], sems.at[4 + n]))
    copies = [
        pltpu.make_async_copy(hot, raw, sems.at[0]),
        pltpu.make_async_copy(near, table.at[pl.ds(here, plain)], sems.at[1]),
        pltpu.make_async_copy(queries.at[pl.ds(first * BLOCK, q.shape[0])], q, sems.at[2]),
        pltpu.make_async_copy(masks.at[pl.ds(first, mask.shape[0])], mask, sems.at[3]),
    ]
    for copy in copies + owns:
        copy.start()
    copies[0].wait()
    part = BLOCK // devices
    for n in range(hot_rows // 16):
        both = raw[:, n * 16 : (n + 1) * 16, :].astype(f32)
        for m in range(2):
            start = here + plain + (2 * n + m) * PAIR * BLOCK
            for kind in range(PAIR):
                low = m * 2 * part + kind * part
                piece = both[:, low : low + part, :].reshape(BLOCK, WIDTH).astype(bf16)
                table[start + kind * BLOCK : start + (kind + 1) * BLOCK, :] = piece
    for copy in copies[1:]:
        copy.wait()
    slots = mask.shape[1] // BLOCK
    per_piece = mask.shape[0] // count
    blank = jnp.zeros((BLOCK, HEAD_DIM), bf16)

    def load(block):
        row = pl.multiple_of(block * BLOCK, BLOCK)
        rows = q[pl.ds(row, BLOCK), :]
        both = jnp.concatenate(
            [
                jnp.concatenate([rows[:, :HEAD_DIM], blank], axis=1),
                jnp.concatenate([blank, rows[:, HEAD_DIM:]], axis=1),
            ],
            axis=0,
        )
        base = (first + block) * slots
        return both, [
            pl.multiple_of(at[base + j] * PAIR * BLOCK, PAIR * BLOCK) for j in range(slots)
        ]

    def piece_of(n, put):
        items = [load(where[n] * per_piece + i) for i in range(per_piece)]
        logits = []
        for both, picks in items:
            keys = jnp.concatenate([table[pl.ds(p, BLOCK), :] for p in picks], axis=0)
            logits.append(
                lax.dot_general(both, keys, (((1,), (1,)), ((), ())), preferred_element_type=f32)
            )
        weights = []
        for i in range(per_piece):
            block = where[n] * per_piece + i
            weights.append(jnp.exp2(logits[i]) * mask[pl.ds(block, 1), :])
        for i, (both, picks) in enumerate(items):
            values = jnp.concatenate(
                [table[pl.ds(p + BLOCK, BLOCK), :] for p in picks], axis=0
            )
            sums = jnp.dot(weights[i].astype(bf16), values, preferred_element_type=f32)
            scale = 1.0 / jnp.sum(weights[i], axis=-1, keepdims=True)
            to = slice(i * BLOCK, (i + 1) * BLOCK)
            put(to, slice(0, HEAD_DIM), sums[:BLOCK, :HEAD_DIM] * scale[:BLOCK])
            put(to, slice(HEAD_DIM, WIDTH), sums[BLOCK:, HEAD_DIM:] * scale[BLOCK:])

    for n in range(count):
        if n % (count // steps) == 0:
            owns[n // (count // steps)].wait()

        def put(rows, lanes, value, n=n):
            if whole:
                outs[0][n, rows, lanes] = value.astype(bf16)
            else:
                outs[n][rows, lanes] = value.astype(bf16)

        piece_of(n, put)


def attend(first, blocks, split, at, where, queries, mask, pairs, near, hot):
    ranks = where.shape[0]
    length = blocks * BLOCK
    slots = mask.shape[1] // BLOCK
    rows = length // ranks
    anywhere = pl.BlockSpec(memory_space=pl.ANY)
    shape = (rows, WIDTH) if split else (ranks, rows, WIDTH)
    count = ranks if split else 1
    height = pairs.shape[0] + near.shape[0] + HOT * PAIR * BLOCK
    outs = pl.pallas_call(
        functools.partial(attention_kernel, first),
        grid_spec=pltpu.PrefetchScalarGridSpec(
            num_scalar_prefetch=2,
            grid=(1,),
            in_specs=[
                anywhere,
                anywhere,
                anywhere,
                anywhere,
                anywhere,
            ],
            out_specs=[whole_block(*shape)] * count,
            scratch_shapes=[
                pltpu.VMEM((length, WIDTH), bf16),
                pltpu.VMEM((blocks, slots * BLOCK), f32),
                pltpu.VMEM((height, WIDTH), bf16),
                pltpu.VMEM(hot.shape, bf16),
                pltpu.SemaphoreType.DMA((6,)),
            ],
        ),
        out_shape=[jax.ShapeDtypeStruct(shape, bf16)] * count,
        compiler_params=pltpu.CompilerParams(vmem_limit_bytes=VMEM_LIMIT),
        cost_estimate=pl.CostEstimate(
            flops=8 * length * WIDTH * slots * BLOCK, bytes_accessed=10 << 20, transcendentals=0
        ),
        name="attend",
    )(at, where, queries, mask, pairs, near, hot)
    return list(outs) if split else outs[0]


def out_kernel(order, slot, *refs):
    count = order.shape[0]
    n = pl.program_id(0)
    if len(refs) > 2 * count + 4:
        pieces, refs = refs[:count], refs[count:]
    else:
        pieces, refs = [refs[0].at[order[k]] for k in range(count)], refs[1:]
    weights, gain, refs = refs[:count], refs[count], refs[count + 1 :]
    outs, (mixed, squares) = refs[:-2], refs[-2:]
    rows = jnp.concatenate([piece[...] for piece in pieces], axis=1)
    weight = jnp.concatenate([w[...] for w in weights], axis=0)
    sums = jnp.dot(rows, weight, preferred_element_type=f32)
    tile = sums.shape[1]
    for i in range(tile // WIDTH):
        mixed[(tile // WIDTH) * n + i] = sums[:, i * WIDTH : (i + 1) * WIDTH]
    part = sum(sums[:, i : i + 128] * sums[:, i : i + 128] for i in range(0, tile, 128))

    @pl.when(n == 0)
    def _():
        squares[...] = part

    @pl.when(n > 0)
    def _():
        squares[...] += part

    @pl.when(n == pl.num_programs(0) - 1)
    def _():
        total = jnp.sum(squares[...], axis=-1, keepdims=True)
        factor = lax.rsqrt(total * (1.0 / (count * WIDTH)) + norm_eps)
        for k in range(count):
            value = (mixed[slot[k]] * factor * gain[slot[k]]).astype(bf16)
            if len(outs) == 1:
                outs[0][k] = value
            else:
                outs[k][...] = value


def project_out(split, order, slot, pieces, weights, gain):
    count = len(weights)
    pieces = list(pieces) if split else [pieces]
    rows = pieces[0].shape[-2]
    depth, width = weights[0].shape
    tile = 4 * WIDTH
    shape = (rows, WIDTH) if split else (count, rows, WIDTH)
    outs = pl.pallas_call(
        out_kernel,
        grid_spec=pltpu.PrefetchScalarGridSpec(
            num_scalar_prefetch=2,
            grid=(width // tile,),
            in_specs=[whole_block(*shape)] * len(pieces)
            + [pl.BlockSpec((depth, tile), lambda n, *_: (0, n))] * count
            + [whole_block(*gain.shape)],
            out_specs=[whole_block(*shape)] * len(pieces),
            scratch_shapes=[
                pltpu.VMEM((count, rows, WIDTH), f32),
                pltpu.VMEM((rows, 128), f32),
            ],
        ),
        out_shape=[jax.ShapeDtypeStruct(shape, bf16)] * len(pieces),
        compiler_params=pltpu.CompilerParams(vmem_limit_bytes=KERNEL_LIMIT),
        cost_estimate=pl.CostEstimate(
            flops=2 * rows * width * width, bytes_accessed=12 << 20, transcendentals=0
        ),
        name="project_out",
    )(order, slot, *pieces, *weights, gain)
    return list(outs) if split else outs[0]


def place_whole_kernel(order, whole, own, out, sems):
    base, rows = whole.shape[0], own.shape[0]
    to = pl.multiple_of(base + order[0] * rows, BLOCK)
    copies = [
        pltpu.make_async_copy(whole, out.at[pl.ds(0, base)], sems.at[0]),
        pltpu.make_async_copy(own, out.at[pl.ds(to, rows)], sems.at[1]),
    ]
    for copy in copies:
        copy.start()
    for copy in copies:
        copy.wait()


def place_parts_kernel(order, filled, *rest):
    parts, out, sems = rest[:-2], rest[-2], rest[-1]
    rows = parts[0].shape[0]
    base = out.shape[0] - (len(parts) + 1) * rows
    copies = []
    for k, part in enumerate(parts):
        to = pl.multiple_of(base + order[k + 1] * rows, BLOCK)
        copies.append(pltpu.make_async_copy(part, out.at[pl.ds(to, rows)], sems.at[k]))
    for copy in copies:
        copy.start()
    for copy in copies:
        copy.wait()


def place(kernel, length, order, *arrays, aliases=()):
    anywhere = pl.BlockSpec(memory_space=pl.ANY)
    return pl.pallas_call(
        kernel,
        grid_spec=pltpu.PrefetchScalarGridSpec(
            num_scalar_prefetch=1,
            grid=(1,),
            in_specs=[anywhere] * len(arrays),
            out_specs=anywhere,
            scratch_shapes=[pltpu.SemaphoreType.DMA((len(arrays),))],
        ),
        out_shape=jax.ShapeDtypeStruct((length, WIDTH), bf16),
        input_output_aliases=dict(aliases),
        compiler_params=pltpu.CompilerParams(vmem_limit_bytes=8 << 20),
        cost_estimate=pl.CostEstimate(flops=1 << 20, bytes_accessed=4 << 20, transcendentals=0),
        name="place",
    )(order, *arrays)


def exchange(pieces, axes):
    return lax.all_to_all(pieces, axes, split_axis=0, concat_axis=0, tiled=True)


def tied(*arrays):
    return lax.optimization_barrier(arrays)


def along_y(piece, shift):
    ring = lax.axis_size(TP[0])
    return lax.ppermute(piece, TP[0], [(i, (i + shift) % ring) for i in range(ring)])


def across(piece):
    return lax.ppermute(piece, TP[1], [(0, 1), (1, 0)])


def chosen_of(options, index):
    result = options[0]
    for n, option in enumerate(options[1:], 1):
        result = jnp.where(index == n, option, result)
    return result


def both_cores(parts):
    same = jnp.stack(parts)
    return same, across(same)


OFFSETS = (0, -1, 1, 2)


def piece_order(sign):
    ring = lax.axis_size(TP[0])
    y = lax.axis_index(TP[0])
    c = lax.axis_index(TP[1])
    rows = jnp.stack([(y + ring + sign * d) % ring for d in OFFSETS])
    return jnp.concatenate([2 * rows + c, 2 * rows + 1 - c]).astype(jnp.int32)


def send_pieces(pieces):
    ring = lax.axis_size(TP[0])
    got = []
    for k in range(2 * ring):
        step, swap = OFFSETS[k % ring], k // ring
        pairs = [
            (2 * y + c, 2 * ((y - step) % ring) + (c + swap) % 2)
            for y in range(ring)
            for c in range(2)
        ]
        got.append(lax.ppermute(pieces[k], TP, pairs) if k else pieces[0])
    return got


def local(tokens, w_query, w_key, w_value, w_out, query_gain, key_gain, out_gain, chosen):
    length, _ = tokens.shape
    blocks_here = length // BLOCK
    devices = lax.axis_size(KV)
    position = lax.axis_index(KV)
    ranks = lax.axis_size(TP)
    key_row = key_gain[None, :]
    query_row = (query_gain * (HEAD_DIM ** (-0.5) * LOG2E))[None, :]

    rank = lax.axis_index(TP).astype(jnp.int32).reshape(1)
    long, side = lax.axis_size(KV[0]), lax.axis_size(KV[1])
    z, x = lax.axis_index(KV[0]), lax.axis_index(KV[1])
    columns = token_shares(rank, tokens, long, side)
    chosen, *columns = tied(chosen, *columns)
    columns = columns[:1] + [lax.ppermute(columns[n], KV, [(0, n * side)]) for n in range(1, long)]

    usable = chosen >= 0
    pick = jnp.where(usable, chosen, 0)
    owner_of = pick // blocks_here
    all_blocks = jnp.arange(devices * blocks_here, dtype=jnp.int32)
    marked = jnp.where(usable & (owner_of != position), chosen, -1)
    wanted = jnp.any(marked[:, :, None] == all_blocks[None, None, :], axis=(0, 1)).reshape(
        devices, blocks_here
    )
    rank_of = jnp.cumsum(wanted.astype(jnp.int32), axis=1) - 1
    local_ids = jnp.arange(blocks_here, dtype=jnp.int32)
    places = wanted[:, :, None] & (
        rank_of[:, :, None] == jnp.arange(HOT, dtype=jnp.int32)[None, None, :]
    )
    named = jnp.sum(jnp.where(places, local_ids[None, :, None], 0), axis=1).astype(jnp.int32)
    requests = jnp.concatenate([named, jnp.broadcast_to(named[:1], named.shape)], axis=1)
    order = piece_order(1)
    toward = piece_order(-1)
    same_order = jnp.arange(ranks, dtype=jnp.int32)

    asked = exchange(requests, KV)
    pairs = project_kv(tokens, w_key, w_value, key_row).reshape(-1, WIDTH)
    asked_near = asked[:, :REACH].reshape(-1)
    asked_hot = asked[:, HOT:].reshape(-1)

    sent = gather_near(asked_near, pairs)
    sent, *columns = tied(sent, *columns)
    held = [chosen_of([c[n] for c in columns], z) for n in range(side)]
    starts = range(0, devices, side)
    held = held[:1] + [
        lax.ppermute(held[n], KV, [(i, i + n) for i in starts]) for n in range(1, side)
    ]
    near = exchange(sent.reshape(devices, -1, WIDTH), KV).reshape(-1, WIDTH)
    shares = chosen_of(held, x)
    parts = [shares] + [along_y(shares, shift) for shift in (1, -1, 2)]
    w_after = along_y(w_out, 1)
    w_own = across(w_out)
    again, sent = tied(tokens, sent)
    queries = project_q(again, w_query, query_row)
    queries, *parts = tied(queries, *parts)
    rows_same, rows_other = both_cores(parts)
    sent_hot = project_sent(
        asked_hot, order, rows_same, rows_other, w_key, w_value, key_row, devices
    )
    pick, owner_of, rank_of, usable, sent_hot = tied(pick, owner_of, rank_of, usable, sent_hot)
    flat_rank = rank_of.reshape(-1)
    slot_rank = jnp.sum(
        jnp.where(pick[:, :, None] == all_blocks[None, None, :], flat_rank[None, None, :], 0), axis=-1
    )
    near_at = blocks_here + owner_of * REACH + slot_rank
    hot_at = blocks_here + devices * REACH + slot_rank
    at = jnp.where(
        owner_of == position, pick % blocks_here, jnp.where(owner_of == 0, hot_at, near_at)
    )
    at = jnp.where(usable, at, 0).astype(jnp.int32).reshape(-1)
    mask = jnp.repeat(usable.astype(f32), BLOCK, axis=1)

    order, toward, same_order, sent_hot = tied(order, toward, same_order, sent_hot)
    near, sent_hot = tied(near, sent_hot)
    hot = exchange(sent_hot, KV)
    w_before = along_y(w_out, -1)
    w_far = along_y(w_after, 1)

    gains = out_gain.reshape(ranks, 1, WIDTH)
    early = (FIRST_BLOCKS * blocks_here) // 8
    first = attend(0, early, False, at, same_order, queries, mask, pairs, near, hot)
    first = exchange(first, TP)
    second = attend(early, blocks_here - early, True, at, toward, queries, mask, pairs, near, hot)
    *second, w_after, w_before, w_far = tied(*second, w_after, w_before, w_far)
    w_swapped = [across(w_after), across(w_before), across(w_far)]
    weights = [w_out, w_after, w_before, w_far, w_own] + w_swapped
    second = send_pieces(second)
    first = project_out(False, order, same_order, first, weights, gains)
    moved = exchange(first, TP)
    second = tied(first, *second)[1:]
    second = project_out(True, order, toward, second, weights, gains)
    second = send_pieces(second)
    filled = place(place_whole_kernel, length, order, moved.reshape(-1, WIDTH), second[0])
    return place(place_parts_kernel, length, order, filled, *second[1:], aliases={1: 0})


def solution(mesh):
    split = Mesh(mesh.devices.reshape(4, 4, 4, 2), KV + TP)
    return jax.shard_map(
        local,
        mesh=split,
        in_specs=(
            P(KV, None),
            P(None, TP),
            P(None, TP),
            P(None, TP),
            P(TP, None),
            P(),
            P(),
            P(),
            P(KV, None),
        ),
        out_specs=P(KV, TP),
        check_vma=False,
    )
```
